32 devices in a mesh: sp: 16 (over z, y, x), tp: 2 (over core).
Axes of the slice: x: 2, y: 2, z: 4, core: 2. Of those that a mesh axis runs over, the one named last changes fastest.
Arguments:
- queries: bfloat16 [6144, 2048], P('sp', 'tp'), may hold values from -6 to 6
- key_heads: bfloat16 [6144, 1024], P('sp', 'tp'), may hold values from -6 to 6
- value_heads: bfloat16 [6144, 1024], P('sp', 'tp'), may hold values from -6 to 6
- sink_logit: float32 [16], P('tp'), may hold values from 3 to 7
- doc_ids: int32 [6144], replicated, may hold values from 0 to 3, never falling along the last dimension, each value on 1 to 3072 neighbouring positions
- residual: bfloat16 [6144, 2048], P('sp'), may hold values from -6 to 6
- out_proj: bfloat16 [2048, 2048], P('tp'), may hold values from -0.125 to 0.125
- gain_mix: float32 [2048], replicated, may hold values from 0.1 to 1.9
- up_proj: bfloat16 [2048, 8192], P('sp', 'tp'), may hold values from -0.125 to 0.125
- down_proj: bfloat16 [8192, 2048], P('tp', 'sp'), may hold values from -0.0625 to 0.0625
- gain_ffn_in: float32 [2048], replicated, may hold values from 0.1 to 1.9
- gain_ffn_out: float32 [2048], replicated, may hold values from 0.1 to 1.9
Outputs:
- layer_out: bfloat16 [6144, 2048], P(('sp', 'tp'))
The draws below stay inside these ranges and needn't reach their ends.
All inputs are finite; a program needn't handle non-finite values.
Results may differ from the reference program's by a relative error of at most 0.019.
Values may be sent and summed in bfloat16 or wider, within the bound.
A program may use at most 128 MiB of HBM per device.

```python
import math
import jax
import jax.numpy as jnp
import numpy as np
from jax import lax

D = 2048
HEADS = 16
KV = 8
HD = 128
FF = 8192
WINDOW = 128
TOKENS = 6144
DOCS = 4
DOC_MOST = 3072
N_TP = 2


def draw_key_heads(key, part):
    noise_key = jax.random.fold_in(key, 2)
    noise = jax.random.normal(noise_key, (TOKENS, KV * HD), jnp.float32)
    return jnp.clip(noise, -6.0, 6.0).astype(jnp.bfloat16)


def draw_queries(key, part):
    noise_key = jax.random.fold_in(key, 1)
    noise = jax.random.normal(noise_key, (TOKENS, HEADS * HD), jnp.float32)
    return jnp.clip(noise, -6.0, 6.0).astype(jnp.bfloat16)


def level_of(key, extent, pieces, low, largest):
    loudness, own = 1.0, jax.random.fold_in(key, 6)
    for axis_at, shards_of in pieces:
        heights = jnp.exp(jax.random.uniform(jax.random.fold_in(own, axis_at), (shards_of,), jnp.float32, low / len(pieces), largest / len(pieces)))
        loudness = loudness * jnp.repeat(heights, extent[axis_at] // shards_of).reshape([-1 if axis == axis_at else 1 for axis in range(len(extent))])
    return loudness


def length_profile(amount, total, bound, slope):
    loads = [(1 << 20) // math.isqrt(rank ** slope) + 1 for rank in range(2, amount + 1)]
    spare, holding = total - bound - (amount - 1), [1] * (amount - 1)
    while spare > 0:
        movable = [i for i in range(amount - 1) if holding[i] < bound]
        mass, budget = sum([loads[i] for i in movable]), spare
        for i in movable:
            extra = min(bound - holding[i], max(1, budget * loads[i] // mass), spare)
            holding[i] = holding[i] + extra
            spare = spare - extra
    return np.array([bound] + holding)


def uneven_parts(own_key, amount, total, most, skew):
    if amount == 2:
        one = jax.random.randint(own_key, (), max(1, total - most), min(most, total - 1) + 1)
        return jnp.stack([one, total - one])
    sizes = jnp.asarray(length_profile(amount, total, most, skew), jnp.int32)
    couples = (amount - 1) // 2
    donor, sink = sizes[1:1 + 2 * couples:2], sizes[2:2 + 2 * couples:2]
    room = jnp.minimum(donor - 1, most - sink)
    shifted = jax.random.randint(jax.random.fold_in(own_key, 1), (couples,), 0, 1 << 20) % (room + 1)
    sizes = sizes.at[1:1 + 2 * couples:2].set(donor - shifted).at[2:2 + 2 * couples:2].set(sink + shifted)
    return sizes[jax.random.permutation(jax.random.fold_in(own_key, 2), amount)]


def centred(rng, dims, spread, bound, cuts=(), held_as=jnp.bfloat16):
    array = spread * jax.random.normal(rng, dims, jnp.float32)
    if cuts:
        array = array * level_of(rng, dims, cuts, -0.22, 0.18)
    return jnp.clip(array, -bound, bound).astype(held_as)


def setup_inputs(seed: int = 0) -> dict:
    keys = jax.random.split(jax.random.key(seed), 13)
    return {
        "queries": draw_queries(jax.random.fold_in(keys[12], 71), 0),
        "key_heads": draw_key_heads(jax.random.fold_in(keys[12], 71), 0),
        "value_heads": centred(keys[2], (TOKENS, KV * HD), 1.0, 6.0, ((0, 16), (1, 2))),
        "sink_logit": jnp.clip(3.0 + 4.0 * jax.random.uniform(keys[3], (HEADS,), jnp.float32) ** level_of(keys[3], (HEADS,), ((0, 2),), -0.2, 0.2), 3.0, 7.0),
        "doc_ids": jnp.searchsorted(jnp.cumsum(uneven_parts(keys[4], DOCS, TOKENS, DOC_MOST, 1)), jnp.arange(TOKENS), side="right").astype(jnp.int32),
        "residual": centred(keys[5], (TOKENS, D), 1.0, 6.0, ((0, 16),)),
        "out_proj": centred(keys[6], (HEADS * HD, D), (HEADS * HD) ** -0.5, 0.125, ((0, 2),)),
        "gain_mix": jnp.clip(1.0 + 0.18 * jax.random.normal(keys[7], (D,), jnp.float32), 0.1, 1.9),
        "up_proj": centred(keys[8], (D, FF), D ** -0.5, 0.125, ((0, 16), (1, 2))),
        "down_proj": centred(keys[9], (FF, D), FF ** -0.5, 0.0625, ((0, 2), (1, 16))),
        "gain_ffn_in": jnp.clip(1.0 + 0.18 * jax.random.normal(keys[10], (D,), jnp.float32), 0.1, 1.9),
        "gain_ffn_out": jnp.clip(1.0 + 0.18 * jax.random.normal(keys[11], (D,), jnp.float32), 0.1, 1.9),
    }


def rotate(field, places):
    half_dim = HD // 2
    inv_freq = 10000.0 ** (-jnp.arange(0, HD, 2, dtype=jnp.float32) / HD)
    angles = places[:, None, None] * inv_freq[None, None, :]
    cosine = jnp.cos(angles)
    sine = jnp.sin(angles)
    lower = field[..., :half_dim].astype(jnp.float32)
    upper = field[..., half_dim:].astype(jnp.float32)
    return jnp.concatenate([lower * cosine - upper * sine, upper * cosine + lower * sine], axis=-1).astype(jnp.bfloat16)

def banded(field, blocks):
    framed = field.reshape((blocks + 2, WINDOW) + field.shape[1:])
    return jnp.concatenate([framed[:-2], framed[1:-1], framed[2:]], axis=1)

def rms_scale(field, gain_vec):
    return field * lax.rsqrt(lax.optimization_barrier(jnp.mean(field * field, axis=-1, keepdims=True)) + 1e-06) * gain_vec

def reference(queries, key_heads, value_heads, sink_logit, doc_ids, residual, out_proj, gain_mix, up_proj, down_proj, gain_ffn_in, gain_ffn_out):
    length = queries.shape[0]
    blocks = length // WINDOW
    group_size = HEADS // KV
    places = jnp.arange(length).astype(jnp.float32)
    rotated_q = rotate(queries.reshape(length, HEADS, HD), places).reshape(blocks, WINDOW, KV, group_size, HD)
    rotated_k = rotate(key_heads.reshape(length, KV, HD), places)
    framing = ((WINDOW, WINDOW), (0, 0), (0, 0))
    key_win = banded(jnp.pad(rotated_k, framing), blocks)
    val_win = banded(jnp.pad(value_heads.reshape(length, KV, HD), framing), blocks)
    key_docs = banded(jnp.pad(doc_ids, (WINDOW, WINDOW), constant_values=-1), blocks)
    query_docs = doc_ids.reshape(blocks, WINDOW)
    q_index = jnp.arange(WINDOW)[:, None]
    k_index = jnp.arange(3 * WINDOW)[None, :]
    in_window = jnp.abs(k_index - WINDOW - q_index) <= WINDOW
    allowed = in_window[None] & (query_docs[:, :, None] == key_docs[:, None, :])

    def one_head(items):
        q_head, k_head, v_head, sink_vec = items
        scores = jnp.einsum('nqgd,nsd->ngqs', q_head.astype(jnp.float32), k_head.astype(jnp.float32)) * HD ** (-0.5)
        masked = jnp.where(allowed[:, None], scores, -1e+30)
        sink_col = sink_vec[None, :, None]
        top_score = jnp.maximum(lax.optimization_barrier(jnp.max(masked, axis=-1)), sink_col)
        exp_scores = jnp.where(allowed[:, None], jnp.exp(masked - top_score[..., None]), 0.0)
        denom_sum = lax.optimization_barrier(jnp.sum(exp_scores, axis=-1)) + jnp.exp(sink_col - top_score)
        probs = (exp_scores / denom_sum[..., None]).astype(jnp.bfloat16)
        return jnp.einsum('ngqs,nsd->nqgd', probs.astype(jnp.float32), v_head.astype(jnp.float32)).astype(jnp.bfloat16)
    attended = lax.map(one_head, (jnp.moveaxis(rotated_q, 2, 0), jnp.moveaxis(key_win, 2, 0), jnp.moveaxis(val_win, 2, 0), sink_logit.reshape(KV, group_size)))
    attn = jnp.moveaxis(attended, 0, 2).reshape(length, HEADS * HD)
    attn_cols = HEADS * HD // N_TP
    mixed = jnp.zeros((length, D), jnp.float32)
    for group in range(N_TP):
        partial_value = jnp.dot(attn[:, group * attn_cols:(group + 1) * attn_cols], out_proj[group * attn_cols:(group + 1) * attn_cols], preferred_element_type=jnp.float32).astype(jnp.bfloat16)
        mixed = mixed + lax.optimization_barrier(partial_value).astype(jnp.float32)
    after_mix = (residual.astype(jnp.float32) + rms_scale(mixed, gain_mix)).astype(jnp.bfloat16)
    normed = rms_scale(after_mix.astype(jnp.float32), gain_ffn_in).astype(jnp.bfloat16)
    hid_cols = FF // N_TP
    ffn_out = jnp.zeros((length, D), jnp.float32)
    for group in range(N_TP):
        up_acts = jnp.dot(normed, up_proj[:, group * hid_cols:(group + 1) * hid_cols], preferred_element_type=jnp.float32)
        hidden = jnp.square(jax.nn.relu(up_acts)).astype(jnp.bfloat16)
        partial_value = jnp.dot(hidden, down_proj[group * hid_cols:(group + 1) * hid_cols], preferred_element_type=jnp.float32).astype(jnp.bfloat16)
        ffn_out = ffn_out + lax.optimization_barrier(partial_value).astype(jnp.float32)
    return (after_mix.astype(jnp.float32) + rms_scale(ffn_out, gain_ffn_out)).astype(jnp.bfloat16)
```

```python
import functools
import math

import jax
import jax.numpy as jnp
from jax import lax
from jax.experimental import pallas as pl
from jax.experimental.pallas import tpu as pltpu
from jax.sharding import Mesh, PartitionSpec as P

MESH = pl.DeviceIdType.MESH
BF16, F32 = jnp.bfloat16, jnp.float32

HD = 128
WINDOW = 128
SP = ("a", "b", "c", "d")
GRP = ("c", "d")
CROSS = ("a", "b")


def padded(shard, sides, width):
    for axis, dim in sides:
        devices, length = (lax.axis_size(axis), shard.shape[dim])
        up = [(i, (i + 1) % devices) for i in range(devices - 1)]
        down = [(j, i) for i, j in up]
        last = lax.slice_in_dim(shard, length - width, length, axis=dim)
        first = lax.slice_in_dim(shard, 0, width, axis=dim)
        before = lax.ppermute(last, axis, up)
        after = lax.ppermute(first, axis, down)
        shard = jnp.concatenate([before, shard, after], axis=dim)
    return shard


def rotate(field, places):
    half_dim = HD // 2
    inv_freq = 10000.0 ** (-jnp.arange(0, HD, 2, dtype=jnp.float32) / HD)
    angles = places[:, None, None] * inv_freq[None, None, :]
    cosine = jnp.cos(angles)
    sine = jnp.sin(angles)
    lower = field[..., :half_dim].astype(jnp.float32)
    upper = field[..., half_dim:].astype(jnp.float32)
    return jnp.concatenate(
        [lower * cosine - upper * sine, upper * cosine + lower * sine], axis=-1
    ).astype(jnp.bfloat16)


def banded(field, blocks):
    framed = field.reshape((blocks + 2, WINDOW) + field.shape[1:])
    return jnp.concatenate([framed[:-2], framed[1:-1], framed[2:]], axis=1)


def rms_scale(field, gain_vec):
    return field * lax.rsqrt(jnp.mean(field * field, axis=-1, keepdims=True) + 1e-06) * gain_vec


def swap_tp(rows):
    return lax.ppermute(rows, "tp", [(0, 1), (1, 0)])


def gather_tp(rows):
    if lax.axis_size("tp") == 2:
        return jnp.concatenate([rows, swap_tp(rows)], axis=0)
    return lax.all_gather(rows, "tp", axis=0, tiled=True)


def scatter_tp(partial_value, own_first=True):
    devices = lax.axis_size("tp")
    if devices != 2:
        return lax.psum_scatter(partial_value, "tp", scatter_dimension=0, tiled=True).astype(
            jnp.float32
        )
    share = partial_value.shape[0] // 2
    if own_first:
        own, other = partial_value[:share], partial_value[share:]
    else:
        me = lax.axis_index("tp")
        own = lax.dynamic_slice_in_dim(partial_value, me * share, share, 0)
        other = lax.dynamic_slice_in_dim(partial_value, (1 - me) * share, share, 0)
    return own.astype(jnp.float32) + swap_tp(other).astype(jnp.float32)


def to_peer(rows, k):
    if k == 0:
        return rows
    return lax.ppermute(rows, GRP, [(i, i ^ k) for i in range(4)])


def attention_part(sp, queries, key_heads, value_heads, sink_logit, doc_ids, out_proj):
    tok_count = queries.shape[0]
    blocks = tok_count // WINDOW
    q_local = queries.shape[1] // HD
    kv_local = key_heads.shape[1] // HD
    group_size = q_local // kv_local
    offset = lax.axis_index(sp) * tok_count
    places = (offset + jnp.arange(tok_count)).astype(jnp.float32)
    rotated_q = rotate(queries.reshape(tok_count, q_local, HD), places).reshape(
        blocks, WINDOW, kv_local, group_size, HD
    )
    rotated_k = rotate(key_heads.reshape(tok_count, kv_local, HD), places).reshape(
        tok_count, kv_local * HD
    )
    rimmed = padded(jnp.stack([rotated_k, value_heads]), ((sp, 1),), WINDOW)
    key_win = banded(rimmed[0].reshape(-1, kv_local, HD), blocks)
    val_win = banded(rimmed[1].reshape(-1, kv_local, HD), blocks)
    padded_docs = jnp.pad(doc_ids, (WINDOW, WINDOW), constant_values=-1)
    key_docs = banded(lax.dynamic_slice_in_dim(padded_docs, offset, tok_count + 2 * WINDOW), blocks)
    query_docs = lax.dynamic_slice_in_dim(doc_ids, offset, tok_count).reshape(blocks, WINDOW)
    q_index = jnp.arange(WINDOW)[:, None]
    k_index = jnp.arange(3 * WINDOW)[None, :]
    in_window = jnp.abs(k_index - WINDOW - q_index) <= WINDOW
    allowed = (in_window[None] & (query_docs[:, :, None] == key_docs[:, None, :]))[:, None, None]
    scores = jnp.einsum(
        "nqkgd,nskd->nkgqs", rotated_q, key_win, preferred_element_type=jnp.float32
    ) * HD ** (-0.5)
    masked = jnp.where(allowed, scores, -1e30)
    sink_col = sink_logit.reshape(kv_local, group_size)[None, :, :, None]
    top_score = jnp.maximum(jnp.max(masked, axis=-1), sink_col)
    exp_scores = jnp.where(allowed, jnp.exp(masked - top_score[..., None]), 0.0)
    denom_sum = jnp.sum(exp_scores, axis=-1) + jnp.exp(sink_col - top_score)
    probs = (exp_scores / denom_sum[..., None]).astype(jnp.bfloat16)
    attn = (
        jnp.einsum("nkgqs,nskd->nqkgd", probs, val_win, preferred_element_type=jnp.float32)
        .astype(jnp.bfloat16)
        .reshape(tok_count, q_local * HD)
    )
    part = jnp.dot(attn, out_proj, preferred_element_type=jnp.float32).astype(jnp.bfloat16)
    return part


def general_body(
    queries,
    key_heads,
    value_heads,
    sink_logit,
    doc_ids,
    residual,
    out_proj,
    gain_mix,
    up_proj,
    down_proj,
    gain_ffn_in,
    gain_ffn_out,
):
    up_quarter = lax.all_to_all(up_proj, GRP, split_axis=1, concat_axis=0, tiled=True)
    down_quarter = lax.all_to_all(down_proj, GRP, split_axis=0, concat_axis=1, tiled=True)
    queries, key_heads, up_quarter, down_quarter = lax.optimization_barrier(
        (queries, key_heads, up_quarter, down_quarter)
    )
    half_units = up_quarter.shape[1] // 2
    up_early = lax.all_gather(up_quarter[:, :half_units], CROSS, axis=0, tiled=True)
    up_late = lax.all_gather(up_quarter[:, half_units:], CROSS, axis=0, tiled=True)
    down_all = lax.all_gather(down_quarter, CROSS, axis=0, tiled=False)
    share_rows = queries.shape[0] // lax.axis_size("tp")
    part = attention_part(SP, queries, key_heads, value_heads, sink_logit, doc_ids, out_proj)
    part, up_early = lax.optimization_barrier((part, up_early))
    mixed = scatter_tp(part, own_first=False)
    own_residual = lax.dynamic_slice_in_dim(
        residual, lax.axis_index("tp") * share_rows, share_rows, 0
    )
    after_mix = (own_residual.astype(jnp.float32) + rms_scale(mixed, gain_mix)).astype(jnp.bfloat16)
    normed = rms_scale(after_mix.astype(jnp.float32), gain_ffn_in).astype(jnp.bfloat16)
    sizes = [lax.axis_size(a) for a in SP]
    order = [SP.index(a) for a in CROSS + GRP]
    width = normed.shape[1]
    strip = width // math.prod(sizes)
    normed = (
        normed.reshape(share_rows, *sizes, strip)
        .transpose(0, *[1 + o for o in order], 5)
        .reshape(share_rows, width)
    )
    blocks = [to_peer(normed, k) for k in range(4)]
    partials = []
    for k in (3, 2, 1, 0):
        rows = gather_tp(blocks[k])
        hidden = jnp.concatenate(
            [
                jnp.square(
                    jax.nn.relu(jnp.dot(rows, w, preferred_element_type=jnp.float32))
                ).astype(jnp.bfloat16)
                for w in (up_early, up_late)
            ],
            axis=1,
        )
        partial_value = jnp.concatenate(
            [
                jnp.dot(hidden, down_all[i], preferred_element_type=jnp.float32).astype(jnp.bfloat16)
                for i in range(down_all.shape[0])
            ],
            axis=1,
        )
        partials.append(to_peer(scatter_tp(partial_value).astype(jnp.bfloat16), k))
    ffn_out = sum(p.astype(jnp.float32) for p in partials)
    back = [order.index(i) for i in range(4)]
    ffn_out = (
        ffn_out.reshape(share_rows, *[sizes[o] for o in order], strip)
        .transpose(0, *[1 + b for b in back], 5)
        .reshape(share_rows, width)
    )
    return (after_mix.astype(jnp.float32) + rms_scale(ffn_out, gain_ffn_out)).astype(jnp.bfloat16)


def ffn_kernel(
    normed_ref,
    after_ref,
    gain_ref,
    up_ref,
    down_ref,
    out_ref,
    w_up,
    w_down,
    tokens,
    hidden,
    part,
    peer,
    x_out,
    x_in,
    z_out,
    z_in,
    ffn,
    local_sem,
    w_send,
    w_recv,
    y_send,
    y_recv,
    t_send,
    t_recv,
    c_send,
    c_recv,
):
    me, core = lax.axis_index("sp"), lax.axis_index("tp")
    z, y, x = me // 4, lax.rem(me // 2, 2), lax.rem(me, 2)
    zl = lax.rem(z, 2)
    z1, z2, z3 = z + 1 - 2 * zl, lax.rem(z + 2, 4), 3 - z
    xo, yo = 1 - x, 1 - y
    rows, width = normed_ref.shape
    strip, units = up_ref.shape[0], up_ref.shape[1] // 4
    chunk = 2 * strip
    half = 4 * rows

    def place(zz, yy, xx):
        return zz * 4 + yy * 2 + xx

    def col(start, size):
        return pl.ds(pl.multiple_of(start, size), size)

    def slot(w, s):
        if w == 0:
            return w_up.at[col(s * strip, strip), :]
        return w_down.at[:, col(s * strip, strip)]

    def shard(w, zz, xx):
        q = lax.rem(zz, 2) * 2 + xx
        if w == 0:
            return up_ref.at[:, col(q * units, units)]
        return down_ref.at[col(q * units, units), :]

    def remote(src, dst, send, recv, dev, c):
        return pltpu.make_async_remote_copy(
            src_ref=src,
            dst_ref=dst,
            send_sem=send,
            recv_sem=recv,
            device_id=(dev, c),
            device_id_type=MESH,
        )

    direct = ((z, 1), (z3, 0), (z3, 1), (z2, 0), (z2, 1), (z1, 0), (z1, 1))

    def to_x(dx):
        return xo if dx else x

    def send_direct(w, k):
        zz, dx = direct[k]
        return remote(
            shard(w, zz, to_x(dx)),
            slot(w, me),
            w_send.at[w, k],
            w_recv.at[w, z * 2 + dx],
            place(zz, y, to_x(dx)),
            core,
        )

    def send_own_y(w):
        return remote(
            shard(w, z, x),
            slot(w, me),
            w_send.at[w, 7],
            y_recv.at[w, z * 2],
            place(z, yo, x),
            core,
        )

    def keep_own(w):
        return pltpu.make_async_copy(shard(w, z, x), slot(w, me), local_sem.at[w])

    def arrival(w, zz, dx):
        s = slot(w, place(zz, y, to_x(dx)))
        return remote(s, s, y_send.at[w, zz * 2 + dx], w_recv.at[w, zz * 2 + dx], me, core)

    def forward(w, zz, dx):
        s = slot(w, place(zz, y, to_x(dx)))
        return remote(
            s,
            s,
            y_send.at[w, zz * 2 + dx],
            y_recv.at[w, zz * 2 + dx],
            place(z, yo, x),
            core,
        )

    def y_arrival(w, zz, dx):
        s = slot(w, place(zz, yo, to_x(dx)))
        return remote(s, s, y_send.at[w, zz * 2 + dx], y_recv.at[w, zz * 2 + dx], me, core)

    def relay(w, zz, dx):
        arrival(w, zz, dx).wait_recv()
        forward(w, zz, dx).start()

    m_own, m_z = zl * 2 + x, (1 - zl) * 2 + x
    m_x, m_d = zl * 2 + xo, (1 - zl) * 2 + xo

    def token_rows(c, m):
        return tokens.at[col((c * 4 + m) * rows, rows), :]

    def token_copy(k, m, dev, c):
        s = token_rows(core, m)
        return remote(s, s, t_send.at[k], t_recv.at[k], dev, c)

    def token_arrival(k, c, m):
        s = token_rows(c, m)
        return remote(s, s, t_send.at[k], t_recv.at[k], me, core)

    x_dev, z_dev, y_dev = place(z, y, xo), place(z1, y, x), place(z, yo, x)
    barrier = pltpu.get_barrier_semaphore()
    friends = [(place(zz, y, to_x(dx)), core) for zz, dx in direct] + [(y_dev, core), (me, 1 - core)]
    for dev in friends:
        pl.semaphore_signal(barrier, inc=1, device_id=dev, device_id_type=MESH)
    for w in (0, 1):
        keep_own(w).start()
    tokens[col((core * 4 + m_own) * rows, rows), :] = normed_ref[...]
    pl.semaphore_wait(barrier, len(friends))

    token_copy(0, m_own, z_dev, core).start()
    token_copy(1, m_own, x_dev, core).start()
    token_copy(3, m_own, me, 1 - core).start()
    send_own_y(0).start()
    for k in range(7):
        send_direct(0, k).start()
    relay(0, z, 1)
    token_arrival(0, core, m_z).wait_recv()
    token_copy(2, m_z, x_dev, core).start()
    token_copy(4, m_z, me, 1 - core).start()
    send_own_y(1).start()
    for k in range(7):
        send_direct(1, k).start()
    relay(0, z1, 0)
    relay(0, z1, 1)
    token_arrival(1, core, m_x).wait_recv()
    token_copy(5, m_x, me, 1 - core).start()
    for zz in (z3, z2):
        for dx in (0, 1):
            relay(0, zz, dx)
    token_arrival(2, core, m_d).wait_recv()
    token_copy(6, m_d, me, 1 - core).start()
    keep_own(0).wait()
    for zz in (z, z1, z3, z2):
        for dx in (0, 1):
            y_arrival(0, zz, dx).wait_recv()

    def up_rows(c, m):
        def step(n, carry):
            lines = col((c * 4 + m) * rows, rows)
            cols = col(n * chunk, chunk)
            acts = jnp.dot(tokens[lines, :], w_up[:, cols], preferred_element_type=F32)
            acts = jnp.maximum(acts, 0.0)
            hidden[lines, cols] = (acts * acts).astype(BF16)
            return carry

        lax.fori_loop(0, units // chunk, step, 0)

    for k, m in ((3, m_own), (4, m_z), (5, m_x)):
        up_rows(core, m)
        token_arrival(k, 1 - core, m).wait_recv()
        up_rows(1 - core, m)
    relay(1, z, 1)
    relay(1, z1, 0)
    relay(1, z1, 1)
    up_rows(core, m_d)
    token_arrival(6, 1 - core, m_d).wait_recv()
    up_rows(1 - core, m_d)
    keep_own(1).wait()

    zh = z // 2
    near, far = (zh * 2, zh * 2 + 1), (2 - zh * 2, 3 - zh * 2)
    order = [(near[0], y), (near[1], y), (near[0], yo), (near[1], yo)]
    order += [(far[0], y), (far[1], y), (far[0], yo), (far[1], yo)]

    def columns(i):
        zz, yy = order[i]
        return col((zz * 2 + yy) * chunk, chunk)

    def stage_a(i):
        zz, yy = order[i]
        if i >= 4 and i % 4 < 2:
            for dx in (0, 1):
                relay(1, zz, dx)
        elif i % 4 >= 2:
            for dx in (0, 1):
                y_arrival(1, zz, dx).wait_recv()
        cols = columns(i)

        def step(b, carry):
            lines = col(b * 2 * rows, 2 * rows)
            part[lines, cols] = jnp.dot(
                hidden[lines, :], w_down[:, cols], preferred_element_type=F32
            ).astype(BF16)
            return carry

        lax.fori_loop(0, 4, step, 0)
        peer_copy(i).start()

    def peer_copy(i):
        cols = columns(i)
        return remote(
            part.at[col((1 - core) * half, half), cols],
            peer.at[:, cols],
            c_send.at[0, i],
            c_recv.at[0, i],
            me,
            1 - core,
        )

    def chip_sum(m, cols):
        own = part[col((core * 4 + m) * rows, rows), cols].astype(F32)
        return own + peer[col(m * rows, rows), cols].astype(F32)

    def x_copy(i):
        cols = columns(i)
        return remote(x_out.at[:, cols], x_in.at[:, cols], c_send.at[1, i], c_recv.at[1, i], x_dev, core)

    def z_copy(i):
        cols = columns(i)
        return remote(z_out.at[:, cols], z_in.at[:, cols], c_send.at[2, i], c_recv.at[2, i], z_dev, core)

    def stage_b(i):
        cols = columns(i)
        peer_copy(i).wait_recv()
        x_out[:rows, cols] = chip_sum(m_x, cols).astype(BF16)
        x_out[rows:, cols] = chip_sum(m_d, cols).astype(BF16)
        x_copy(i).start()

    def stage_c(i):
        cols = columns(i)
        x_copy(i).wait_recv()
        z_out[:, cols] = (chip_sum(m_z, cols) + x_in[rows:, cols].astype(F32)).astype(BF16)
        z_copy(i).start()

    def stage_d(i):
        cols = columns(i)
        z_copy(i).wait_recv()
        ffn[:, cols] = (
            chip_sum(m_own, cols) + x_in[:rows, cols].astype(F32) + z_in[:, cols].astype(F32)
        )

    for i in range(8 + 4):
        if i < 8:
            stage_a(i)
        if 0 <= i - 1 < 8:
            stage_b(i - 1)
        if 0 <= i - 3 < 8:
            stage_c(i - 3)
        if 0 <= i - 4 < 8:
            stage_d(i - 4)

    def finish(r, carry):
        lines = col(r * 16, 16)
        field = ffn[lines, :]
        scale = lax.rsqrt(jnp.mean(field * field, axis=-1, keepdims=True) + 1e-06)
        out_ref[lines, :] = (
            after_ref[lines, :].astype(F32) + field * scale * gain_ref[...]
        ).astype(BF16)
        return carry

    lax.fori_loop(0, rows // 16, finish, 0)

    for w in (0, 1):
        send_own_y(w).wait_send()
        for k in range(7):
            send_direct(w, k).wait_send()
            zz, dx = direct[k]
            forward(w, zz, dx).wait_send()
    token_copy(0, m_own, z_dev, core).wait_send()
    token_copy(1, m_own, x_dev, core).wait_send()
    token_copy(2, m_z, x_dev, core).wait_send()
    for k, m in ((3, m_own), (4, m_z), (5, m_x), (6, m_d)):
        token_copy(k, m, me, 1 - core).wait_send()
    for i in range(8):
        peer_copy(i).wait_send()
        x_copy(i).wait_send()
        z_copy(i).wait_send()


def ffn_layer(normed, after_mix, gain, up_proj, down_proj):
    rows, width = normed.shape
    units, planes = up_proj.shape[1] // 4, 4
    vmem = pl.BlockSpec(memory_space=pltpu.VMEM)
    hbm = pl.BlockSpec(memory_space=pl.ANY)
    dma = pltpu.SemaphoreType.DMA
    return pl.pallas_call(
        ffn_kernel,
        out_shape=jax.ShapeDtypeStruct((rows, width), BF16),
        in_specs=[vmem, vmem, vmem, hbm, hbm],
        out_specs=vmem,
        scratch_shapes=[
            pltpu.VMEM((width, units), BF16),
            pltpu.VMEM((units, width), BF16),
            pltpu.VMEM((8 * rows, width), BF16),
            pltpu.VMEM((8 * rows, units), BF16),
            pltpu.VMEM((8 * rows, width), BF16),
            pltpu.VMEM((4 * rows, width), BF16),
            pltpu.VMEM((2 * rows, width), BF16),
            pltpu.VMEM((2 * rows, width), BF16),
            pltpu.VMEM((rows, width), BF16),
            pltpu.VMEM((rows, width), BF16),
            pltpu.VMEM((rows, width), F32),
            dma((2,)),
            dma((2, 8)),
            dma((2, 8)),
            dma((2, 8)),
            dma((2, 8)),
            dma((7,)),
            dma((7,)),
            dma((3, 8)),
            dma((3, 8)),
        ],
        compiler_params=pltpu.CompilerParams(
            collective_id=0, has_side_effects=True, vmem_limit_bytes=60 << 20
        ),
        name="ffn_exchange",
    )(normed, after_mix, gain.reshape(1, -1), up_proj, down_proj)


def slice_body(
    queries,
    key_heads,
    value_heads,
    sink_logit,
    doc_ids,
    residual,
    out_proj,
    gain_mix,
    up_proj,
    down_proj,
    gain_ffn_in,
    gain_ffn_out,
):
    part = attention_part(
        ("sp",), queries, key_heads, value_heads, sink_logit, doc_ids, out_proj
    )
    share_rows = queries.shape[0] // lax.axis_size("tp")
    mixed = scatter_tp(part, own_first=False)
    own_residual = lax.dynamic_slice_in_dim(
        residual, lax.axis_index("tp") * share_rows, share_rows, 0
    )
    after_mix = (own_residual.astype(jnp.float32) + rms_scale(mixed, gain_mix)).astype(jnp.bfloat16)
    normed = rms_scale(after_mix.astype(jnp.float32), gain_ffn_in).astype(jnp.bfloat16)
    return ffn_layer(normed, after_mix, gain_ffn_out, up_proj, down_proj)


def solution(mesh):
    sp, tp = mesh.shape["sp"], mesh.shape["tp"]
    direct = sp == 16 and tp == 2
    if direct:
        body, fine, rows = slice_body, mesh, ("sp",)
    else:
        body, rows = general_body, SP
        fine = Mesh(mesh.devices.reshape(sp // 8, 2, 2, 2, tp), SP + ("tp",))
    return jax.shard_map(
        body,
        mesh=fine,
        in_specs=(
            P(rows, "tp"),
            P(rows, "tp"),
            P(rows, "tp"),
            P("tp"),
            P(),
            P(rows, None),
            P("tp", None),
            P(),
            P(rows, "tp"),
            P("tp", rows),
            P(),
            P(),
        ),
        out_specs=P(rows + ("tp",), None),
        check_vma=False,
    )
```

```python
import functools
import math

import jax
import jax.numpy as jnp
from jax import lax
from jax.experimental import pallas as pl
from jax.experimental.pallas import tpu as pltpu
from jax.sharding import Mesh, PartitionSpec as P

MESH = pl.DeviceIdType.MESH
BF16, F32 = jnp.bfloat16, jnp.float32

HD = 128
WINDOW = 128
SP = ("a", "b", "c", "d")
GRP = ("c", "d")
CROSS = ("a", "b")


def padded(shard, sides, width):
    for axis, dim in sides:
        devices, length = (lax.axis_size(axis), shard.shape[dim])
        up = [(i, (i + 1) % devices) for i in range(devices - 1)]
        down = [(j, i) for i, j in up]
        last = lax.slice_in_dim(shard, length - width, length, axis=dim)
        first = lax.slice_in_dim(shard, 0, width, axis=dim)
        before = lax.ppermute(last, axis, up)
        after = lax.ppermute(first, axis, down)
        shard = jnp.concatenate([before, shard, after], axis=dim)
    return shard


def rotate(field, places):
    half_dim = HD // 2
    inv_freq = 10000.0 ** (-jnp.arange(0, HD, 2, dtype=jnp.float32) / HD)
    angles = places[:, None, None] * inv_freq[None, None, :]
    cosine = jnp.cos(angles)
    sine = jnp.sin(angles)
    lower = field[..., :half_dim].astype(jnp.float32)
    upper = field[..., half_dim:].astype(jnp.float32)
    return jnp.concatenate(
        [lower * cosine - upper * sine, upper * cosine + lower * sine], axis=-1
    ).astype(jnp.bfloat16)


def banded(field, blocks):
    framed = field.reshape((blocks + 2, WINDOW) + field.shape[1:])
    return jnp.concatenate([framed[:-2], framed[1:-1], framed[2:]], axis=1)


def rms_scale(field, gain_vec):
    return field * lax.rsqrt(jnp.mean(field * field, axis=-1, keepdims=True) + 1e-06) * gain_vec


def swap_tp(rows):
    return lax.ppermute(rows, "tp", [(0, 1), (1, 0)])


def gather_tp(rows):
    if lax.axis_size("tp") == 2:
        return jnp.concatenate([rows, swap_tp(rows)], axis=0)
    return lax.all_gather(rows, "tp", axis=0, tiled=True)


def scatter_tp(partial_value, own_first=True):
    devices = lax.axis_size("tp")
    if devices != 2:
        return lax.psum_scatter(partial_value, "tp", scatter_dimension=0, tiled=True).astype(
            jnp.float32
        )
    share = partial_value.shape[0] // 2
    if own_first:
        own, other = partial_value[:share], partial_value[share:]
    else:
        me = lax.axis_index("tp")
        own = lax.dynamic_slice_in_dim(partial_value, me * share, share, 0)
        other = lax.dynamic_slice_in_dim(partial_value, (1 - me) * share, share, 0)
    return own.astype(jnp.float32) + swap_tp(other).astype(jnp.float32)


def to_peer(rows, k):
    if k == 0:
        return rows
    return lax.ppermute(rows, GRP, [(i, i ^ k) for i in range(4)])


def attention_part(sp, queries, key_heads, value_heads, sink_logit, doc_ids, out_proj):
    tok_count = queries.shape[0]
    blocks = tok_count // WINDOW
    q_local = queries.shape[1] // HD
    kv_local = key_heads.shape[1] // HD
    group_size = q_local // kv_local
    offset = lax.axis_index(sp) * tok_count
    places = (offset + jnp.arange(tok_count)).astype(jnp.float32)
    rotated_q = rotate(queries.reshape(tok_count, q_local, HD), places).reshape(
        blocks, WINDOW, kv_local, group_size, HD
    )
    rotated_k = rotate(key_heads.reshape(tok_count, kv_local, HD), places).reshape(
        tok_count, kv_local * HD
    )
    rimmed = padded(jnp.stack([rotated_k, value_heads]), ((sp, 1),), WINDOW)
    key_win = banded(rimmed[0].reshape(-1, kv_local, HD), blocks)
    val_win = banded(rimmed[1].reshape(-1, kv_local, HD), blocks)
    padded_docs = jnp.pad(doc_ids, (WINDOW, WINDOW), constant_values=-1)
    key_docs = banded(lax.dynamic_slice_in_dim(padded_docs, offset, tok_count + 2 * WINDOW), blocks)
    query_docs = lax.dynamic_slice_in_dim(doc_ids, offset, tok_count).reshape(blocks, WINDOW)
    q_index = jnp.arange(WINDOW)[:, None]
    k_index = jnp.arange(3 * WINDOW)[None, :]
    in_window = jnp.abs(k_index - WINDOW - q_index) <= WINDOW
    allowed = (in_window[None] & (query_docs[:, :, None] == key_docs[:, None, :]))[:, None, None]
    scores = jnp.einsum(
        "nqkgd,nskd->nkgqs", rotated_q, key_win, preferred_element_type=jnp.float32
    ) * HD ** (-0.5)
    masked = jnp.where(allowed, scores, -1e30)
    sink_col = sink_logit.reshape(kv_local, group_size)[None, :, :, None]
    top_score = jnp.maximum(jnp.max(masked, axis=-1), sink_col)
    exp_scores = jnp.where(allowed, jnp.exp(masked - top_score[..., None]), 0.0)
    denom_sum = jnp.sum(exp_scores, axis=-1) + jnp.exp(sink_col - top_score)
    probs = (exp_scores / denom_sum[..., None]).astype(jnp.bfloat16)
    attn = (
        jnp.einsum("nkgqs,nskd->nqkgd", probs, val_win, preferred_element_type=jnp.float32)
        .astype(jnp.bfloat16)
        .reshape(tok_count, q_local * HD)
    )
    part = jnp.dot(attn, out_proj, preferred_element_type=jnp.float32).astype(jnp.bfloat16)
    return part


def general_body(
    queries,
    key_heads,
    value_heads,
    sink_logit,
    doc_ids,
    residual,
    out_proj,
    gain_mix,
    up_proj,
    down_proj,
    gain_ffn_in,
    gain_ffn_out,
):
    up_quarter = lax.all_to_all(up_proj, GRP, split_axis=1, concat_axis=0, tiled=True)
    down_quarter = lax.all_to_all(down_proj, GRP, split_axis=0, concat_axis=1, tiled=True)
    queries, key_heads, up_quarter, down_quarter = lax.optimization_barrier(
        (queries, key_heads, up_quarter, down_quarter)
    )
    half_units = up_quarter.shape[1] // 2
    up_early = lax.all_gather(up_quarter[:, :half_units], CROSS, axis=0, tiled=True)
    up_late = lax.all_gather(up_quarter[:, half_units:], CROSS, axis=0, tiled=True)
    down_all = lax.all_gather(down_quarter, CROSS, axis=0, tiled=False)
    share_rows = queries.shape[0] // lax.axis_size("tp")
    part = attention_part(SP, queries, key_heads, value_heads, sink_logit, doc_ids, out_proj)
    part, up_early = lax.optimization_barrier((part, up_early))
    mixed = scatter_tp(part, own_first=False)
    own_residual = lax.dynamic_slice_in_dim(
        residual, lax.axis_index("tp") * share_rows, share_rows, 0
    )
    after_mix = (own_residual.astype(jnp.float32) + rms_scale(mixed, gain_mix)).astype(jnp.bfloat16)
    normed = rms_scale(after_mix.astype(jnp.float32), gain_ffn_in).astype(jnp.bfloat16)
    sizes = [lax.axis_size(a) for a in SP]
    order = [SP.index(a) for a in CROSS + GRP]
    width = normed.shape[1]
    strip = width // math.prod(sizes)
    normed = (
        normed.reshape(share_rows, *sizes, strip)
        .transpose(0, *[1 + o for o in order], 5)
        .reshape(share_rows, width)
    )
    blocks = [to_peer(normed, k) for k in range(4)]
    partials = []
    for k in (3, 2, 1, 0):
        rows = gather_tp(blocks[k])
        hidden = jnp.concatenate(
            [
                jnp.square(
                    jax.nn.relu(jnp.dot(rows, w, preferred_element_type=jnp.float32))
                ).astype(jnp.bfloat16)
                for w in (up_early, up_late)
            ],
            axis=1,
        )
        partial_value = jnp.concatenate(
            [
                jnp.dot(hidden, down_all[i], preferred_element_type=jnp.float32).astype(jnp.bfloat16)
                for i in range(down_all.shape[0])
            ],
            axis=1,
        )
        partials.append(to_peer(scatter_tp(partial_value).astype(jnp.bfloat16), k))
    ffn_out = sum(p.astype(jnp.float32) for p in partials)
    back = [order.index(i) for i in range(4)]
    ffn_out = (
        ffn_out.reshape(share_rows, *[sizes[o] for o in order], strip)
        .transpose(0, *[1 + b for b in back], 5)
        .reshape(share_rows, width)
    )
    return (after_mix.astype(jnp.float32) + rms_scale(ffn_out, gain_ffn_out)).astype(jnp.bfloat16)


def layer_kernel(
    sink_ref,
    cos_ref,
    sin_ref,
    query_docs_ref,
    key_docs_ref,
    gain_mix_ref,
    gain_in_ref,
    gain_out_ref,
    q_ref,
    k_ref,
    v_ref,
    residual_ref,
    proj_ref,
    up_ref,
    down_ref,
    out_ref,
    q_buf,
    k_buf,
    v_buf,
    attn,
    proj,
    resid,
    mix_own,
    mix_out,
    mix_in,
    after,
    w_up,
    w_down,
    tokens,
    hidden,
    part,
    peer,
    x_out,
    x_in,
    z_out,
    z_in,
    ffn,
    local_sem,
    load_sem,
    h_send,
    h_recv,
    m_send,
    m_recv,
    w_send,
    w_recv,
    y_send,
    y_recv,
    t_send,
    t_recv,
    p_send,
    p_recv,
    c_send,
    c_recv,
):
    me, core = lax.axis_index("sp"), lax.axis_index("tp")
    last = lax.axis_size("sp") - 1
    z, y, x = me // 4, lax.rem(me // 2, 2), lax.rem(me, 2)
    zl = lax.rem(z, 2)
    z1, z2, z3 = z + 1 - 2 * zl, lax.rem(z + 2, 4), 3 - z
    xo, yo = 1 - x, 1 - y
    positions = q_ref.shape[0]
    rows = positions // 2
    strip, units = up_ref.shape[0], up_ref.shape[1] // 4
    chunk = 2 * strip
    half = 4 * rows
    blocks = positions // WINDOW
    kv_heads = k_ref.shape[1] // HD
    group_size = q_ref.shape[1] // k_ref.shape[1]

    def place(zz, yy, xx):
        return zz * 4 + yy * 2 + xx

    def col(start, size):
        return pl.ds(pl.multiple_of(start, size), size)

    def slot(w, s):
        if w == 0:
            return w_up.at[col(s * strip, strip), :]
        return w_down.at[:, col(s * strip, strip)]

    def shard(w, zz, xx):
        q = lax.rem(zz, 2) * 2 + xx
        if w == 0:
            return up_ref.at[:, col(q * units, units)]
        return down_ref.at[col(q * units, units), :]

    def remote(src, dst, send, recv, dev, c):
        return pltpu.make_async_remote_copy(
            src_ref=src,
            dst_ref=dst,
            send_sem=send,
            recv_sem=recv,
            device_id=(dev, c),
            device_id_type=MESH,
        )

    direct = ((z, 1), (z1, 0), (z1, 1), (z3, 0), (z3, 1), (z2, 0), (z2, 1))

    def to_x(dx):
        return xo if dx else x

    def send_direct(w, k):
        zz, dx = direct[k]
        return remote(
            shard(w, zz, to_x(dx)),
            slot(w, me),
            w_send.at[w, k],
            w_recv.at[w, z * 2 + dx],
            place(zz, y, to_x(dx)),
            core,
        )

    def send_own_y(w):
        return remote(
            shard(w, z, x),
            slot(w, me),
            w_send.at[w, 7],
            y_recv.at[w, z * 2],
            place(z, yo, x),
            core,
        )

    def keep_own(w):
        return pltpu.make_async_copy(shard(w, z, x), slot(w, me), local_sem.at[w])

    def arrival(w, zz, dx):
        s = slot(w, place(zz, y, to_x(dx)))
        return remote(s, s, y_send.at[w, zz * 2 + dx], w_recv.at[w, zz * 2 + dx], me, core)

    def forward(w, zz, dx):
        s = slot(w, place(zz, y, to_x(dx)))
        return remote(
            s,
            s,
            y_send.at[w, zz * 2 + dx],
            y_recv.at[w, zz * 2 + dx],
            place(z, yo, x),
            core,
        )

    def y_arrival(w, zz, dx):
        s = slot(w, place(zz, yo, to_x(dx)))
        return remote(s, s, y_send.at[w, zz * 2 + dx], y_recv.at[w, zz * 2 + dx], me, core)

    def relay(w, zz, dx):
        with jax.named_scope(f"relay#w={w}"):
            arrival(w, zz, dx).wait_recv()
        forward(w, zz, dx).start()

    m_own, m_z = zl * 2 + x, (1 - zl) * 2 + x
    m_x, m_d = zl * 2 + xo, (1 - zl) * 2 + xo
    x_dev, z_dev, y_dev = place(z, y, xo), place(z1, y, x), place(z, yo, x)
    bit = rows // 2

    def token_bit(c, m, h):
        return tokens.at[col((m * 2 + c) * rows + h * bit, bit), :]

    sent = ((m_own, 0, z_dev), (m_own, 1, z_dev), (m_own, 0, x_dev), (m_own, 1, x_dev), (m_z, 0, x_dev), (m_x, 1, z_dev))
    got = ((m_z, 0), (m_z, 1), (m_x, 0), (m_x, 1), (m_d, 0), (m_d, 1))

    def token_copy(k):
        m, h, dev = sent[k]
        s = token_bit(core, m, h)
        return remote(s, s, t_send.at[k], t_recv.at[k], dev, core)

    def token_arrival(k):
        m, h = got[k]
        s = token_bit(core, m, h)
        return remote(s, s, t_send.at[k], t_recv.at[k], me, core)

    def peer_token(k):
        m, h = got[k] if k < 6 else (m_own, k - 6)
        s = token_bit(core, m, h)
        return remote(s, s, p_send.at[k], p_recv.at[k], me, 1 - core)

    def peer_arrival(k):
        m, h = got[k] if k < 6 else (m_own, k - 6)
        s = token_bit(1 - core, m, h)
        return remote(s, s, p_send.at[k], p_recv.at[k], me, 1 - core)

    def take_token(k):
        with jax.named_scope(f"token#k={k}"):
            token_arrival(k).wait_recv()
        peer_token(k).start()

    def halo(k, side):
        ref, buf = ((k_ref, k_buf), (v_ref, v_buf))[k]
        src = ref.at[positions - WINDOW :, :] if side else ref.at[:WINDOW, :]
        dst = buf.at[:WINDOW, :] if side else buf.at[positions + WINDOW :, :]
        sem = k * 2 + side
        return remote(src, dst, h_send.at[sem], h_recv.at[sem], me + (1 if side else -1), core)

    loads = (
        (k_ref, k_buf.at[WINDOW : positions + WINDOW, :]),
        (v_ref, v_buf.at[WINDOW : positions + WINDOW, :]),
        (q_ref, q_buf),
        (proj_ref, proj),
        (residual_ref.at[col(core * rows, rows), :], resid),
    )

    def load(i):
        return pltpu.make_async_copy(loads[i][0], loads[i][1], load_sem.at[i])

    barrier = pltpu.get_barrier_semaphore()
    friends = [(place(zz, y, to_x(dx)), core) for zz, dx in direct] + [(y_dev, core), (me, 1 - core)]
    for dev in friends:
        pl.semaphore_signal(barrier, inc=1, device_id=dev, device_id_type=MESH)
    beyond = me - 1 + 2 * x
    has_beyond = (beyond >= 0) & (beyond <= last)

    @pl.when(has_beyond)
    def _():
        pl.semaphore_signal(barrier, inc=1, device_id=(beyond, core), device_id_type=MESH)

    for i in range(len(loads)):
        load(i).start()
    for w in (0, 1):
        keep_own(w).start()

    @pl.when(me == 0)
    def _():
        k_buf[:WINDOW, :] = jnp.zeros((WINDOW, k_buf.shape[1]), BF16)
        v_buf[:WINDOW, :] = jnp.zeros((WINDOW, k_buf.shape[1]), BF16)

    @pl.when(me == last)
    def _():
        k_buf[positions + WINDOW :, :] = jnp.zeros((WINDOW, k_buf.shape[1]), BF16)
        v_buf[positions + WINDOW :, :] = jnp.zeros((WINDOW, k_buf.shape[1]), BF16)

    with jax.named_scope("entry"):
        pl.semaphore_wait(barrier, len(friends) + has_beyond.astype(jnp.int32))

    def near_halo(act):
        for k in (0, 1):
            pl.when(x == 0)(lambda: act(halo(k, 1)))
            pl.when(x == 1)(lambda: act(halo(k, 0)))

    def far_halo(act):
        for k in (0, 1):
            pl.when((x == 1) & has_beyond)(lambda: act(halo(k, 1)))
            pl.when((x == 0) & has_beyond)(lambda: act(halo(k, 0)))

    def near_halo_arrival(act):
        for k in (0, 1):
            pl.when(x == 1)(lambda: act(halo(k, 1)))
            pl.when(x == 0)(lambda: act(halo(k, 0)))

    def far_halo_arrival(act):
        for k in (0, 1):
            pl.when((x == 0) & has_beyond)(lambda: act(halo(k, 1)))
            pl.when((x == 1) & has_beyond)(lambda: act(halo(k, 0)))

    near_halo(lambda c: c.start())
    far_halo(lambda c: c.start())
    send_own_y(0).start()
    for k in (1, 3, 5):
        send_direct(0, k).start()

    def rotate_rows(buf, base, heads, shift):
        def step(b, carry):
            lines = col(base + b * WINDOW, WINDOW)
            turn = col(base + shift + b * WINDOW, WINDOW)
            cosine, sine = cos_ref[turn, :], sin_ref[turn, :]
            for h in range(heads):
                lanes = slice(h * HD, (h + 1) * HD)
                u = buf[lines, lanes].astype(F32)
                buf[lines, lanes] = (u * cosine + pltpu.roll(u, HD // 2, 1) * sine).astype(BF16)
            return carry

        return step

    with jax.named_scope("rotate"):
        load(0).wait()
        lax.fori_loop(0, blocks, rotate_rows(k_buf, WINDOW, kv_heads, 0), 0)
        load(2).wait()
        lax.fori_loop(0, blocks, rotate_rows(q_buf, 0, kv_heads * group_size, WINDOW), 0)
        load(1).wait()

    def attend(b):
        lines = col(b * WINDOW, WINDOW)
        window = pl.ds(pl.multiple_of(b * WINDOW, WINDOW), 3 * WINDOW)
        shape = (WINDOW, 3 * WINDOW)
        away = lax.broadcasted_iota(jnp.int32, shape, 1) - lax.broadcasted_iota(jnp.int32, shape, 0)
        same = query_docs_ref[lines, :] == key_docs_ref[:, window]
        allowed = (away >= 0) & (away <= 2 * WINDOW) & same
        bias = jnp.where(allowed, 0.0, -1e30)

        def step(h, carry):
            keys = k_buf[window, col(h * HD, HD)]
            values = v_buf[window, col(h * HD, HD)]
            for g in range(group_size):
                head = h * group_size + g
                sink = sink_ref[head]
                scores = lax.dot_general(
                    q_buf[lines, col(head * HD, HD)],
                    keys,
                    (((1,), (1,)), ((), ())),
                    preferred_element_type=F32,
                )
                scores = scores * HD ** (-0.5) + bias
                top = jnp.maximum(jnp.max(scores, axis=1, keepdims=True), sink)
                exps = jnp.exp(scores - top)
                total = jnp.sum(exps, axis=1, keepdims=True) + jnp.exp(sink - top)
                probs = (exps * (1.0 / total)).astype(BF16)
                attn[lines, col(head * HD, HD)] = jnp.dot(
                    probs, values, preferred_element_type=F32
                ).astype(BF16)
            return carry

        with jax.named_scope("attend"):
            lax.fori_loop(0, kv_heads, step, 0)

    attend(1)
    send_direct(0, 0).start()
    with jax.named_scope("halo_near"):
        near_halo_arrival(lambda c: c.wait_recv())
    rotate_rows(k_buf, (1 - x) * (positions + WINDOW), kv_heads, 0)(0, 0)
    attend((1 - x) * (blocks - 1))
    for k in (2, 4, 6):
        send_direct(0, k).start()
    with jax.named_scope("halo_far"):
        far_halo_arrival(lambda c: c.wait_recv())
    rotate_rows(k_buf, x * (positions + WINDOW), kv_heads, 0)(0, 0)
    attend(x * (blocks - 1))
    load(3).wait()

    def project(start, target):
        def step(n, carry):
            cols = col(n * chunk, chunk)
            target[:, cols] = jnp.dot(
                attn[col(start, rows), :], proj[:, cols], preferred_element_type=F32
            ).astype(BF16)
            return carry

        with jax.named_scope("project"):
            lax.fori_loop(0, proj.shape[1] // chunk, step, 0)

    project((1 - core) * rows, mix_out)
    mix_copy = remote(mix_out, mix_in, m_send, m_recv, me, 1 - core)
    mix_copy.start()
    relay(0, z, 1)
    project(core * rows, mix_own)
    relay(0, z1, 0)
    load(4).wait()
    mix_copy.wait_recv()

    def norm_rows(r, carry):
        lines = col(r * 16, 16)
        field = mix_own[lines, :].astype(F32) + mix_in[lines, :].astype(F32)
        scale = lax.rsqrt(jnp.mean(field * field, axis=-1, keepdims=True) + 1e-06)
        mixed = resid[lines, :].astype(F32) + field * scale * gain_mix_ref[...]
        after[lines, :] = mixed.astype(BF16)
        field = after[lines, :].astype(F32)
        scale = lax.rsqrt(jnp.mean(field * field, axis=-1, keepdims=True) + 1e-06)
        own = pl.ds(pl.multiple_of((m_own * 2 + core) * rows + r * 16, 16), 16)
        tokens[own, :] = (field * scale * gain_in_ref[...]).astype(BF16)
        return carry

    for h in (0, 1):
        with jax.named_scope("norm"):
            lax.fori_loop(h * bit // 16, (h + 1) * bit // 16, norm_rows, 0)
        token_copy(h).start()
        token_copy(2 + h).start()
        peer_token(6 + h).start()

    send_own_y(1).start()
    inner = (z == 1) | (z == 2)

    def send_middle(when):
        @pl.when(when)
        def _():
            for k in (3, 4):
                send_direct(1, k).start()

    send_middle(inner)
    relay(0, z1, 1)
    relay(0, z3, 0)
    relay(0, z3, 1)
    take_token(2)
    take_token(3)
    token_copy(5).start()
    relay(0, z2, 0)
    relay(0, z2, 1)
    take_token(0)
    token_copy(4).start()
    take_token(1)
    for k in (0, 1, 2):
        send_direct(1, k).start()
    send_middle(jnp.logical_not(inner))
    for k in (5, 6):
        send_direct(1, k).start()
    keep_own(0).wait()
    with jax.named_scope("up_y"):
        for zz in (z, z1, z3, z2):
            for dx in (0, 1):
                y_arrival(0, zz, dx).wait_recv()

    def up_rows(m):
        def step(n, carry):
            lines = col(m * 2 * rows, 2 * rows)
            cols = col(n * chunk, chunk)
            acts = jnp.dot(tokens[lines, :], w_up[:, cols], preferred_element_type=F32)
            acts = jnp.maximum(acts, 0.0)
            hidden[lines, cols] = (acts * acts).astype(BF16)
            return carry

        with jax.named_scope("up_mm"):
            lax.fori_loop(0, units // chunk, step, 0)

    def peer_pair(k):
        with jax.named_scope(f"peer#k={k}"):
            peer_arrival(k).wait_recv()
            peer_arrival(k + 1).wait_recv()

    peer_pair(6)
    up_rows(m_own)
    peer_pair(2)
    up_rows(m_x)
    peer_pair(0)
    up_rows(m_z)
    take_token(5)
    take_token(4)
    relay(1, z, 1)
    relay(1, z1, 0)
    relay(1, z1, 1)
    peer_pair(4)
    up_rows(m_d)
    keep_own(1).wait()

    zh = z // 2
    near, far = (zh * 2, zh * 2 + 1), (2 - zh * 2, 3 - zh * 2)
    order = [(near[0], y), (near[1], y), (near[0], yo), (near[1], yo)]
    order += [(far[0], y), (far[1], y), (far[0], yo), (far[1], yo)]

    def columns(i):
        zz, yy = order[i]
        return col((zz * 2 + yy) * chunk, chunk)

    def stage_a(i):
        zz, yy = order[i]
        if i >= 4 and i % 4 < 2:
            for dx in (0, 1):
                relay(1, zz, dx)
        elif i % 4 >= 2:
            with jax.named_scope("down_y"):
                for dx in (0, 1):
                    y_arrival(1, zz, dx).wait_recv()
        cols = columns(i)

        def step(m, carry):
            both = jnp.dot(
                hidden[col(m * 2 * rows, 2 * rows), :], w_down[:, cols], preferred_element_type=F32
            ).astype(BF16)
            part[col(m * rows, rows), cols] = both[:rows]
            part[col((4 + m) * rows, rows), cols] = both[rows:]
            return carry

        with jax.named_scope("down_mm"):
            lax.fori_loop(0, 4, step, 0)
        peer_copy(i).start()

    def peer_copy(i):
        cols = columns(i)
        return remote(
            part.at[col((1 - core) * half, half), cols],
            peer.at[:, cols],
            c_send.at[0, i],
            c_recv.at[0, i],
            me,
            1 - core,
        )

    def chip_sum(m, cols):
        own = part[col((core * 4 + m) * rows, rows), cols].astype(F32)
        return own + peer[col(m * rows, rows), cols].astype(F32)

    def x_copy(i):
        cols = columns(i)
        return remote(x_out.at[:, cols], x_in.at[:, cols], c_send.at[1, i], c_recv.at[1, i], x_dev, core)

    def z_copy(i):
        cols = columns(i)
        return remote(z_out.at[:, cols], z_in.at[:, cols], c_send.at[2, i], c_recv.at[2, i], z_dev, core)

    def stage_b(i):
        cols = columns(i)
        with jax.named_scope("part_peer"):
            peer_copy(i).wait_recv()
        x_out[:rows, cols] = chip_sum(m_x, cols).astype(BF16)
        x_out[rows:, cols] = chip_sum(m_d, cols).astype(BF16)
        x_copy(i).start()

    def stage_c(i):
        cols = columns(i)
        with jax.named_scope("part_x"):
            x_copy(i).wait_recv()
        z_out[:, cols] = (chip_sum(m_z, cols) + x_in[rows:, cols].astype(F32)).astype(BF16)
        z_copy(i).start()

    def stage_d(i):
        cols = columns(i)
        with jax.named_scope("part_z"):
            z_copy(i).wait_recv()
        ffn[:, cols] = (
            chip_sum(m_own, cols) + x_in[:rows, cols].astype(F32) + z_in[:, cols].astype(F32)
        )

    for i in range(8 + 3):
        if i < 8:
            stage_a(i)
        if 0 <= i - 1 < 8:
            stage_c(i - 1)
        if 0 <= i - 2 < 8:
            stage_d(i - 2)
        if i < 8:
            stage_b(i)

    def finish(r, carry):
        lines = col(r * 16, 16)
        field = ffn[lines, :]
        scale = lax.rsqrt(jnp.mean(field * field, axis=-1, keepdims=True) + 1e-06)
        out_ref[lines, :] = (
            after[lines, :].astype(F32) + field * scale * gain_out_ref[...]
        ).astype(BF16)
        return carry

    with jax.named_scope("finish"):
        lax.fori_loop(0, rows // 16, finish, 0)

    near_halo(lambda c: c.wait_send())
    far_halo(lambda c: c.wait_send())
    mix_copy.wait_send()
    for w in (0, 1):
        send_own_y(w).wait_send()
        for k in range(7):
            send_direct(w, k).wait_send()
            zz, dx = direct[k]
            forward(w, zz, dx).wait_send()
    for k in range(6):
        token_copy(k).wait_send()
    for k in range(8):
        peer_token(k).wait_send()
    for i in range(8):
        peer_copy(i).wait_send()
        x_copy(i).wait_send()
        z_copy(i).wait_send()


def slice_body(
    queries,
    key_heads,
    value_heads,
    sink_logit,
    doc_ids,
    residual,
    out_proj,
    gain_mix,
    up_proj,
    down_proj,
    gain_ffn_in,
    gain_ffn_out,
):
    positions, width = residual.shape
    rows = positions // lax.axis_size("tp")
    units = up_proj.shape[1] // 4
    heads, kv = queries.shape[1], key_heads.shape[1]
    offset = lax.axis_index("sp") * positions
    framed = positions + 2 * WINDOW
    places = (offset - WINDOW + jnp.arange(framed)).astype(F32)
    inv_freq = 10000.0 ** (-jnp.arange(0, HD, 2, dtype=F32) / HD)
    angles = places[:, None] * jnp.concatenate([inv_freq, inv_freq])[None, :]
    cosine = jnp.cos(angles)
    sine = jnp.sin(angles) * jnp.where(jnp.arange(HD) < HD // 2, -1.0, 1.0)[None, :]
    padded_docs = jnp.pad(doc_ids, (WINDOW, WINDOW), constant_values=-1)
    key_docs = lax.dynamic_slice_in_dim(padded_docs, offset, framed).reshape(1, -1)
    query_docs = lax.dynamic_slice_in_dim(doc_ids, offset, positions).reshape(-1, 1)
    vmem = pl.BlockSpec(memory_space=pltpu.VMEM)
    hbm = pl.BlockSpec(memory_space=pl.ANY)
    dma = pltpu.SemaphoreType.DMA
    shapes = [
        ((positions, heads), BF16),
        ((framed, kv), BF16),
        ((framed, kv), BF16),
        ((positions, heads), BF16),
        ((heads, width), BF16),
        ((rows, width), BF16),
        ((rows, width), BF16),
        ((rows, width), BF16),
        ((rows, width), BF16),
        ((rows, width), BF16),
        ((width, units), BF16),
        ((units, width), BF16),
        ((8 * rows, width), BF16),
        ((8 * rows, units), BF16),
        ((8 * rows, width), BF16),
        ((4 * rows, width), BF16),
        ((2 * rows, width), BF16),
        ((2 * rows, width), BF16),
        ((rows, width), BF16),
        ((rows, width), BF16),
        ((rows, width), F32),
    ]
    sems = [(2,), (5,), (4,), (4,), None, None] + [(2, 8)] * 4 + [(6,), (6,), (8,), (8,), (3, 8), (3, 8)]
    return pl.pallas_call(
        layer_kernel,
        out_shape=jax.ShapeDtypeStruct((rows, width), BF16),
        in_specs=[pl.BlockSpec(memory_space=pltpu.SMEM)] + [vmem] * 7 + [hbm] * 7,
        out_specs=vmem,
        scratch_shapes=[pltpu.VMEM(s, t) for s, t in shapes]
        + [dma if s is None else dma(s) for s in sems],
        compiler_params=pltpu.CompilerParams(
            collective_id=0, has_side_effects=True, vmem_limit_bytes=62 << 20
        ),
        name="layer",
    )(
        sink_logit,
        cosine,
        sine,
        query_docs,
        key_docs,
        gain_mix.reshape(1, -1),
        gain_ffn_in.reshape(1, -1),
        gain_ffn_out.reshape(1, -1),
        queries,
        key_heads,
        value_heads,
        residual,
        out_proj,
        up_proj,
        down_proj,
    )


def solution(mesh):
    sp, tp = mesh.shape["sp"], mesh.shape["tp"]
    direct = sp == 16 and tp == 2
    if direct:
        body, fine, rows = slice_body, mesh, ("sp",)
    else:
        body, rows = general_body, SP
        fine = Mesh(mesh.devices.reshape(sp // 8, 2, 2, 2, tp), SP + ("tp",))
    return jax.shard_map(
        body,
        mesh=fine,
        in_specs=(
            P(rows, "tp"),
            P(rows, "tp"),
            P(rows, "tp"),
            P("tp"),
            P(),
            P(rows, None),
            P("tp", None),
            P(),
            P(rows, "tp"),
            P("tp", rows),
            P(),
            P(),
        ),
        out_specs=P(rows + ("tp",), None),
        check_vma=False,
    )
```

```python
import functools
import math

import jax
import jax.numpy as jnp
from jax import lax
from jax.experimental import pallas as pl
from jax.experimental.pallas import tpu as pltpu
from jax.sharding import Mesh, PartitionSpec as P

MESH = pl.DeviceIdType.MESH
BF16, F32 = jnp.bfloat16, jnp.float32

HD = 128
WINDOW = 128
SP = ("a", "b", "c", "d")
GRP = ("c", "d")
CROSS = ("a", "b")


def padded(shard, sides, width):
    for axis, dim in sides:
        devices, length = (lax.axis_size(axis), shard.shape[dim])
        up = [(i, (i + 1) % devices) for i in range(devices - 1)]
        down = [(j, i) for i, j in up]
        last = lax.slice_in_dim(shard, length - width, length, axis=dim)
        first = lax.slice_in_dim(shard, 0, width, axis=dim)
        before = lax.ppermute(last, axis, up)
        after = lax.ppermute(first, axis, down)
        shard = jnp.concatenate([before, shard, after], axis=dim)
    return shard


def rotate(field, places):
    half_dim = HD // 2
    inv_freq = 10000.0 ** (-jnp.arange(0, HD, 2, dtype=jnp.float32) / HD)
    angles = places[:, None, None] * inv_freq[None, None, :]
    cosine = jnp.cos(angles)
    sine = jnp.sin(angles)
    lower = field[..., :half_dim].astype(jnp.float32)
    upper = field[..., half_dim:].astype(jnp.float32)
    return jnp.concatenate(
        [lower * cosine - upper * sine, upper * cosine + lower * sine], axis=-1
    ).astype(jnp.bfloat16)


def banded(field, blocks):
    framed = field.reshape((blocks + 2, WINDOW) + field.shape[1:])
    return jnp.concatenate([framed[:-2], framed[1:-1], framed[2:]], axis=1)


def rms_scale(field, gain_vec):
    return field * lax.rsqrt(jnp.mean(field * field, axis=-1, keepdims=True) + 1e-06) * gain_vec


def swap_tp(rows):
    return lax.ppermute(rows, "tp", [(0, 1), (1, 0)])


def gather_tp(rows):
    if lax.axis_size("tp") == 2:
        return jnp.concatenate([rows, swap_tp(rows)], axis=0)
    return lax.all_gather(rows, "tp", axis=0, tiled=True)


def scatter_tp(partial_value, own_first=True):
    devices = lax.axis_size("tp")
    if devices != 2:
        return lax.psum_scatter(partial_value, "tp", scatter_dimension=0, tiled=True).astype(
            jnp.float32
        )
    share = partial_value.shape[0] // 2
    if own_first:
        own, other = partial_value[:share], partial_value[share:]
    else:
        me = lax.axis_index("tp")
        own = lax.dynamic_slice_in_dim(partial_value, me * share, share, 0)
        other = lax.dynamic_slice_in_dim(partial_value, (1 - me) * share, share, 0)
    return own.astype(jnp.float32) + swap_tp(other).astype(jnp.float32)


def to_peer(rows, k):
    if k == 0:
        return rows
    return lax.ppermute(rows, GRP, [(i, i ^ k) for i in range(4)])


def attention_part(sp, queries, key_heads, value_heads, sink_logit, doc_ids, out_proj):
    tok_count = queries.shape[0]
    blocks = tok_count // WINDOW
    q_local = queries.shape[1] // HD
    kv_local = key_heads.shape[1] // HD
    group_size = q_local // kv_local
    offset = lax.axis_index(sp) * tok_count
    places = (offset + jnp.arange(tok_count)).astype(jnp.float32)
    rotated_q = rotate(queries.reshape(tok_count, q_local, HD), places).reshape(
        blocks, WINDOW, kv_local, group_size, HD
    )
    rotated_k = rotate(key_heads.reshape(tok_count, kv_local, HD), places).reshape(
        tok_count, kv_local * HD
    )
    rimmed = padded(jnp.stack([rotated_k, value_heads]), ((sp, 1),), WINDOW)
    key_win = banded(rimmed[0].reshape(-1, kv_local, HD), blocks)
    val_win = banded(rimmed[1].reshape(-1, kv_local, HD), blocks)
    padded_docs = jnp.pad(doc_ids, (WINDOW, WINDOW), constant_values=-1)
    key_docs = banded(lax.dynamic_slice_in_dim(padded_docs, offset, tok_count + 2 * WINDOW), blocks)
    query_docs = lax.dynamic_slice_in_dim(doc_ids, offset, tok_count).reshape(blocks, WINDOW)
    q_index = jnp.arange(WINDOW)[:, None]
    k_index = jnp.arange(3 * WINDOW)[None, :]
    in_window = jnp.abs(k_index - WINDOW - q_index) <= WINDOW
    allowed = (in_window[None] & (query_docs[:, :, None] == key_docs[:, None, :]))[:, None, None]
    scores = jnp.einsum(
        "nqkgd,nskd->nkgqs", rotated_q, key_win, preferred_element_type=jnp.float32
    ) * HD ** (-0.5)
    masked = jnp.where(allowed, scores, -1e30)
    sink_col = sink_logit.reshape(kv_local, group_size)[None, :, :, None]
    top_score = jnp.maximum(jnp.max(masked, axis=-1), sink_col)
    exp_scores = jnp.where(allowed, jnp.exp(masked - top_score[..., None]), 0.0)
    denom_sum = jnp.sum(exp_scores, axis=-1) + jnp.exp(sink_col - top_score)
    probs = (exp_scores / denom_sum[..., None]).astype(jnp.bfloat16)
    attn = (
        jnp.einsum("nkgqs,nskd->nqkgd", probs, val_win, preferred_element_type=jnp.float32)
        .astype(jnp.bfloat16)
        .reshape(tok_count, q_local * HD)
    )
    part = jnp.dot(attn, out_proj, preferred_element_type=jnp.float32).astype(jnp.bfloat16)
    return part


def general_body(
    queries,
    key_heads,
    value_heads,
    sink_logit,
    doc_ids,
    residual,
    out_proj,
    gain_mix,
    up_proj,
    down_proj,
    gain_ffn_in,
    gain_ffn_out,
):
    up_quarter = lax.all_to_all(up_proj, GRP, split_axis=1, concat_axis=0, tiled=True)
    down_quarter = lax.all_to_all(down_proj, GRP, split_axis=0, concat_axis=1, tiled=True)
    queries, key_heads, up_quarter, down_quarter = lax.optimization_barrier(
        (queries, key_heads, up_quarter, down_quarter)
    )
    half_units = up_quarter.shape[1] // 2
    up_early = lax.all_gather(up_quarter[:, :half_units], CROSS, axis=0, tiled=True)
    up_late = lax.all_gather(up_quarter[:, half_units:], CROSS, axis=0, tiled=True)
    down_all = lax.all_gather(down_quarter, CROSS, axis=0, tiled=False)
    share_rows = queries.shape[0] // lax.axis_size("tp")
    part = attention_part(SP, queries, key_heads, value_heads, sink_logit, doc_ids, out_proj)
    part, up_early = lax.optimization_barrier((part, up_early))
    mixed = scatter_tp(part, own_first=False)
    own_residual = lax.dynamic_slice_in_dim(
        residual, lax.axis_index("tp") * share_rows, share_rows, 0
    )
    after_mix = (own_residual.astype(jnp.float32) + rms_scale(mixed, gain_mix)).astype(jnp.bfloat16)
    normed = rms_scale(after_mix.astype(jnp.float32), gain_ffn_in).astype(jnp.bfloat16)
    sizes = [lax.axis_size(a) for a in SP]
    order = [SP.index(a) for a in CROSS + GRP]
    width = normed.shape[1]
    strip = width // math.prod(sizes)
    normed = (
        normed.reshape(share_rows, *sizes, strip)
        .transpose(0, *[1 + o for o in order], 5)
        .reshape(share_rows, width)
    )
    blocks = [to_peer(normed, k) for k in range(4)]
    partials = []
    for k in (3, 2, 1, 0):
        rows = gather_tp(blocks[k])
        hidden = jnp.concatenate(
            [
                jnp.square(
                    jax.nn.relu(jnp.dot(rows, w, preferred_element_type=jnp.float32))
                ).astype(jnp.bfloat16)
                for w in (up_early, up_late)
            ],
            axis=1,
        )
        partial_value = jnp.concatenate(
            [
                jnp.dot(hidden, down_all[i], preferred_element_type=jnp.float32).astype(jnp.bfloat16)
                for i in range(down_all.shape[0])
            ],
            axis=1,
        )
        partials.append(to_peer(scatter_tp(partial_value).astype(jnp.bfloat16), k))
    ffn_out = sum(p.astype(jnp.float32) for p in partials)
    back = [order.index(i) for i in range(4)]
    ffn_out = (
        ffn_out.reshape(share_rows, *[sizes[o] for o in order], strip)
        .transpose(0, *[1 + b for b in back], 5)
        .reshape(share_rows, width)
    )
    return (after_mix.astype(jnp.float32) + rms_scale(ffn_out, gain_ffn_out)).astype(jnp.bfloat16)


def layer_kernel(
    sink_ref,
    freq_ref,
    docs_ref,
    gain_mix_ref,
    gain_in_ref,
    gain_out_ref,
    q_ref,
    k_ref,
    v_ref,
    residual_ref,
    proj_ref,
    up_ref,
    down_ref,
    out_ref,
    cos_ref,
    sin_ref,
    q_buf,
    k_buf,
    v_buf,
    attn,
    proj,
    resid,
    mix_own,
    mix_out,
    mix_in,
    after,
    w_up,
    w_down,
    spare_up,
    spare_down,
    tokens,
    hidden,
    part,
    peer,
    a_out,
    a_in,
    b_out,
    b_in,
    ffn,
    local_sem,
    load_sem,
    h_send,
    h_recv,
    m_send,
    m_recv,
    a_send,
    s_recv,
    w_send,
    w_recv,
    y_send,
    y_recv,
    t_send,
    t_recv,
    p_send,
    p_recv,
    c_send,
    c_recv,
):
    me, core = lax.axis_index("sp"), lax.axis_index("tp")
    last = lax.axis_size("sp") - 1
    z, y, x = me // 4, lax.rem(me // 2, 2), lax.rem(me, 2)
    zl = lax.rem(z, 2)
    z1, z2, z3 = z + 1 - 2 * zl, lax.rem(z + 2, 4), 3 - z
    xo, yo = 1 - x, 1 - y
    positions = q_ref.shape[0]
    rows = positions // 2
    strip, units = up_ref.shape[0], up_ref.shape[1] // 4
    chunk = 2 * strip
    half = 4 * rows
    blocks = positions // WINDOW
    kv_heads = k_ref.shape[1] // HD
    group_size = q_ref.shape[1] // k_ref.shape[1]

    def place(zz, yy, xx):
        return zz * 4 + yy * 2 + xx

    def col(start, size):
        return pl.ds(pl.multiple_of(start, size), size)

    x_dev, z_dev, y_dev = place(z, y, xo), place(z1, y, x), place(z, yo, x)

    def slot(w, s):
        if w == 0:
            return w_up.at[col(s * strip, strip), :]
        return w_down.at[s]

    def shard(w, zz, xx):
        q = lax.rem(zz, 2) * 2 + xx
        if w == 0:
            return up_ref.at[:, col(q * units, units)]
        return down_ref.at[col(q * units, units), :]

    def remote(src, dst, send, recv, dev, c):
        return pltpu.make_async_remote_copy(
            src_ref=src,
            dst_ref=dst,
            send_sem=send,
            recv_sem=recv,
            device_id=(dev, c),
            device_id_type=MESH,
        )

    def to_x(dx):
        return xo if dx else x

    def spare(w):
        return (spare_up, spare_down)[w]

    def x_send(w, k):
        return remote(
            shard(w, z1 if k else z, xo),
            spare(w) if k else slot(w, me),
            a_send.at[w, k],
            s_recv.at[w] if k else w_recv.at[w, z * 2 + 1],
            x_dev,
            core,
        )

    columns_z = (z1, z3, z2)

    def z_own(w, k):
        zz = columns_z[k]
        return remote(
            shard(w, zz, x),
            slot(w, me),
            w_send.at[w, k],
            w_recv.at[w, z * 2],
            place(zz, y, x),
            core,
        )

    def z_pass(w, k):
        zz = columns_z[k]
        return remote(
            slot(w, x_dev) if k == 2 else spare(w),
            slot(w, x_dev),
            w_send.at[w, 3 + k],
            w_recv.at[w, z * 2 + 1],
            place(zz, y, x),
            core,
        )

    def spare_arrival(w):
        with jax.named_scope(f"spare#w={w}"):
            remote(spare(w), spare(w), a_send.at[w, 1], s_recv.at[w], me, core).wait_recv()

    def send_own_y(w):
        return remote(
            shard(w, z, x),
            slot(w, me),
            w_send.at[w, 6],
            y_recv.at[w, z * 2],
            place(z, yo, x),
            core,
        )

    def keep_own(w):
        return pltpu.make_async_copy(shard(w, z, x), slot(w, me), local_sem.at[w])

    def arrival(w, zz, dx):
        s = slot(w, place(zz, y, to_x(dx)))
        return remote(s, s, y_send.at[w, zz * 2 + dx], w_recv.at[w, zz * 2 + dx], me, core)

    def forward(w, zz, dx):
        s = slot(w, place(zz, y, to_x(dx)))
        return remote(
            s,
            s,
            y_send.at[w, zz * 2 + dx],
            y_recv.at[w, zz * 2 + dx],
            place(z, yo, x),
            core,
        )

    def y_arrival(w, zz, dx):
        s = slot(w, place(zz, yo, to_x(dx)))
        return remote(s, s, y_send.at[w, zz * 2 + dx], y_recv.at[w, zz * 2 + dx], me, core)

    def relay(w, zz, dx):
        with jax.named_scope(f"relay#w={w}"):
            arrival(w, zz, dx).wait_recv()
        forward(w, zz, dx).start()

    m_own, m_z = zl * 2 + x, (1 - zl) * 2 + x
    m_x, m_d = zl * 2 + xo, (1 - zl) * 2 + xo
    bit = rows // 2

    def token_bit(c, m, h):
        return tokens.at[col((m * 2 + c) * rows + h * bit, bit), :]

    sent = ((m_own, 0, z_dev), (m_own, 1, z_dev), (m_own, 0, x_dev), (m_own, 1, x_dev), (m_z, 0, x_dev), (m_z, 1, x_dev))
    got = ((m_z, 0), (m_z, 1), (m_x, 0), (m_x, 1), (m_d, 0), (m_d, 1))

    def token_copy(k):
        m, h, dev = sent[k]
        s = token_bit(core, m, h)
        return remote(s, s, t_send.at[k], t_recv.at[k], dev, core)

    def token_arrival(k):
        m, h = got[k]
        s = token_bit(core, m, h)
        return remote(s, s, t_send.at[k], t_recv.at[k], me, core)

    def peer_token(k):
        m, h = got[k] if k < 6 else (m_own, k - 6)
        s = token_bit(core, m, h)
        return remote(s, s, p_send.at[k], p_recv.at[k], me, 1 - core)

    def peer_arrival(k):
        m, h = got[k] if k < 6 else (m_own, k - 6)
        s = token_bit(1 - core, m, h)
        return remote(s, s, p_send.at[k], p_recv.at[k], me, 1 - core)

    def take_token(k):
        with jax.named_scope(f"token#k={k}"):
            token_arrival(k).wait_recv()
        peer_token(k).start()

    def halo(k, side):
        ref, buf = ((k_ref, k_buf), (v_ref, v_buf))[k]
        src = ref.at[positions - WINDOW :, :] if side else ref.at[:WINDOW, :]
        dst = buf.at[:WINDOW, :] if side else buf.at[positions + WINDOW :, :]
        sem = k * 2 + side
        return remote(src, dst, h_send.at[sem], h_recv.at[sem], me + (1 if side else -1), core)

    loads = (
        (k_ref, k_buf.at[WINDOW : positions + WINDOW, :]),
        (v_ref, v_buf.at[WINDOW : positions + WINDOW, :]),
        (q_ref, q_buf),
        (proj_ref, proj),
        (residual_ref.at[col(core * rows, rows), :], resid),
    )

    def load(i):
        return pltpu.make_async_copy(loads[i][0], loads[i][1], load_sem.at[i])

    barrier = pltpu.get_barrier_semaphore()
    friends = [(place(zz, y, x), core) for zz in columns_z] + [(x_dev, core), (y_dev, core), (me, 1 - core)]
    for dev in friends:
        pl.semaphore_signal(barrier, inc=1, device_id=dev, device_id_type=MESH)
    beyond = me - 1 + 2 * x
    has_beyond = (beyond >= 0) & (beyond <= last)

    @pl.when(has_beyond)
    def _():
        pl.semaphore_signal(barrier, inc=1, device_id=(beyond, core), device_id_type=MESH)

    for i in range(len(loads)):
        load(i).start()
    for w in (0, 1):
        keep_own(w).start()

    @pl.when(me == 0)
    def _():
        k_buf[:WINDOW, :] = jnp.zeros((WINDOW, k_buf.shape[1]), BF16)
        v_buf[:WINDOW, :] = jnp.zeros((WINDOW, k_buf.shape[1]), BF16)

    @pl.when(me == last)
    def _():
        k_buf[positions + WINDOW :, :] = jnp.zeros((WINDOW, k_buf.shape[1]), BF16)
        v_buf[positions + WINDOW :, :] = jnp.zeros((WINDOW, k_buf.shape[1]), BF16)

    def turn(b, carry):
        shape = (WINDOW, HD)
        at = (me * blocks + b - 1) * WINDOW + lax.broadcasted_iota(jnp.int32, shape, 0)
        angles = at.astype(F32) * freq_ref[...]
        lower = lax.broadcasted_iota(jnp.int32, shape, 1) < HD // 2
        lines = col(b * WINDOW, WINDOW)
        cos_ref[lines, :] = jnp.cos(angles)
        sine = jnp.sin(angles)
        sin_ref[lines, :] = jnp.where(lower, -sine, sine)
        return carry

    with jax.named_scope("angles"):
        lax.fori_loop(0, blocks + 2, turn, 0)
    with jax.named_scope("entry"):
        pl.semaphore_wait(barrier, len(friends) + has_beyond.astype(jnp.int32))

    def near_halo(act):
        for k in (0, 1):
            pl.when(x == 0)(lambda: act(halo(k, 1)))
            pl.when(x == 1)(lambda: act(halo(k, 0)))

    def far_halo(act):
        for k in (0, 1):
            pl.when((x == 1) & has_beyond)(lambda: act(halo(k, 1)))
            pl.when((x == 0) & has_beyond)(lambda: act(halo(k, 0)))

    def near_halo_arrival(act):
        for k in (0, 1):
            pl.when(x == 1)(lambda: act(halo(k, 1)))
            pl.when(x == 0)(lambda: act(halo(k, 0)))

    def far_halo_arrival(act):
        for k in (0, 1):
            pl.when((x == 0) & has_beyond)(lambda: act(halo(k, 1)))
            pl.when((x == 1) & has_beyond)(lambda: act(halo(k, 0)))

    near_halo(lambda c: c.start())
    x_send(0, 0).start()
    far_halo(lambda c: c.start())
    x_send(0, 1).start()
    send_own_y(0).start()
    for k in range(3):
        z_own(0, k).start()

    def rotate_rows(buf, base, heads, shift):
        def step(b, carry):
            lines = col(base + b * WINDOW, WINDOW)
            turn = col(base + shift + b * WINDOW, WINDOW)
            cosine, sine = cos_ref[turn, :], sin_ref[turn, :]
            for h in range(heads):
                lanes = slice(h * HD, (h + 1) * HD)
                u = buf[lines, lanes].astype(F32)
                buf[lines, lanes] = (u * cosine + pltpu.roll(u, HD // 2, 1) * sine).astype(BF16)
            return carry

        return step

    with jax.named_scope("rotate"):
        load(0).wait()
        lax.fori_loop(0, blocks, rotate_rows(k_buf, WINDOW, kv_heads, 0), 0)
        load(2).wait()
        lax.fori_loop(0, blocks, rotate_rows(q_buf, 0, kv_heads * group_size, WINDOW), 0)
        load(1).wait()

    def attend(b):
        lines = col(b * WINDOW, WINDOW)
        window = pl.ds(pl.multiple_of(b * WINDOW, WINDOW), 3 * WINDOW)
        shape = (WINDOW, WINDOW)
        away = lax.broadcasted_iota(jnp.int32, shape, 1) - lax.broadcasted_iota(jnp.int32, shape, 0)

        def docs(j):
            at = me * blocks + b + j - 1
            inside = (at >= 0) & (at <= (last + 1) * blocks - 1)
            row = docs_ref[pl.ds(jnp.clip(at, 0, (last + 1) * blocks - 1), 1), :]
            return jnp.broadcast_to(jnp.where(inside, row, -1).astype(F32), shape)

        own_docs = jnp.transpose(docs(1))
        limits = (away >= 0, None, away <= 0)
        bias = []
        for j in range(3):
            same = own_docs == docs(j)
            allowed = same if limits[j] is None else limits[j] & same
            bias.append(jnp.where(allowed, 0.0, -1e30))
        bias = jnp.concatenate(bias, axis=1)

        def step(h, carry):
            keys = k_buf[window, col(h * HD, HD)]
            values = v_buf[window, col(h * HD, HD)]
            for g in range(group_size):
                head = h * group_size + g
                sink = sink_ref[head]
                scores = lax.dot_general(
                    q_buf[lines, col(head * HD, HD)],
                    keys,
                    (((1,), (1,)), ((), ())),
                    preferred_element_type=F32,
                )
                scores = scores * HD ** (-0.5) + bias
                top = jnp.maximum(jnp.max(scores, axis=1, keepdims=True), sink)
                exps = jnp.exp(scores - top)
                total = jnp.sum(exps, axis=1, keepdims=True) + jnp.exp(sink - top)
                probs = (exps * (1.0 / total)).astype(BF16)
                attn[lines, col(head * HD, HD)] = jnp.dot(
                    probs, values, preferred_element_type=F32
                ).astype(BF16)
            return carry

        with jax.named_scope("attend"):
            lax.fori_loop(0, kv_heads, step, 0)

    attend(1)
    with jax.named_scope("halo_near"):
        near_halo_arrival(lambda c: c.wait_recv())
    rotate_rows(k_buf, (1 - x) * (positions + WINDOW), kv_heads, 0)(0, 0)
    attend((1 - x) * (blocks - 1))
    relay(0, z1, 0)
    with jax.named_scope("halo_far"):
        far_halo_arrival(lambda c: c.wait_recv())
    rotate_rows(k_buf, x * (positions + WINDOW), kv_heads, 0)(0, 0)
    attend(x * (blocks - 1))
    relay(0, z, 1)
    z_pass(0, 2).start()
    load(3).wait()

    def project(start, target):
        def step(n, carry):
            cols = col(n * chunk, chunk)
            target[:, cols] = jnp.dot(
                attn[col(start, rows), :], proj[:, cols], preferred_element_type=F32
            ).astype(BF16)
            return carry

        with jax.named_scope("project"):
            lax.fori_loop(0, proj.shape[1] // chunk, step, 0)

    project((1 - core) * rows, mix_out)
    mix_copy = remote(mix_out, mix_in, m_send, m_recv, me, 1 - core)
    mix_copy.start()
    spare_arrival(0)
    for k in (0, 1):
        z_pass(0, k).start()
    for k in (1, 0):
        x_send(1, k).start()
    project(core * rows, mix_own)
    load(4).wait()
    mix_copy.wait_recv()

    def norm_rows(r, carry):
        lines = col(r * 16, 16)
        field = mix_own[lines, :].astype(F32) + mix_in[lines, :].astype(F32)
        scale = lax.rsqrt(jnp.mean(field * field, axis=-1, keepdims=True) + 1e-06)
        mixed = resid[lines, :].astype(F32) + field * scale * gain_mix_ref[...]
        after[lines, :] = mixed.astype(BF16)
        field = after[lines, :].astype(F32)
        scale = lax.rsqrt(jnp.mean(field * field, axis=-1, keepdims=True) + 1e-06)
        own = pl.ds(pl.multiple_of((m_own * 2 + core) * rows + r * 16, 16), 16)
        tokens[own, :] = (field * scale * gain_in_ref[...]).astype(BF16)
        return carry

    for h in (0, 1):
        with jax.named_scope("norm"):
            lax.fori_loop(h * bit // 16, (h + 1) * bit // 16, norm_rows, 0)
        token_copy(h).start()
        token_copy(2 + h).start()
        peer_token(6 + h).start()

    inner = (z == 1) | (z == 2)
    outer = jnp.logical_not(inner)
    z_own(1, 0).start()
    send_own_y(1).start()
    pl.when(inner)(lambda: z_own(1, 1).start())
    relay(0, z2, 0)
    relay(0, z3, 0)
    relay(0, z1, 1)
    relay(1, z, 1)
    spare_arrival(1)
    z_pass(1, 0).start()
    pl.when(inner)(lambda: z_pass(1, 1).start())
    take_token(2)
    relay(0, z3, 1)
    relay(0, z2, 1)
    take_token(3)
    take_token(0)
    token_copy(4).start()
    take_token(1)
    token_copy(5).start()

    @pl.when(outer)
    def _():
        for k in (2, 1):
            z_own(1, k).start()
            z_pass(1, k).start()

    keep_own(0).wait()
    with jax.named_scope("up_y"):
        for zz in (z, z1, z3, z2):
            for dx in (0, 1):
                y_arrival(0, zz, dx).wait_recv()

    def up_rows(m):
        def step(n, carry):
            lines = col(m * 2 * rows, 2 * rows)
            cols = col(n * chunk, chunk)
            acts = jnp.dot(tokens[lines, :], w_up[:, cols], preferred_element_type=F32)
            acts = jnp.maximum(acts, 0.0)
            hidden[lines, cols] = (acts * acts).astype(BF16)
            return carry

        with jax.named_scope("up_mm"):
            lax.fori_loop(0, units // chunk, step, 0)

    def peer_pair(k):
        with jax.named_scope(f"peer#k={k}"):
            peer_arrival(k).wait_recv()
            peer_arrival(k + 1).wait_recv()

    peer_pair(6)
    up_rows(m_own)
    peer_pair(2)
    up_rows(m_x)

    @pl.when(inner)
    def _():
        z_own(1, 2).start()
        z_pass(1, 2).start()

    peer_pair(0)
    up_rows(m_z)
    take_token(4)
    take_token(5)
    relay(1, z1, 0)
    relay(1, z1, 1)
    peer_pair(4)
    up_rows(m_d)
    keep_own(1).wait()

    zh = z // 2
    near, far = (zh * 2, zh * 2 + 1), (2 - zh * 2, 3 - zh * 2)
    order = [(near[0], y), (near[1], y), (near[0], yo), (near[1], yo)]
    x_first = (True, True, True, True, True, False, True, False)
    order += [(far[0], y), (far[1], y), (far[0], yo), (far[1], yo)]

    def columns(i):
        zz, yy = order[i]
        return col((zz * 2 + yy) * chunk, chunk)

    def stage_a(i):
        zz, yy = order[i]
        if i == 2:
            relay(1, z3, 0)
        if i == 3:
            relay(1, z2, 0)
        if i == 4:
            relay(1, z3, 1)
            relay(1, z2, 1)
        if i % 4 >= 2:
            with jax.named_scope("down_y"):
                for dx in (0, 1):
                    y_arrival(1, zz, dx).wait_recv()
        zz, yy = order[i]
        first = zz * 4 + yy * 2

        def step(m, carry):
            weights = jnp.concatenate([w_down[first], w_down[first + 1]], axis=1)
            both = jnp.dot(
                hidden[col(m * 2 * rows, 2 * rows), :], weights, preferred_element_type=F32
            ).astype(BF16)
            part[i, col(m * rows, rows), :] = both[:rows]
            part[i, col((4 + m) * rows, rows), :] = both[rows:]
            return carry

        with jax.named_scope("down_mm"):
            lax.fori_loop(0, 4, step, 0)
        peer_copy(i).start()

    def peer_copy(i):
        return remote(
            part.at[i, col((1 - core) * half, half), :],
            peer.at[i],
            c_send.at[0, i],
            c_recv.at[0, i],
            me,
            1 - core,
        )

    def chip_sum(i, m):
        own = part[i, col((core * 4 + m) * rows, rows), :].astype(F32)
        return own + peer[i, col(m * rows, rows), :].astype(F32)

    def legs(i):
        x_leg, z_leg = (x_dev, m_x), (z_dev, m_z)
        return (x_leg, z_leg) if x_first[i] else (z_leg, x_leg)

    def first_copy(i):
        dev = legs(i)[0][0]
        return remote(a_out.at[i], a_in.at[i], c_send.at[1, i], c_recv.at[1, i], dev, core)

    def second_copy(i):
        dev = legs(i)[1][0]
        return remote(b_out.at[i], b_in.at[i], c_send.at[2, i], c_recv.at[2, i], dev, core)

    def stage_b(i):
        with jax.named_scope("part_peer"):
            peer_copy(i).wait_recv()
        a_out[i, :rows, :] = chip_sum(i, legs(i)[0][1]).astype(BF16)
        a_out[i, rows:, :] = chip_sum(i, m_d).astype(BF16)
        first_copy(i).start()

    def stage_c(i):
        with jax.named_scope("part_first"):
            first_copy(i).wait_recv()
        b_out[i] = (chip_sum(i, legs(i)[1][1]) + a_in[i, rows:, :].astype(F32)).astype(BF16)
        second_copy(i).start()

    def stage_d(i):
        with jax.named_scope("part_second"):
            second_copy(i).wait_recv()
        ffn[:, columns(i)] = (
            chip_sum(i, m_own) + a_in[i, :rows, :].astype(F32) + b_in[i].astype(F32)
        )

    for i in range(8 + 3):
        if i < 8:
            stage_a(i)
        if 0 <= i - 2 < 8:
            stage_c(i - 2)
        if 0 <= i - 3 < 8:
            stage_d(i - 3)
        if i < 8:
            stage_b(i)

    def finish(r, carry):
        lines = col(r * 16, 16)
        field = ffn[lines, :]
        scale = lax.rsqrt(jnp.mean(field * field, axis=-1, keepdims=True) + 1e-06)
        out_ref[lines, :] = (
            after[lines, :].astype(F32) + field * scale * gain_out_ref[...]
        ).astype(BF16)
        return carry

    with jax.named_scope("finish"):
        lax.fori_loop(0, rows // 16, finish, 0)

    near_halo(lambda c: c.wait_send())
    far_halo(lambda c: c.wait_send())
    mix_copy.wait_send()
    for w in (0, 1):
        send_own_y(w).wait_send()
        for k in (0, 1):
            x_send(w, k).wait_send()
        for k in range(3):
            z_own(w, k).wait_send()
            z_pass(w, k).wait_send()
        forward(w, z, 1).wait_send()
        for zz in columns_z:
            for dx in (0, 1):
                forward(w, zz, dx).wait_send()
    for k in range(6):
        token_copy(k).wait_send()
    for k in range(8):
        peer_token(k).wait_send()
    for i in range(8):
        peer_copy(i).wait_send()
        first_copy(i).wait_send()
        second_copy(i).wait_send()


def slice_body(
    queries,
    key_heads,
    value_heads,
    sink_logit,
    doc_ids,
    residual,
    out_proj,
    gain_mix,
    up_proj,
    down_proj,
    gain_ffn_in,
    gain_ffn_out,
):
    positions, width = residual.shape
    rows = positions // lax.axis_size("tp")
    units = up_proj.shape[1] // 4
    strips = width // up_proj.shape[0]
    chunk = 2 * down_proj.shape[1]
    heads, kv = queries.shape[1], key_heads.shape[1]
    framed = positions + 2 * WINDOW
    inv_freq = 10000.0 ** (-jnp.arange(0, HD, 2, dtype=F32) / HD)
    freq = jnp.concatenate([inv_freq, inv_freq]).reshape(1, HD)
    vmem = pl.BlockSpec(memory_space=pltpu.VMEM)
    hbm = pl.BlockSpec(memory_space=pl.ANY)
    dma = pltpu.SemaphoreType.DMA
    shapes = [
        ((framed, HD), F32),
        ((framed, HD), F32),
        ((positions, heads), BF16),
        ((framed, kv), BF16),
        ((framed, kv), BF16),
        ((positions, heads), BF16),
        ((heads, width), BF16),
        ((rows, width), BF16),
        ((rows, width), BF16),
        ((rows, width), BF16),
        ((rows, width), BF16),
        ((rows, width), BF16),
        ((width, units), BF16),
        ((strips, units, down_proj.shape[1]), BF16),
        ((up_proj.shape[0], units), BF16),
        ((units, down_proj.shape[1]), BF16),
        ((8 * rows, width), BF16),
        ((8 * rows, units), BF16),
        ((strips // 2, 8 * rows, chunk), BF16),
        ((strips // 2, 4 * rows, chunk), BF16),
        ((strips // 2, 2 * rows, chunk), BF16),
        ((strips // 2, 2 * rows, chunk), BF16),
        ((strips // 2, rows, chunk), BF16),
        ((strips // 2, rows, chunk), BF16),
        ((rows, width), F32),
    ]
    sems = [(2,), (5,), (4,), (4,), None, None, (2, 2), (2,)] + [(2, 8)] * 4 + [(6,), (6,), (8,), (8,), (3, 8), (3, 8)]
    return pl.pallas_call(
        layer_kernel,
        out_shape=jax.ShapeDtypeStruct((rows, width), BF16),
        in_specs=[pl.BlockSpec(memory_space=pltpu.SMEM)] + [vmem] * 5 + [hbm] * 7,
        out_specs=vmem,
        scratch_shapes=[pltpu.VMEM(s, t) for s, t in shapes]
        + [dma if s is None else dma(s) for s in sems],
        compiler_params=pltpu.CompilerParams(
            collective_id=0, has_side_effects=True, vmem_limit_bytes=62 << 20
        ),
        name="layer",
    )(
        sink_logit,
        freq,
        doc_ids.reshape(-1, WINDOW),
        gain_mix.reshape(1, -1),
        gain_ffn_in.reshape(1, -1),
        gain_ffn_out.reshape(1, -1),
        queries,
        key_heads,
        value_heads,
        residual,
        out_proj,
        up_proj,
        down_proj,
    )


def solution(mesh):
    sp, tp = mesh.shape["sp"], mesh.shape["tp"]
    direct = sp == 16 and tp == 2
    if direct:
        body, fine, rows = slice_body, mesh, ("sp",)
    else:
        body, rows = general_body, SP
        fine = Mesh(mesh.devices.reshape(sp // 8, 2, 2, 2, tp), SP + ("tp",))
    return jax.shard_map(
        body,
        mesh=fine,
        in_specs=(
            P(rows, "tp"),
            P(rows, "tp"),
            P(rows, "tp"),
            P("tp"),
            P(),
            P(rows, None),
            P("tp", None),
            P(),
            P(rows, "tp"),
            P("tp", rows),
            P(),
            P(),
        ),
        out_specs=P(rows + ("tp",), None),
        check_vma=False,
    )
```

```python
import math

import jax
import jax.numpy as jnp
import numpy as np
from jax import lax
from jax.experimental import pallas as pl
from jax.experimental.pallas import tpu as pltpu
from jax.sharding import Mesh, PartitionSpec as P

MESH = pl.DeviceIdType.MESH
BF16, F32 = jnp.bfloat16, jnp.float32

HD = 128
WINDOW = 128
SP = ("a", "b", "c", "d")
GRP = ("c", "d")
CROSS = ("a", "b")


def padded(shard, sides, width):
    for axis, dim in sides:
        devices, length = (lax.axis_size(axis), shard.shape[dim])
        up = [(i, (i + 1) % devices) for i in range(devices - 1)]
        down = [(j, i) for i, j in up]
        last = lax.slice_in_dim(shard, length - width, length, axis=dim)
        first = lax.slice_in_dim(shard, 0, width, axis=dim)
        before = lax.ppermute(last, axis, up)
        after = lax.ppermute(first, axis, down)
        shard = jnp.concatenate([before, shard, after], axis=dim)
    return shard


def rotate(field, places):
    half_dim = HD // 2
    inv_freq = 10000.0 ** (-jnp.arange(0, HD, 2, dtype=jnp.float32) / HD)
    angles = places[:, None, None] * inv_freq[None, None, :]
    cosine = jnp.cos(angles)
    sine = jnp.sin(angles)
    lower = field[..., :half_dim].astype(jnp.float32)
    upper = field[..., half_dim:].astype(jnp.float32)
    return jnp.concatenate(
        [lower * cosine - upper * sine, upper * cosine + lower * sine], axis=-1
    ).astype(jnp.bfloat16)


def banded(field, blocks):
    framed = field.reshape((blocks + 2, WINDOW) + field.shape[1:])
    return jnp.concatenate([framed[:-2], framed[1:-1], framed[2:]], axis=1)


def rms_scale(field, gain_vec):
    return field * lax.rsqrt(jnp.mean(field * field, axis=-1, keepdims=True) + 1e-06) * gain_vec


def swap_tp(rows):
    return lax.ppermute(rows, "tp", [(0, 1), (1, 0)])


def gather_tp(rows):
    if lax.axis_size("tp") == 2:
        return jnp.concatenate([rows, swap_tp(rows)], axis=0)
    return lax.all_gather(rows, "tp", axis=0, tiled=True)


def scatter_tp(partial_value, own_first=True):
    devices = lax.axis_size("tp")
    if devices != 2:
        return lax.psum_scatter(partial_value, "tp", scatter_dimension=0, tiled=True).astype(
            jnp.float32
        )
    share = partial_value.shape[0] // 2
    if own_first:
        own, other = partial_value[:share], partial_value[share:]
    else:
        me = lax.axis_index("tp")
        own = lax.dynamic_slice_in_dim(partial_value, me * share, share, 0)
        other = lax.dynamic_slice_in_dim(partial_value, (1 - me) * share, share, 0)
    return own.astype(jnp.float32) + swap_tp(other).astype(jnp.float32)


def to_peer(rows, k):
    if k == 0:
        return rows
    return lax.ppermute(rows, GRP, [(i, i ^ k) for i in range(4)])


def attention_part(sp, queries, key_heads, value_heads, sink_logit, doc_ids, out_proj):
    tok_count = queries.shape[0]
    blocks = tok_count // WINDOW
    q_local = queries.shape[1] // HD
    kv_local = key_heads.shape[1] // HD
    group_size = q_local // kv_local
    offset = lax.axis_index(sp) * tok_count
    places = (offset + jnp.arange(tok_count)).astype(jnp.float32)
    rotated_q = rotate(queries.reshape(tok_count, q_local, HD), places).reshape(
        blocks, WINDOW, kv_local, group_size, HD
    )
    rotated_k = rotate(key_heads.reshape(tok_count, kv_local, HD), places).reshape(
        tok_count, kv_local * HD
    )
    rimmed = padded(jnp.stack([rotated_k, value_heads]), ((sp, 1),), WINDOW)
    key_win = banded(rimmed[0].reshape(-1, kv_local, HD), blocks)
    val_win = banded(rimmed[1].reshape(-1, kv_local, HD), blocks)
    padded_docs = jnp.pad(doc_ids, (WINDOW, WINDOW), constant_values=-1)
    key_docs = banded(lax.dynamic_slice_in_dim(padded_docs, offset, tok_count + 2 * WINDOW), blocks)
    query_docs = lax.dynamic_slice_in_dim(doc_ids, offset, tok_count).reshape(blocks, WINDOW)
    q_index = jnp.arange(WINDOW)[:, None]
    k_index = jnp.arange(3 * WINDOW)[None, :]
    in_window = jnp.abs(k_index - WINDOW - q_index) <= WINDOW
    allowed = (in_window[None] & (query_docs[:, :, None] == key_docs[:, None, :]))[:, None, None]
    scores = jnp.einsum(
        "nqkgd,nskd->nkgqs", rotated_q, key_win, preferred_element_type=jnp.float32
    ) * HD ** (-0.5)
    masked = jnp.where(allowed, scores, -1e30)
    sink_col = sink_logit.reshape(kv_local, group_size)[None, :, :, None]
    top_score = jnp.maximum(jnp.max(masked, axis=-1), sink_col)
    exp_scores = jnp.where(allowed, jnp.exp(masked - top_score[..., None]), 0.0)
    denom_sum = jnp.sum(exp_scores, axis=-1) + jnp.exp(sink_col - top_score)
    probs = (exp_scores / denom_sum[..., None]).astype(jnp.bfloat16)
    attn = (
        jnp.einsum("nkgqs,nskd->nqkgd", probs, val_win, preferred_element_type=jnp.float32)
        .astype(jnp.bfloat16)
        .reshape(tok_count, q_local * HD)
    )
    part = jnp.dot(attn, out_proj, preferred_element_type=jnp.float32).astype(jnp.bfloat16)
    return part


def general_body(
    queries,
    key_heads,
    value_heads,
    sink_logit,
    doc_ids,
    residual,
    out_proj,
    gain_mix,
    up_proj,
    down_proj,
    gain_ffn_in,
    gain_ffn_out,
):
    up_quarter = lax.all_to_all(up_proj, GRP, split_axis=1, concat_axis=0, tiled=True)
    down_quarter = lax.all_to_all(down_proj, GRP, split_axis=0, concat_axis=1, tiled=True)
    queries, key_heads, up_quarter, down_quarter = lax.optimization_barrier(
        (queries, key_heads, up_quarter, down_quarter)
    )
    half_units = up_quarter.shape[1] // 2
    up_early = lax.all_gather(up_quarter[:, :half_units], CROSS, axis=0, tiled=True)
    up_late = lax.all_gather(up_quarter[:, half_units:], CROSS, axis=0, tiled=True)
    down_all = lax.all_gather(down_quarter, CROSS, axis=0, tiled=False)
    share_rows = queries.shape[0] // lax.axis_size("tp")
    part = attention_part(SP, queries, key_heads, value_heads, sink_logit, doc_ids, out_proj)
    part, up_early = lax.optimization_barrier((part, up_early))
    mixed = scatter_tp(part, own_first=False)
    own_residual = lax.dynamic_slice_in_dim(
        residual, lax.axis_index("tp") * share_rows, share_rows, 0
    )
    after_mix = (own_residual.astype(jnp.float32) + rms_scale(mixed, gain_mix)).astype(jnp.bfloat16)
    normed = rms_scale(after_mix.astype(jnp.float32), gain_ffn_in).astype(jnp.bfloat16)
    sizes = [lax.axis_size(a) for a in SP]
    order = [SP.index(a) for a in CROSS + GRP]
    width = normed.shape[1]
    strip = width // math.prod(sizes)
    normed = (
        normed.reshape(share_rows, *sizes, strip)
        .transpose(0, *[1 + o for o in order], 5)
        .reshape(share_rows, width)
    )
    blocks = [to_peer(normed, k) for k in range(4)]
    partials = []
    for k in (3, 2, 1, 0):
        rows = gather_tp(blocks[k])
        hidden = jnp.concatenate(
            [
                jnp.square(
                    jax.nn.relu(jnp.dot(rows, w, preferred_element_type=jnp.float32))
                ).astype(jnp.bfloat16)
                for w in (up_early, up_late)
            ],
            axis=1,
        )
        partial_value = jnp.concatenate(
            [
                jnp.dot(hidden, down_all[i], preferred_element_type=jnp.float32).astype(jnp.bfloat16)
                for i in range(down_all.shape[0])
            ],
            axis=1,
        )
        partials.append(to_peer(scatter_tp(partial_value).astype(jnp.bfloat16), k))
    ffn_out = sum(p.astype(jnp.float32) for p in partials)
    back = [order.index(i) for i in range(4)]
    ffn_out = (
        ffn_out.reshape(share_rows, *[sizes[o] for o in order], strip)
        .transpose(0, *[1 + b for b in back], 5)
        .reshape(share_rows, width)
    )
    return (after_mix.astype(jnp.float32) + rms_scale(ffn_out, gain_ffn_out)).astype(jnp.bfloat16)


def layer_kernel(
    sink_ref,
    freq_ref,
    docs_ref,
    gain_mix_ref,
    gain_in_ref,
    gain_out_ref,
    q_ref,
    k_ref,
    v_ref,
    residual_ref,
    proj_ref,
    up_ref,
    down_ref,
    out_ref,
    cos_ref,
    sin_ref,
    q_buf,
    k_buf,
    v_buf,
    attn,
    proj,
    resid,
    mix_own,
    mix_out,
    mix_in,
    after,
    w_up,
    w_down,
    spare_up,
    spare_down,
    tokens,
    acts,
    hidden,
    part,
    peer,
    a_out,
    a_in,
    b_out,
    b_in,
    ffn,
    local_sem,
    load_sem,
    h_send,
    h_recv,
    m_send,
    m_recv,
    a_send,
    s_recv,
    w_send,
    w_recv,
    y_send,
    y_recv,
    t_send,
    t_recv,
    p_send,
    p_recv,
    c_send,
    c_recv,
):
    me, core = lax.axis_index("sp"), lax.axis_index("tp")
    last = lax.axis_size("sp") - 1
    z, y, x = me // 4, lax.rem(me // 2, 2), lax.rem(me, 2)
    zl = lax.rem(z, 2)
    z1, z2, z3 = z + 1 - 2 * zl, lax.rem(z + 2, 4), 3 - z
    xo, yo = 1 - x, 1 - y
    positions = q_ref.shape[0]
    rows = positions // 2
    strip, units = up_ref.shape[0], up_ref.shape[1] // 4
    chunk = 2 * strip
    half = 4 * rows
    blocks = positions // WINDOW
    kv_heads = k_ref.shape[1] // HD
    group_size = q_ref.shape[1] // k_ref.shape[1]

    def place(zz, yy, xx):
        return zz * 4 + yy * 2 + xx

    def col(start, size):
        return pl.ds(pl.multiple_of(start, size), size)

    x_dev, z_dev, y_dev = place(z, y, xo), place(z1, y, x), place(z, yo, x)

    def slot(w, s):
        if w == 0:
            return w_up.at[col(s * strip, strip), :]
        return w_down.at[s]

    def shard(w, zz, xx):
        q = lax.rem(zz, 2) * 2 + xx
        if w == 0:
            return up_ref.at[:, col(q * units, units)]
        return down_ref.at[col(q * units, units), :]

    def remote(src, dst, send, recv, dev, c):
        return pltpu.make_async_remote_copy(
            src_ref=src,
            dst_ref=dst,
            send_sem=send,
            recv_sem=recv,
            device_id=(dev, c),
            device_id_type=MESH,
        )

    def to_x(dx):
        return xo if dx else x

    def spare(w):
        return (spare_up, spare_down)[w]

    def x_send(w, k):
        return remote(
            shard(w, z1 if k else z, xo),
            spare(w) if k else slot(w, me),
            a_send.at[w, k],
            s_recv.at[w] if k else w_recv.at[w, z * 2 + 1],
            x_dev,
            core,
        )

    columns_z = (z1, z3, z2)

    def z_own(w, k):
        zz = columns_z[k]
        return remote(
            shard(w, zz, x),
            slot(w, me),
            w_send.at[w, k],
            w_recv.at[w, z * 2],
            place(zz, y, x),
            core,
        )

    def z_pass(w, k):
        zz = columns_z[k]
        return remote(
            slot(w, x_dev) if k == 2 else spare(w),
            slot(w, x_dev),
            w_send.at[w, 3 + k],
            w_recv.at[w, z * 2 + 1],
            place(zz, y, x),
            core,
        )

    def spare_arrival(w):
        with jax.named_scope(f"spare#w={w}"):
            remote(spare(w), spare(w), a_send.at[w, 1], s_recv.at[w], me, core).wait_recv()

    def send_own_y(w):
        return remote(
            shard(w, z, x),
            slot(w, me),
            w_send.at[w, 6],
            y_recv.at[w, z * 2],
            place(z, yo, x),
            core,
        )

    def keep_own(w):
        return pltpu.make_async_copy(shard(w, z, x), slot(w, me), local_sem.at[w])

    def arrival(w, zz, dx):
        s = slot(w, place(zz, y, to_x(dx)))
        return remote(s, s, y_send.at[w, zz * 2 + dx], w_recv.at[w, zz * 2 + dx], me, core)

    def forward(w, zz, dx):
        s = slot(w, place(zz, y, to_x(dx)))
        return remote(
            s,
            s,
            y_send.at[w, zz * 2 + dx],
            y_recv.at[w, zz * 2 + dx],
            place(z, yo, x),
            core,
        )

    def y_arrival(w, zz, dx):
        s = slot(w, place(zz, yo, to_x(dx)))
        return remote(s, s, y_send.at[w, zz * 2 + dx], y_recv.at[w, zz * 2 + dx], me, core)

    def relay(w, zz, dx):
        with jax.named_scope(f"relay#w={w}"):
            arrival(w, zz, dx).wait_recv()
        forward(w, zz, dx).start()

    m_own, m_z = zl * 2 + x, (1 - zl) * 2 + x
    m_x, m_d = zl * 2 + xo, (1 - zl) * 2 + xo
    bit = rows // 2

    def token_bit(c, m, h):
        return tokens.at[col((m * 2 + c) * rows + h * bit, bit), :]

    sent = ((m_own, 0, z_dev), (m_own, 1, z_dev), (m_own, 0, x_dev), (m_own, 1, x_dev), (m_z, 0, x_dev), (m_z, 1, x_dev))
    got = ((m_z, 0), (m_z, 1), (m_x, 0), (m_x, 1), (m_d, 0), (m_d, 1))

    def token_copy(k):
        m, h, dev = sent[k]
        s = token_bit(core, m, h)
        return remote(s, s, t_send.at[k], t_recv.at[k], dev, core)

    def token_arrival(k):
        m, h = got[k]
        s = token_bit(core, m, h)
        return remote(s, s, t_send.at[k], t_recv.at[k], me, core)

    def peer_token(k):
        m, h = got[k] if k < 6 else (m_own, k - 6)
        s = token_bit(core, m, h)
        return remote(s, s, p_send.at[k], p_recv.at[k], me, 1 - core)

    def peer_arrival(k):
        m, h = got[k] if k < 6 else (m_own, k - 6)
        s = token_bit(1 - core, m, h)
        return remote(s, s, p_send.at[k], p_recv.at[k], me, 1 - core)

    def take_token(k):
        with jax.named_scope(f"token#k={k}"):
            token_arrival(k).wait_recv()
        peer_token(k).start()

    def halo(k, side):
        ref, buf = ((k_ref, k_buf), (v_ref, v_buf))[k]
        src = ref.at[positions - WINDOW :, :] if side else ref.at[:WINDOW, :]
        dst = buf.at[:WINDOW, :] if side else buf.at[positions + WINDOW :, :]
        sem = k * 2 + side
        return remote(src, dst, h_send.at[sem], h_recv.at[sem], me + (1 if side else -1), core)

    loads = (
        (k_ref, k_buf.at[WINDOW : positions + WINDOW, :]),
        (v_ref, v_buf.at[WINDOW : positions + WINDOW, :]),
        (q_ref, q_buf),
        (proj_ref, proj),
        (residual_ref.at[col(core * rows, rows), :], resid),
    )

    def load(i):
        return pltpu.make_async_copy(loads[i][0], loads[i][1], load_sem.at[i])

    barrier = pltpu.get_barrier_semaphore()
    friends = [(place(zz, y, x), core) for zz in columns_z] + [(x_dev, core), (y_dev, core), (me, 1 - core)]
    for dev in friends:
        pl.semaphore_signal(barrier, inc=1, device_id=dev, device_id_type=MESH)
    beyond = me - 1 + 2 * x
    has_beyond = (beyond >= 0) & (beyond <= last)

    @pl.when(has_beyond)
    def _():
        pl.semaphore_signal(barrier, inc=1, device_id=(beyond, core), device_id_type=MESH)

    for i in range(len(loads)):
        load(i).start()
    for w in (0, 1):
        keep_own(w).start()

    @pl.when(me == 0)
    def _():
        k_buf[:WINDOW, :] = jnp.zeros((WINDOW, k_buf.shape[1]), BF16)
        v_buf[:WINDOW, :] = jnp.zeros((WINDOW, k_buf.shape[1]), BF16)

    @pl.when(me == last)
    def _():
        k_buf[positions + WINDOW :, :] = jnp.zeros((WINDOW, k_buf.shape[1]), BF16)
        v_buf[positions + WINDOW :, :] = jnp.zeros((WINDOW, k_buf.shape[1]), BF16)

    def turn(b, carry):
        shape = (WINDOW, HD)
        at = (me * blocks + b - 1) * WINDOW + lax.broadcasted_iota(jnp.int32, shape, 0)
        angles = at.astype(F32) * freq_ref[...]
        lower = lax.broadcasted_iota(jnp.int32, shape, 1) < HD // 2
        lines = col(b * WINDOW, WINDOW)
        cos_ref[lines, :] = jnp.cos(angles)
        sine = jnp.sin(angles)
        sin_ref[lines, :] = jnp.where(lower, -sine, sine)
        return carry

    with jax.named_scope("angles"):
        lax.fori_loop(0, blocks + 2, turn, 0)
    with jax.named_scope("entry"):
        pl.semaphore_wait(barrier, len(friends) + has_beyond.astype(jnp.int32))

    def near_halo(act):
        for k in (0, 1):
            pl.when(x == 0)(lambda: act(halo(k, 1)))
            pl.when(x == 1)(lambda: act(halo(k, 0)))

    def far_halo(act):
        for k in (0, 1):
            pl.when((x == 1) & has_beyond)(lambda: act(halo(k, 1)))
            pl.when((x == 0) & has_beyond)(lambda: act(halo(k, 0)))

    def near_halo_arrival(act):
        for k in (0, 1):
            pl.when(x == 1)(lambda: act(halo(k, 1)))
            pl.when(x == 0)(lambda: act(halo(k, 0)))

    def far_halo_arrival(act):
        for k in (0, 1):
            pl.when((x == 0) & has_beyond)(lambda: act(halo(k, 1)))
            pl.when((x == 1) & has_beyond)(lambda: act(halo(k, 0)))

    near_halo(lambda c: c.start())
    x_send(0, 0).start()
    far_halo(lambda c: c.start())
    x_send(0, 1).start()
    send_own_y(0).start()
    for k in range(3):
        z_own(0, k).start()
    inner = (z == 1) | (z == 2)
    outer = jnp.logical_not(inner)
    soon, late = jnp.where(outer, z2, z3), jnp.where(outer, z3, z2)
    send_own_y(1).start()
    pl.when(inner)(lambda: z_own(1, 0).start())

    def rotate_rows(buf, base, heads, shift):
        def step(b, carry):
            lines = col(base + b * WINDOW, WINDOW)
            turn = col(base + shift + b * WINDOW, WINDOW)
            cosine, sine = cos_ref[turn, :], sin_ref[turn, :]
            for h in range(heads):
                lanes = slice(h * HD, (h + 1) * HD)
                u = buf[lines, lanes].astype(F32)
                buf[lines, lanes] = (u * cosine + pltpu.roll(u, HD // 2, 1) * sine).astype(BF16)
            return carry

        return step

    with jax.named_scope("rotate"):
        load(0).wait()
        lax.fori_loop(0, blocks, rotate_rows(k_buf, WINDOW, kv_heads, 0), 0)
        load(2).wait()
        lax.fori_loop(0, blocks, rotate_rows(q_buf, 0, kv_heads * group_size, WINDOW), 0)
        load(1).wait()

    def attend(b):
        lines = col(b * WINDOW, WINDOW)
        window = pl.ds(pl.multiple_of(b * WINDOW, WINDOW), 3 * WINDOW)
        shape = (WINDOW, WINDOW)
        away = lax.broadcasted_iota(jnp.int32, shape, 1) - lax.broadcasted_iota(jnp.int32, shape, 0)

        def docs(j):
            at = me * blocks + b + j - 1
            inside = (at >= 0) & (at <= (last + 1) * blocks - 1)
            row = docs_ref[pl.ds(jnp.clip(at, 0, (last + 1) * blocks - 1), 1), :]
            return jnp.broadcast_to(jnp.where(inside, row, -1).astype(F32), shape)

        own_docs = jnp.transpose(docs(1))
        limits = (away >= 0, None, away <= 0)
        bias = []
        for j in range(3):
            same = own_docs == docs(j)
            allowed = same if limits[j] is None else limits[j] & same
            bias.append(jnp.where(allowed, 0.0, -1e30))
        bias = jnp.concatenate(bias, axis=1)

        def step(h, carry):
            keys = k_buf[window, col(h * HD, HD)]
            values = v_buf[window, col(h * HD, HD)]
            for g in range(group_size):
                head = h * group_size + g
                sink = sink_ref[head]
                scores = lax.dot_general(
                    q_buf[lines, col(head * HD, HD)],
                    keys,
                    (((1,), (1,)), ((), ())),
                    preferred_element_type=F32,
                )
                scores = scores * HD ** (-0.5) + bias
                top = jnp.maximum(jnp.max(scores, axis=1, keepdims=True), sink)
                exps = jnp.exp(scores - top)
                total = jnp.sum(exps, axis=1, keepdims=True) + jnp.exp(sink - top)
                probs = (exps * (1.0 / total)).astype(BF16)
                attn[lines, col(head * HD, HD)] = jnp.dot(
                    probs, values, preferred_element_type=F32
                ).astype(BF16)
            return carry

        with jax.named_scope("attend"):
            lax.fori_loop(0, kv_heads, step, 0)

    attend(1)
    with jax.named_scope("halo_near"):
        near_halo_arrival(lambda c: c.wait_recv())
    rotate_rows(k_buf, (1 - x) * (positions + WINDOW), kv_heads, 0)(0, 0)
    attend((1 - x) * (blocks - 1))
    relay(0, z1, 0)
    with jax.named_scope("halo_far"):
        far_halo_arrival(lambda c: c.wait_recv())
    rotate_rows(k_buf, x * (positions + WINDOW), kv_heads, 0)(0, 0)
    attend(x * (blocks - 1))
    relay(0, z, 1)
    z_pass(0, 2).start()
    load(3).wait()

    def project(start, target):
        def step(n, carry):
            cols = col(n * chunk, chunk)
            target[:, cols] = jnp.dot(
                attn[col(start, rows), :], proj[:, cols], preferred_element_type=F32
            ).astype(BF16)
            return carry

        with jax.named_scope("project"):
            lax.fori_loop(0, proj.shape[1] // chunk, step, 0)

    project((1 - core) * rows, mix_out)
    mix_copy = remote(mix_out, mix_in, m_send, m_recv, me, 1 - core)
    mix_copy.start()
    spare_arrival(0)
    for k in (0, 1):
        z_pass(0, k).start()
    for k in (1, 0):
        x_send(1, k).start()
    project(core * rows, mix_own)
    load(4).wait()
    mix_copy.wait_recv()

    def norm_rows(r, carry):
        lines = col(r * 16, 16)
        field = mix_own[lines, :].astype(F32) + mix_in[lines, :].astype(F32)
        scale = lax.rsqrt(jnp.mean(field * field, axis=-1, keepdims=True) + 1e-06)
        mixed = resid[lines, :].astype(F32) + field * scale * gain_mix_ref[...]
        after[lines, :] = mixed.astype(BF16)
        field = after[lines, :].astype(F32)
        scale = lax.rsqrt(jnp.mean(field * field, axis=-1, keepdims=True) + 1e-06)
        own = pl.ds(pl.multiple_of((m_own * 2 + core) * rows + r * 16, 16), 16)
        tokens[own, :] = (field * scale * gain_in_ref[...]).astype(BF16)
        return carry

    for h in (0, 1):
        with jax.named_scope("norm"):
            lax.fori_loop(h * bit // 16, (h + 1) * bit // 16, norm_rows, 0)
        token_copy(h).start()
        token_copy(2 + h).start()
        peer_token(6 + h).start()

    pl.when(outer)(lambda: z_own(1, 0).start())
    pl.when(inner)(lambda: z_own(1, 1).start())
    relay(0, z2, 0)
    relay(0, z3, 0)
    relay(0, z1, 1)
    spare_arrival(1)
    z_pass(1, 0).start()
    pl.when(inner)(lambda: z_pass(1, 1).start())
    pl.when(outer)(lambda: z_own(1, 2).start())
    relay(0, z3, 1)
    relay(0, z2, 1)
    relay(1, z, 1)
    pl.when(outer)(lambda: z_pass(1, 2).start())
    take_token(2)
    take_token(3)
    take_token(0)
    token_copy(4).start()
    take_token(1)
    token_copy(5).start()

    keep_own(0).wait()

    def half_dot(yy, m, cols):
        total = None
        for zz in range(4):
            depth = col((zz * 2 + yy) * chunk, chunk)
            term = jnp.dot(
                tokens[col(m * 2 * rows, 2 * rows), depth], w_up[depth, cols], preferred_element_type=F32
            )
            total = term if total is None else total + term
        return total

    def up_early(m):
        def step(n, carry):
            cols = col(n * chunk, chunk)
            acts[col(m * 2 * rows, 2 * rows), cols] = half_dot(y, m, cols)
            return carry

        with jax.named_scope("up_early"):
            lax.fori_loop(0, units // chunk, step, 0)

    def up_late(m):
        def step(n, carry):
            lines, cols = col(m * 2 * rows, 2 * rows), col(n * chunk, chunk)
            total = jnp.maximum(acts[lines, cols] + half_dot(yo, m, cols), 0.0)
            hidden[lines, cols] = (total * total).astype(BF16)
            return carry

        with jax.named_scope("up_late"):
            lax.fori_loop(0, units // chunk, step, 0)

    def peer_pair(k):
        with jax.named_scope(f"peer#k={k}"):
            peer_arrival(k).wait_recv()
            peer_arrival(k + 1).wait_recv()

    peer_pair(6)
    up_early(m_own)

    peer_pair(2)
    up_early(m_x)

    @pl.when(inner)
    def _():
        z_own(1, 2).start()
        z_pass(1, 2).start()

    peer_pair(0)
    up_early(m_z)
    relay(1, z1, 0)
    with jax.named_scope("up_y"):
        for zz in (z, z1, z3, z2):
            for dx in (0, 1):
                y_arrival(0, zz, dx).wait_recv()
    up_late(m_own)
    relay(1, z1, 1)

    @pl.when(outer)
    def _():
        z_own(1, 1).start()
        z_pass(1, 1).start()

    up_late(m_x)
    up_late(m_z)
    take_token(4)
    take_token(5)
    peer_pair(4)
    up_early(m_d)
    up_late(m_d)
    keep_own(1).wait()

    zh = z // 2
    near, far = (zh * 2, zh * 2 + 1), (soon, late)
    order = [(near[0], y), (near[1], y), (near[0], yo), (near[1], yo)]
    x_first = (True, True, True, True, True, True, False, True)
    order += [(far[0], y), (far[1], y), (far[0], yo), (far[1], yo)]

    def columns(i):
        zz, yy = order[i]
        return col((zz * 2 + yy) * chunk, chunk)

    def stage_a(i):
        zz, yy = order[i]
        if i % 4 >= 2:
            with jax.named_scope("down_y"):
                for dx in (0, 1):
                    y_arrival(1, zz, dx).wait_recv()
        zz, yy = order[i]
        first = zz * 4 + yy * 2

        def step(p, carry):
            weights = jnp.concatenate([w_down[first], w_down[first + 1]], axis=1)
            both = jnp.dot(
                hidden[col(p * half, half), :], weights, preferred_element_type=F32
            ).astype(BF16)
            for k in range(2):
                for c in range(2):
                    lines = slice((2 * k + c) * rows, (2 * k + c + 1) * rows)
                    part[i, col((4 * c + 2 * p + k) * rows, rows), :] = both[lines]
            return carry

        with jax.named_scope("down_mm"):
            lax.fori_loop(0, 2, step, 0)
        peer_copy(i).start()

    def peer_copy(i):
        return remote(
            part.at[i, col((1 - core) * half, half), :],
            peer.at[i],
            c_send.at[0, i],
            c_recv.at[0, i],
            me,
            1 - core,
        )

    def chip_sum(i, m):
        own = part[i, col((core * 4 + m) * rows, rows), :].astype(F32)
        return own + peer[i, col(m * rows, rows), :].astype(F32)

    def legs(i):
        x_leg, z_leg = (x_dev, m_x), (z_dev, m_z)
        return (x_leg, z_leg) if x_first[i] else (z_leg, x_leg)

    def first_copy(i):
        dev = legs(i)[0][0]
        return remote(a_out.at[i], a_in.at[i], c_send.at[1, i], c_recv.at[1, i], dev, core)

    def second_copy(i):
        dev = legs(i)[1][0]
        return remote(b_out.at[i], b_in.at[i], c_send.at[2, i], c_recv.at[2, i], dev, core)

    def stage_b(i):
        with jax.named_scope("part_peer"):
            peer_copy(i).wait_recv()
        a_out[i, :rows, :] = chip_sum(i, legs(i)[0][1]).astype(BF16)
        a_out[i, rows:, :] = chip_sum(i, m_d).astype(BF16)
        first_copy(i).start()

    def stage_c(i):
        with jax.named_scope("part_first"):
            first_copy(i).wait_recv()
        b_out[i] = (chip_sum(i, legs(i)[1][1]) + a_in[i, rows:, :].astype(F32)).astype(BF16)
        second_copy(i).start()

    def stage_d(i):
        with jax.named_scope("part_second"):
            second_copy(i).wait_recv()
        ffn[:, columns(i)] = (
            chip_sum(i, m_own) + a_in[i, :rows, :].astype(F32) + b_in[i].astype(F32)
        )

    def far_relay(who, zz, sides):
        @pl.when(who)
        def _():
            for dx in sides:
                relay(1, zz, dx)

    far_relay(inner, soon, (0, 1))
    for i in range(8 + 3):
        if i < 8:
            stage_a(i)
        if 0 <= i - 2 < 8:
            stage_c(i - 2)
        if 0 <= i - 3 < 8:
            stage_d(i - 3)
        if i < 8:
            stage_b(i)
        if i == 0:
            far_relay(inner, late, (0, 1))
        if i == 2:
            far_relay(outer, soon, (0, 1))
        if i == 3:
            far_relay(outer, late, (0, 1))

    def finish(r, carry):
        lines = col(r * 16, 16)
        field = ffn[lines, :]
        scale = lax.rsqrt(jnp.mean(field * field, axis=-1, keepdims=True) + 1e-06)
        out_ref[lines, :] = (
            after[lines, :].astype(F32) + field * scale * gain_out_ref[...]
        ).astype(BF16)
        return carry

    with jax.named_scope("finish"):
        lax.fori_loop(0, rows // 16, finish, 0)

    near_halo(lambda c: c.wait_send())
    far_halo(lambda c: c.wait_send())
    mix_copy.wait_send()
    for w in (0, 1):
        send_own_y(w).wait_send()
        for k in (0, 1):
            x_send(w, k).wait_send()
        for k in range(3):
            z_own(w, k).wait_send()
            z_pass(w, k).wait_send()
        forward(w, z, 1).wait_send()
        for zz in columns_z:
            for dx in (0, 1):
                forward(w, zz, dx).wait_send()
    for k in range(6):
        token_copy(k).wait_send()
    for k in range(8):
        peer_token(k).wait_send()
    for i in range(8):
        peer_copy(i).wait_send()
        first_copy(i).wait_send()
        second_copy(i).wait_send()


def slice_body(
    queries,
    key_heads,
    value_heads,
    sink_logit,
    doc_ids,
    residual,
    out_proj,
    gain_mix,
    up_proj,
    down_proj,
    gain_ffn_in,
    gain_ffn_out,
):
    positions, width = residual.shape
    rows = positions // lax.axis_size("tp")
    units = up_proj.shape[1] // 4
    strips = width // up_proj.shape[0]
    chunk = 2 * down_proj.shape[1]
    heads, kv = queries.shape[1], key_heads.shape[1]
    framed = positions + 2 * WINDOW
    inv_freq = np.float32(10000.0) ** (-np.arange(0, HD, 2, dtype=np.float32) / HD)
    freq = jnp.asarray(np.concatenate([inv_freq, inv_freq]).reshape(1, HD))
    vmem = pl.BlockSpec(memory_space=pltpu.VMEM)
    hbm = pl.BlockSpec(memory_space=pl.ANY)
    dma = pltpu.SemaphoreType.DMA
    shapes = [
        ((framed, HD), F32),
        ((framed, HD), F32),
        ((positions, heads), BF16),
        ((framed, kv), BF16),
        ((framed, kv), BF16),
        ((positions, heads), BF16),
        ((heads, width), BF16),
        ((rows, width), BF16),
        ((rows, width), BF16),
        ((rows, width), BF16),
        ((rows, width), BF16),
        ((rows, width), BF16),
        ((width, units), BF16),
        ((strips, units, down_proj.shape[1]), BF16),
        ((up_proj.shape[0], units), BF16),
        ((units, down_proj.shape[1]), BF16),
        ((8 * rows, width), BF16),
        ((8 * rows, units), F32),
        ((8 * rows, units), BF16),
        ((strips // 2, 8 * rows, chunk), BF16),
        ((strips // 2, 4 * rows, chunk), BF16),
        ((strips // 2, 2 * rows, chunk), BF16),
        ((strips // 2, 2 * rows, chunk), BF16),
        ((strips // 2, rows, chunk), BF16),
        ((strips // 2, rows, chunk), BF16),
        ((rows, width), F32),
    ]
    sems = [(2,), (5,), (4,), (4,), None, None, (2, 2), (2,)] + [(2, 8)] * 4 + [(6,), (6,), (8,), (8,), (3, 8), (3, 8)]
    return pl.pallas_call(
        layer_kernel,
        out_shape=jax.ShapeDtypeStruct((rows, width), BF16),
        in_specs=[pl.BlockSpec(memory_space=pltpu.SMEM)] + [vmem] * 5 + [hbm] * 7,
        out_specs=vmem,
        scratch_shapes=[pltpu.VMEM(s, t) for s, t in shapes]
        + [dma if s is None else dma(s) for s in sems],
        compiler_params=pltpu.CompilerParams(
            collective_id=0, has_side_effects=True, vmem_limit_bytes=58 << 20
        ),
        name="layer",
    )(
        sink_logit,
        freq,
        doc_ids.reshape(-1, WINDOW),
        gain_mix.reshape(1, -1),
        gain_ffn_in.reshape(1, -1),
        gain_ffn_out.reshape(1, -1),
        queries,
        key_heads,
        value_heads,
        residual,
        out_proj,
        up_proj,
        down_proj,
    )


def solution(mesh):
    sp, tp = mesh.shape["sp"], mesh.shape["tp"]
    direct = sp == 16 and tp == 2
    if direct:
        body, fine, rows = slice_body, mesh, ("sp",)
    else:
        body, rows = general_body, SP
        fine = Mesh(mesh.devices.reshape(sp // 8, 2, 2, 2, tp), SP + ("tp",))
    return jax.shard_map(
        body,
        mesh=fine,
        in_specs=(
            P(rows, "tp"),
            P(rows, "tp"),
            P(rows, "tp"),
            P("tp"),
            P(),
            P(rows, None),
            P("tp", None),
            P(),
            P(rows, "tp"),
            P("tp", rows),
            P(),
            P(),
        ),
        out_specs=P(rows + ("tp",), None),
        check_vma=False,
    )
```

```python
import math

import jax
import jax.numpy as jnp
import numpy as np
from jax import lax
from jax.experimental import pallas as pl
from jax.experimental.pallas import tpu as pltpu
from jax.sharding import Mesh, PartitionSpec as P

MESH = pl.DeviceIdType.MESH
BF16, F32 = jnp.bfloat16, jnp.float32

HD = 128
WINDOW = 128
SP = ("a", "b", "c", "d")
GRP = ("c", "d")
CROSS = ("a", "b")


def padded(shard, sides, width):
    for axis, dim in sides:
        devices, length = (lax.axis_size(axis), shard.shape[dim])
        up = [(i, (i + 1) % devices) for i in range(devices - 1)]
        down = [(j, i) for i, j in up]
        last = lax.slice_in_dim(shard, length - width, length, axis=dim)
        first = lax.slice_in_dim(shard, 0, width, axis=dim)
        before = lax.ppermute(last, axis, up)
        after = lax.ppermute(first, axis, down)
        shard = jnp.concatenate([before, shard, after], axis=dim)
    return shard


def rotate(field, places):
    half_dim = HD // 2
    inv_freq = 10000.0 ** (-jnp.arange(0, HD, 2, dtype=jnp.float32) / HD)
    angles = places[:, None, None] * inv_freq[None, None, :]
    cosine = jnp.cos(angles)
    sine = jnp.sin(angles)
    lower = field[..., :half_dim].astype(jnp.float32)
    upper = field[..., half_dim:].astype(jnp.float32)
    return jnp.concatenate(
        [lower * cosine - upper * sine, upper * cosine + lower * sine], axis=-1
    ).astype(jnp.bfloat16)


def banded(field, blocks):
    framed = field.reshape((blocks + 2, WINDOW) + field.shape[1:])
    return jnp.concatenate([framed[:-2], framed[1:-1], framed[2:]], axis=1)


def rms_scale(field, gain_vec):
    return field * lax.rsqrt(jnp.mean(field * field, axis=-1, keepdims=True) + 1e-06) * gain_vec


def swap_tp(rows):
    return lax.ppermute(rows, "tp", [(0, 1), (1, 0)])


def gather_tp(rows):
    if lax.axis_size("tp") == 2:
        return jnp.concatenate([rows, swap_tp(rows)], axis=0)
    return lax.all_gather(rows, "tp", axis=0, tiled=True)


def scatter_tp(partial_value, own_first=True):
    devices = lax.axis_size("tp")
    if devices != 2:
        return lax.psum_scatter(partial_value, "tp", scatter_dimension=0, tiled=True).astype(
            jnp.float32
        )
    share = partial_value.shape[0] // 2
    if own_first:
        own, other = partial_value[:share], partial_value[share:]
    else:
        me = lax.axis_index("tp")
        own = lax.dynamic_slice_in_dim(partial_value, me * share, share, 0)
        other = lax.dynamic_slice_in_dim(partial_value, (1 - me) * share, share, 0)
    return own.astype(jnp.float32) + swap_tp(other).astype(jnp.float32)


def to_peer(rows, k):
    if k == 0:
        return rows
    return lax.ppermute(rows, GRP, [(i, i ^ k) for i in range(4)])


def attention_part(sp, queries, key_heads, value_heads, sink_logit, doc_ids, out_proj):
    tok_count = queries.shape[0]
    blocks = tok_count // WINDOW
    q_local = queries.shape[1] // HD
    kv_local = key_heads.shape[1] // HD
    group_size = q_local // kv_local
    offset = lax.axis_index(sp) * tok_count
    places = (offset + jnp.arange(tok_count)).astype(jnp.float32)
    rotated_q = rotate(queries.reshape(tok_count, q_local, HD), places).reshape(
        blocks, WINDOW, kv_local, group_size, HD
    )
    rotated_k = rotate(key_heads.reshape(tok_count, kv_local, HD), places).reshape(
        tok_count, kv_local * HD
    )
    rimmed = padded(jnp.stack([rotated_k, value_heads]), ((sp, 1),), WINDOW)
    key_win = banded(rimmed[0].reshape(-1, kv_local, HD), blocks)
    val_win = banded(rimmed[1].reshape(-1, kv_local, HD), blocks)
    padded_docs = jnp.pad(doc_ids, (WINDOW, WINDOW), constant_values=-1)
    key_docs = banded(lax.dynamic_slice_in_dim(padded_docs, offset, tok_count + 2 * WINDOW), blocks)
    query_docs = lax.dynamic_slice_in_dim(doc_ids, offset, tok_count).reshape(blocks, WINDOW)
    q_index = jnp.arange(WINDOW)[:, None]
    k_index = jnp.arange(3 * WINDOW)[None, :]
    in_window = jnp.abs(k_index - WINDOW - q_index) <= WINDOW
    allowed = (in_window[None] & (query_docs[:, :, None] == key_docs[:, None, :]))[:, None, None]
    scores = jnp.einsum(
        "nqkgd,nskd->nkgqs", rotated_q, key_win, preferred_element_type=jnp.float32
    ) * HD ** (-0.5)
    masked = jnp.where(allowed, scores, -1e30)
    sink_col = sink_logit.reshape(kv_local, group_size)[None, :, :, None]
    top_score = jnp.maximum(jnp.max(masked, axis=-1), sink_col)
    exp_scores = jnp.where(allowed, jnp.exp(masked - top_score[..., None]), 0.0)
    denom_sum = jnp.sum(exp_scores, axis=-1) + jnp.exp(sink_col - top_score)
    probs = (exp_scores / denom_sum[..., None]).astype(jnp.bfloat16)
    attn = (
        jnp.einsum("nkgqs,nskd->nqkgd", probs, val_win, preferred_element_type=jnp.float32)
        .astype(jnp.bfloat16)
        .reshape(tok_count, q_local * HD)
    )
    part = jnp.dot(attn, out_proj, preferred_element_type=jnp.float32).astype(jnp.bfloat16)
    return part


def general_body(
    queries,
    key_heads,
    value_heads,
    sink_logit,
    doc_ids,
    residual,
    out_proj,
    gain_mix,
    up_proj,
    down_proj,
    gain_ffn_in,
    gain_ffn_out,
):
    up_quarter = lax.all_to_all(up_proj, GRP, split_axis=1, concat_axis=0, tiled=True)
    down_quarter = lax.all_to_all(down_proj, GRP, split_axis=0, concat_axis=1, tiled=True)
    queries, key_heads, up_quarter, down_quarter = lax.optimization_barrier(
        (queries, key_heads, up_quarter, down_quarter)
    )
    half_units = up_quarter.shape[1] // 2
    up_early = lax.all_gather(up_quarter[:, :half_units], CROSS, axis=0, tiled=True)
    up_late = lax.all_gather(up_quarter[:, half_units:], CROSS, axis=0, tiled=True)
    down_all = lax.all_gather(down_quarter, CROSS, axis=0, tiled=False)
    share_rows = queries.shape[0] // lax.axis_size("tp")
    part = attention_part(SP, queries, key_heads, value_heads, sink_logit, doc_ids, out_proj)
    part, up_early = lax.optimization_barrier((part, up_early))
    mixed = scatter_tp(part, own_first=False)
    own_residual = lax.dynamic_slice_in_dim(
        residual, lax.axis_index("tp") * share_rows, share_rows, 0
    )
    after_mix = (own_residual.astype(jnp.float32) + rms_scale(mixed, gain_mix)).astype(jnp.bfloat16)
    normed = rms_scale(after_mix.astype(jnp.float32), gain_ffn_in).astype(jnp.bfloat16)
    sizes = [lax.axis_size(a) for a in SP]
    order = [SP.index(a) for a in CROSS + GRP]
    width = normed.shape[1]
    strip = width // math.prod(sizes)
    normed = (
        normed.reshape(share_rows, *sizes, strip)
        .transpose(0, *[1 + o for o in order], 5)
        .reshape(share_rows, width)
    )
    blocks = [to_peer(normed, k) for k in range(4)]
    partials = []
    for k in (3, 2, 1, 0):
        rows = gather_tp(blocks[k])
        hidden = jnp.concatenate(
            [
                jnp.square(
                    jax.nn.relu(jnp.dot(rows, w, preferred_element_type=jnp.float32))
                ).astype(jnp.bfloat16)
                for w in (up_early, up_late)
            ],
            axis=1,
        )
        partial_value = jnp.concatenate(
            [
                jnp.dot(hidden, down_all[i], preferred_element_type=jnp.float32).astype(jnp.bfloat16)
                for i in range(down_all.shape[0])
            ],
            axis=1,
        )
        partials.append(to_peer(scatter_tp(partial_value).astype(jnp.bfloat16), k))
    ffn_out = sum(p.astype(jnp.float32) for p in partials)
    back = [order.index(i) for i in range(4)]
    ffn_out = (
        ffn_out.reshape(share_rows, *[sizes[o] for o in order], strip)
        .transpose(0, *[1 + b for b in back], 5)
        .reshape(share_rows, width)
    )
    return (after_mix.astype(jnp.float32) + rms_scale(ffn_out, gain_ffn_out)).astype(jnp.bfloat16)


def layer_kernel(
    sink_ref,
    freq_ref,
    docs_ref,
    gain_mix_ref,
    gain_in_ref,
    gain_out_ref,
    q_ref,
    k_ref,
    v_ref,
    residual_ref,
    proj_ref,
    up_ref,
    down_ref,
    out_ref,
    cos_ref,
    sin_ref,
    q_buf,
    k_buf,
    v_buf,
    attn,
    proj,
    resid,
    mix_own,
    mix_out,
    mix_in,
    after,
    w_up,
    w_down,
    spare_up,
    spare_down,
    tokens,
    acts,
    hidden,
    part,
    peer,
    a_out,
    a_in,
    b_out,
    b_in,
    ffn,
    local_sem,
    load_sem,
    h_send,
    h_recv,
    m_send,
    m_recv,
    a_send,
    s_recv,
    w_send,
    w_recv,
    y_send,
    y_recv,
    t_send,
    t_recv,
    p_send,
    p_recv,
    c_send,
    c_recv,
):
    me, core = lax.axis_index("sp"), lax.axis_index("tp")
    last = lax.axis_size("sp") - 1
    z, y, x = me // 4, lax.rem(me // 2, 2), lax.rem(me, 2)
    zl = lax.rem(z, 2)
    z1, z2, z3 = z + 1 - 2 * zl, lax.rem(z + 2, 4), 3 - z
    xo, yo = 1 - x, 1 - y
    positions = q_ref.shape[0]
    rows = positions // 2
    strip, span = up_ref.shape[0], up_ref.shape[1] // 2
    small, big = span // 2 - strip, span // 2 + strip
    chunk = 2 * strip
    half = 4 * rows
    blocks = positions // WINDOW
    kv_heads = k_ref.shape[1] // HD
    group_size = q_ref.shape[1] // k_ref.shape[1]

    def place(zz, yy, xx):
        return zz * 4 + yy * 2 + xx

    def col(start, size):
        return pl.ds(pl.multiple_of(start, size), size)

    x_dev, z_dev, y_dev = place(z, y, xo), place(z1, y, x), place(z, yo, x)

    inner = (z == 1) | (z == 2)
    outer = jnp.logical_not(inner)

    def either(act):
        pl.when(inner)(lambda: act(True))
        pl.when(outer)(lambda: act(False))

    def size(role):
        return big if role else small

    def slot(w, s, role):
        if w == 0:
            return w_up.at[col(s * strip, strip), : size(role)]
        return w_down.at[s, : size(role), :]

    def spare(w, role):
        return spare_down.at[: size(role), :] if w else spare_up.at[:, : size(role)]

    def shard(w, role, xx):
        start = pl.multiple_of(xx * span + (small if role else 0), strip)
        if w == 0:
            return up_ref.at[:, pl.ds(start, size(role))]
        return down_ref.at[pl.ds(start, size(role)), :]

    def remote(src, dst, send, recv, dev, c):
        return pltpu.make_async_remote_copy(
            src_ref=src,
            dst_ref=dst,
            send_sem=send,
            recv_sem=recv,
            device_id=(dev, c),
            device_id_type=MESH,
        )

    def to_x(dx):
        return xo if dx else x

    def x_send(w, k, role):
        target = (not role) if k else role
        return remote(
            shard(w, target, xo),
            spare(w, target) if k else slot(w, me, target),
            a_send.at[w, k],
            s_recv.at[w] if k else w_recv.at[w, z * 2 + 1],
            x_dev,
            core,
        )

    columns_z = (z1, z3, z2)

    def z_own(w, k, role):
        target = role if k == 1 else not role
        return remote(
            shard(w, target, x),
            slot(w, me, target),
            w_send.at[w, k],
            w_recv.at[w, z * 2],
            place(columns_z[k], y, x),
            core,
        )

    def z_pass(w, k, role):
        target = role if k == 1 else not role
        return remote(
            slot(w, x_dev, target) if k == 1 else spare(w, target),
            slot(w, x_dev, target),
            w_send.at[w, 3 + k],
            w_recv.at[w, z * 2 + 1],
            place(columns_z[k], y, x),
            core,
        )

    def spare_arrival(w):
        def act(role):
            ref = spare(w, not role)
            remote(ref, ref, a_send.at[w, 1], s_recv.at[w], me, core).wait_recv()

        with jax.named_scope(f"spare#w={w}"):
            either(act)

    def send_own_y(w, role):
        return remote(
            shard(w, role, x),
            slot(w, me, role),
            w_send.at[w, 6],
            y_recv.at[w, z * 2],
            y_dev,
            core,
        )

    def keep_own(w, role):
        return pltpu.make_async_copy(shard(w, role, x), slot(w, me, role), local_sem.at[w])

    def arrival(w, zz, dx, role):
        s = slot(w, place(zz, y, to_x(dx)), role)
        return remote(s, s, y_send.at[w, zz * 2 + dx], w_recv.at[w, zz * 2 + dx], me, core)

    def forward(w, zz, dx, role):
        s = slot(w, place(zz, y, to_x(dx)), role)
        return remote(s, s, y_send.at[w, zz * 2 + dx], y_recv.at[w, zz * 2 + dx], y_dev, core)

    def y_arrival(w, zz, dx, role):
        s = slot(w, place(zz, yo, to_x(dx)), role)
        return remote(s, s, y_send.at[w, zz * 2 + dx], y_recv.at[w, zz * 2 + dx], me, core)

    def relay(w, zz, dx):
        def act(role):
            arrival(w, zz, dx, role).wait_recv()
            forward(w, zz, dx, role).start()

        with jax.named_scope(f"relay#w={w}"):
            either(act)

    def go(copy, *at):
        either(lambda role: copy(*at, role).start())

    def go_inner(copy, *at):
        pl.when(inner)(lambda: copy(*at, True).start())

    def go_outer(copy, *at):
        pl.when(outer)(lambda: copy(*at, False).start())

    m_own, m_z = zl * 2 + x, (1 - zl) * 2 + x
    m_x, m_d = zl * 2 + xo, (1 - zl) * 2 + xo
    bit = rows // 2

    def token_bit(c, m, h):
        return tokens.at[col((m * 2 + c) * rows + h * bit, bit), :]

    sent = ((m_own, 0, z_dev), (m_own, 1, z_dev), (m_own, 0, x_dev), (m_own, 1, x_dev), (m_z, 0, x_dev), (m_z, 1, x_dev))
    got = ((m_z, 0), (m_z, 1), (m_x, 0), (m_x, 1), (m_d, 0), (m_d, 1))

    def token_copy(k):
        m, h, dev = sent[k]
        s = token_bit(core, m, h)
        return remote(s, s, t_send.at[k], t_recv.at[k], dev, core)

    def token_arrival(k):
        m, h = got[k]
        s = token_bit(core, m, h)
        return remote(s, s, t_send.at[k], t_recv.at[k], me, core)

    def peer_token(k):
        m, h = got[k] if k < 6 else (m_own, k - 6)
        s = token_bit(core, m, h)
        return remote(s, s, p_send.at[k], p_recv.at[k], me, 1 - core)

    def peer_arrival(k):
        m, h = got[k] if k < 6 else (m_own, k - 6)
        s = token_bit(1 - core, m, h)
        return remote(s, s, p_send.at[k], p_recv.at[k], me, 1 - core)

    def take_token(k):
        with jax.named_scope(f"token#k={k}"):
            token_arrival(k).wait_recv()
        peer_token(k).start()

    def halo(k, side):
        ref, buf = ((k_ref, k_buf), (v_ref, v_buf))[k]
        src = ref.at[positions - WINDOW :, :] if side else ref.at[:WINDOW, :]
        dst = buf.at[:WINDOW, :] if side else buf.at[positions + WINDOW :, :]
        sem = k * 2 + side
        return remote(src, dst, h_send.at[sem], h_recv.at[sem], me + (1 if side else -1), core)

    loads = (
        (k_ref, k_buf.at[WINDOW : positions + WINDOW, :]),
        (v_ref, v_buf.at[WINDOW : positions + WINDOW, :]),
        (q_ref, q_buf),
        (proj_ref, proj),
        (residual_ref.at[col(core * rows, rows), :], resid),
    )

    def load(i):
        return pltpu.make_async_copy(loads[i][0], loads[i][1], load_sem.at[i])

    barrier = pltpu.get_barrier_semaphore()
    friends = [(place(zz, y, x), core) for zz in columns_z] + [(x_dev, core), (y_dev, core), (me, 1 - core)]
    for dev in friends:
        pl.semaphore_signal(barrier, inc=1, device_id=dev, device_id_type=MESH)
    beyond = me - 1 + 2 * x
    has_beyond = (beyond >= 0) & (beyond <= last)

    @pl.when(has_beyond)
    def _():
        pl.semaphore_signal(barrier, inc=1, device_id=(beyond, core), device_id_type=MESH)

    for i in range(len(loads)):
        load(i).start()
    for w in (0, 1):
        go(keep_own, w)

    @pl.when(me == 0)
    def _():
        k_buf[:WINDOW, :] = jnp.zeros((WINDOW, k_buf.shape[1]), BF16)
        v_buf[:WINDOW, :] = jnp.zeros((WINDOW, k_buf.shape[1]), BF16)

    @pl.when(me == last)
    def _():
        k_buf[positions + WINDOW :, :] = jnp.zeros((WINDOW, k_buf.shape[1]), BF16)
        v_buf[positions + WINDOW :, :] = jnp.zeros((WINDOW, k_buf.shape[1]), BF16)

    def turn(b, carry):
        shape = (WINDOW, HD)
        at = (me * blocks + b - 1) * WINDOW + lax.broadcasted_iota(jnp.int32, shape, 0)
        angles = at.astype(F32) * freq_ref[...]
        lower = lax.broadcasted_iota(jnp.int32, shape, 1) < HD // 2
        lines = col(b * WINDOW, WINDOW)
        cos_ref[lines, :] = jnp.cos(angles)
        sine = jnp.sin(angles)
        sin_ref[lines, :] = jnp.where(lower, -sine, sine)
        return carry

    with jax.named_scope("angles"):
        lax.fori_loop(0, blocks + 2, turn, 0)
    with jax.named_scope("entry"):
        pl.semaphore_wait(barrier, len(friends) + has_beyond.astype(jnp.int32))

    def near_halo(act):
        for k in (0, 1):
            pl.when(x == 0)(lambda: act(halo(k, 1)))
            pl.when(x == 1)(lambda: act(halo(k, 0)))

    def far_halo(act):
        for k in (0, 1):
            pl.when((x == 1) & has_beyond)(lambda: act(halo(k, 1)))
            pl.when((x == 0) & has_beyond)(lambda: act(halo(k, 0)))

    def near_halo_arrival(act):
        for k in (0, 1):
            pl.when(x == 1)(lambda: act(halo(k, 1)))
            pl.when(x == 0)(lambda: act(halo(k, 0)))

    def far_halo_arrival(act):
        for k in (0, 1):
            pl.when((x == 0) & has_beyond)(lambda: act(halo(k, 1)))
            pl.when((x == 1) & has_beyond)(lambda: act(halo(k, 0)))

    near_halo(lambda c: c.start())
    go(x_send, 0, 0)
    far_halo(lambda c: c.start())
    go(x_send, 0, 1)
    go(send_own_y, 0)
    for k in range(3):
        go(z_own, 0, k)
    soon, late = jnp.where(outer, z2, z3), jnp.where(outer, z3, z2)
    go(send_own_y, 1)
    go_inner(z_own, 1, 0)

    def rotate_rows(buf, base, heads, shift):
        def step(b, carry):
            lines = col(base + b * WINDOW, WINDOW)
            turn = col(base + shift + b * WINDOW, WINDOW)
            cosine, sine = cos_ref[turn, :], sin_ref[turn, :]
            for h in range(heads):
                lanes = slice(h * HD, (h + 1) * HD)
                u = buf[lines, lanes].astype(F32)
                buf[lines, lanes] = (u * cosine + pltpu.roll(u, HD // 2, 1) * sine).astype(BF16)
            return carry

        return step

    with jax.named_scope("rotate"):
        load(0).wait()
        lax.fori_loop(0, blocks, rotate_rows(k_buf, WINDOW, kv_heads, 0), 0)
        load(2).wait()
        lax.fori_loop(0, blocks, rotate_rows(q_buf, 0, kv_heads * group_size, WINDOW), 0)
        load(1).wait()

    def attend(b):
        lines = col(b * WINDOW, WINDOW)
        window = pl.ds(pl.multiple_of(b * WINDOW, WINDOW), 3 * WINDOW)
        shape = (WINDOW, WINDOW)
        away = lax.broadcasted_iota(jnp.int32, shape, 1) - lax.broadcasted_iota(jnp.int32, shape, 0)

        def docs(j):
            at = me * blocks + b + j - 1
            inside = (at >= 0) & (at <= (last + 1) * blocks - 1)
            row = docs_ref[pl.ds(jnp.clip(at, 0, (last + 1) * blocks - 1), 1), :]
            return jnp.broadcast_to(jnp.where(inside, row, -1).astype(F32), shape)

        own_docs = jnp.transpose(docs(1))
        limits = (away >= 0, None, away <= 0)
        bias = []
        for j in range(3):
            same = own_docs == docs(j)
            allowed = same if limits[j] is None else limits[j] & same
            bias.append(jnp.where(allowed, 0.0, -1e30))
        bias = jnp.concatenate(bias, axis=1)

        def step(h, carry):
            keys = k_buf[window, col(h * HD, HD)]
            values = v_buf[window, col(h * HD, HD)]
            for g in range(group_size):
                head = h * group_size + g
                sink = sink_ref[head]
                scores = lax.dot_general(
                    q_buf[lines, col(head * HD, HD)],
                    keys,
                    (((1,), (1,)), ((), ())),
                    preferred_element_type=F32,
                )
                scores = scores * HD ** (-0.5) + bias
                top = jnp.maximum(jnp.max(scores, axis=1, keepdims=True), sink)
                exps = jnp.exp(scores - top)
                total = jnp.sum(exps, axis=1, keepdims=True) + jnp.exp(sink - top)
                probs = (exps * (1.0 / total)).astype(BF16)
                attn[lines, col(head * HD, HD)] = jnp.dot(
                    probs, values, preferred_element_type=F32
                ).astype(BF16)
            return carry

        with jax.named_scope("attend"):
            lax.fori_loop(0, kv_heads, step, 0)

    attend(1)
    with jax.named_scope("halo_near"):
        near_halo_arrival(lambda c: c.wait_recv())
    rotate_rows(k_buf, (1 - x) * (positions + WINDOW), kv_heads, 0)(0, 0)
    attend((1 - x) * (blocks - 1))
    relay(0, z1, 0)
    with jax.named_scope("halo_far"):
        far_halo_arrival(lambda c: c.wait_recv())
    rotate_rows(k_buf, x * (positions + WINDOW), kv_heads, 0)(0, 0)
    attend(x * (blocks - 1))
    relay(0, z, 1)
    go(z_pass, 0, 1)
    load(3).wait()

    def project(start, target):
        def step(n, carry):
            cols = col(n * chunk, chunk)
            target[:, cols] = jnp.dot(
                attn[col(start, rows), :], proj[:, cols], preferred_element_type=F32
            ).astype(BF16)
            return carry

        with jax.named_scope("project"):
            lax.fori_loop(0, proj.shape[1] // chunk, step, 0)

    project((1 - core) * rows, mix_out)
    mix_copy = remote(mix_out, mix_in, m_send, m_recv, me, 1 - core)
    mix_copy.start()
    spare_arrival(0)
    for k in (0, 2):
        go(z_pass, 0, k)
    for k in (1, 0):
        go(x_send, 1, k)
    project(core * rows, mix_own)
    load(4).wait()
    mix_copy.wait_recv()

    def norm_rows(r, carry):
        lines = col(r * 16, 16)
        field = mix_own[lines, :].astype(F32) + mix_in[lines, :].astype(F32)
        scale = lax.rsqrt(jnp.mean(field * field, axis=-1, keepdims=True) + 1e-06)
        mixed = resid[lines, :].astype(F32) + field * scale * gain_mix_ref[...]
        after[lines, :] = mixed.astype(BF16)
        field = after[lines, :].astype(F32)
        scale = lax.rsqrt(jnp.mean(field * field, axis=-1, keepdims=True) + 1e-06)
        own = pl.ds(pl.multiple_of((m_own * 2 + core) * rows + r * 16, 16), 16)
        tokens[own, :] = (field * scale * gain_in_ref[...]).astype(BF16)
        return carry

    for h in (0, 1):
        with jax.named_scope("norm"):
            lax.fori_loop(h * bit // 16, (h + 1) * bit // 16, norm_rows, 0)
        token_copy(h).start()
        token_copy(2 + h).start()
        peer_token(6 + h).start()

    go_outer(z_own, 1, 0)
    go_inner(z_own, 1, 1)
    relay(0, z2, 0)
    relay(0, z3, 0)
    relay(0, z1, 1)
    spare_arrival(1)
    go(z_pass, 1, 0)
    go_outer(z_own, 1, 2)
    go_outer(z_pass, 1, 2)
    relay(0, z3, 1)
    relay(0, z2, 1)
    relay(1, z, 1)
    go_inner(z_pass, 1, 1)
    take_token(2)
    take_token(3)
    take_token(0)
    token_copy(4).start()
    take_token(1)
    token_copy(5).start()
    go_inner(z_own, 1, 2)
    go_inner(z_pass, 1, 2)

    either(lambda role: keep_own(0, role).wait())

    def half_dot(yy, m, cols):
        total = None
        for zz in range(4):
            depth = col((zz * 2 + yy) * chunk, chunk)
            term = jnp.dot(
                tokens[col(m * 2 * rows, 2 * rows), depth], w_up[depth, cols], preferred_element_type=F32
            )
            total = term if total is None else total + term
        return total

    full = jnp.where(inner, big // chunk, small // chunk)

    def each_columns(act):
        def step(n, carry):
            act(col(n * chunk, chunk))
            return carry

        lax.fori_loop(0, full, step, 0)
        act(pl.ds(pl.multiple_of(full * chunk, strip), strip))

    def up_early(m):
        def act(cols):
            acts[col(m * 2 * rows, 2 * rows), cols] = half_dot(y, m, cols)

        with jax.named_scope("up_early"):
            each_columns(act)

    def up_late(m):
        def act(cols):
            lines = col(m * 2 * rows, 2 * rows)
            total = jnp.maximum(acts[lines, cols] + half_dot(yo, m, cols), 0.0)
            hidden[lines, cols] = (total * total).astype(BF16)

        with jax.named_scope("up_late"):
            each_columns(act)

    def peer_pair(k):
        with jax.named_scope(f"peer#k={k}"):
            peer_arrival(k).wait_recv()
            peer_arrival(k + 1).wait_recv()

    peer_pair(6)
    up_early(m_own)

    peer_pair(2)
    up_early(m_x)


    peer_pair(0)
    up_early(m_z)
    relay(1, z1, 0)
    with jax.named_scope("up_y"):
        for zz in (z, z1, z3, z2):
            for dx in (0, 1):
                either(lambda role: y_arrival(0, zz, dx, role).wait_recv())
    up_late(m_own)
    relay(1, z1, 1)

    up_late(m_x)
    go_outer(z_own, 1, 1)
    go_outer(z_pass, 1, 1)
    up_late(m_z)
    take_token(4)
    take_token(5)
    peer_pair(4)
    up_early(m_d)
    up_late(m_d)
    either(lambda role: keep_own(1, role).wait())

    zh = z // 2
    near, far = (zh * 2, zh * 2 + 1), (soon, late)
    order = [(near[0], y), (near[1], y), (near[0], yo), (near[1], yo)]
    x_first = (True, True, True, False, True, False, True, False)
    order += [(far[0], y), (far[1], y), (far[0], yo), (far[1], yo)]

    def columns(i):
        zz, yy = order[i]
        return col((zz * 2 + yy) * chunk, chunk)

    def stage_a(i):
        zz, yy = order[i]
        if i % 4 >= 2:
            with jax.named_scope("down_y"):
                for dx in (0, 1):
                    either(lambda role: y_arrival(1, zz, dx, role).wait_recv())
        zz, yy = order[i]
        first = zz * 4 + yy * 2

        def multiply(role):
            depth = size(role)

            def step(p, carry):
                weights = jnp.concatenate(
                    [w_down[first, :depth, :], w_down[first + 1, :depth, :]], axis=1
                )
                both = jnp.dot(
                    hidden[col(p * half, half), :depth], weights, preferred_element_type=F32
                ).astype(BF16)
                for k in range(2):
                    for c in range(2):
                        lines = slice((2 * k + c) * rows, (2 * k + c + 1) * rows)
                        part[i, col((4 * c + 2 * p + k) * rows, rows), :] = both[lines]
                return carry

            lax.fori_loop(0, 2, step, 0)

        with jax.named_scope("down_mm"):
            either(multiply)
        peer_copy(i).start()

    def peer_copy(i):
        return remote(
            part.at[i, col((1 - core) * half, half), :],
            peer.at[i],
            c_send.at[0, i],
            c_recv.at[0, i],
            me,
            1 - core,
        )

    def chip_sum(i, m):
        own = part[i, col((core * 4 + m) * rows, rows), :].astype(F32)
        return own + peer[i, col(m * rows, rows), :].astype(F32)

    def legs(i):
        x_leg, z_leg = (x_dev, m_x), (z_dev, m_z)
        return (x_leg, z_leg) if x_first[i] else (z_leg, x_leg)

    def first_copy(i):
        dev = legs(i)[0][0]
        return remote(a_out.at[i], a_in.at[i], c_send.at[1, i], c_recv.at[1, i], dev, core)

    def second_copy(i):
        dev = legs(i)[1][0]
        return remote(b_out.at[i], b_in.at[i], c_send.at[2, i], c_recv.at[2, i], dev, core)

    def stage_b(i):
        with jax.named_scope("part_peer"):
            peer_copy(i).wait_recv()
        a_out[i, :rows, :] = chip_sum(i, legs(i)[0][1]).astype(BF16)
        a_out[i, rows:, :] = chip_sum(i, m_d).astype(BF16)
        first_copy(i).start()

    def stage_c(i):
        with jax.named_scope("part_first"):
            first_copy(i).wait_recv()
        b_out[i] = (chip_sum(i, legs(i)[1][1]) + a_in[i, rows:, :].astype(F32)).astype(BF16)
        second_copy(i).start()

    def stage_d(i):
        with jax.named_scope("part_second"):
            second_copy(i).wait_recv()
        ffn[:, columns(i)] = (
            chip_sum(i, m_own) + a_in[i, :rows, :].astype(F32) + b_in[i].astype(F32)
        )

    def far_relay(who, zz, sides):
        @pl.when(who)
        def _():
            for dx in sides:
                relay(1, zz, dx)


    far_relay(inner, soon, (0, 1))
    for i in range(8 + 5):
        if i < 8:
            stage_a(i)
        if 6 <= i < 8:
            stage_b(i)
        if 0 <= i - 2 < 8:
            stage_c(i - 2)
        if 0 <= i - 5 < 8:
            stage_d(i - 5)
        if i < 6:
            stage_b(i)
        if i == 0:
            far_relay(inner, late, (0, 1))
        if i == 1:
            far_relay(outer, soon, (0, 1))
        if i == 2:
            far_relay(outer, late, (0,))
        if i == 3:
            far_relay(outer, late, (1,))

    def finish(r, carry):
        lines = col(r * 16, 16)
        field = ffn[lines, :]
        scale = lax.rsqrt(jnp.mean(field * field, axis=-1, keepdims=True) + 1e-06)
        out_ref[lines, :] = (
            after[lines, :].astype(F32) + field * scale * gain_out_ref[...]
        ).astype(BF16)
        return carry

    with jax.named_scope("finish"):
        lax.fori_loop(0, rows // 16, finish, 0)

    near_halo(lambda c: c.wait_send())
    far_halo(lambda c: c.wait_send())
    mix_copy.wait_send()
    for w in (0, 1):

        def done(role):
            send_own_y(w, role).wait_send()
            for k in (0, 1):
                x_send(w, k, role).wait_send()
            for k in range(3):
                z_own(w, k, role).wait_send()
                z_pass(w, k, role).wait_send()
            forward(w, z, 1, role).wait_send()
            for zz in columns_z:
                for dx in (0, 1):
                    forward(w, zz, dx, role).wait_send()

        either(done)
    for k in range(6):
        token_copy(k).wait_send()
    for k in range(8):
        peer_token(k).wait_send()
    for i in range(8):
        peer_copy(i).wait_send()
        first_copy(i).wait_send()
        second_copy(i).wait_send()


def slice_body(
    queries,
    key_heads,
    value_heads,
    sink_logit,
    doc_ids,
    residual,
    out_proj,
    gain_mix,
    up_proj,
    down_proj,
    gain_ffn_in,
    gain_ffn_out,
):
    positions, width = residual.shape
    rows = positions // lax.axis_size("tp")
    units = up_proj.shape[1] // 4 + up_proj.shape[0]
    strips = width // up_proj.shape[0]
    chunk = 2 * down_proj.shape[1]
    heads, kv = queries.shape[1], key_heads.shape[1]
    framed = positions + 2 * WINDOW
    inv_freq = np.float32(10000.0) ** (-np.arange(0, HD, 2, dtype=np.float32) / HD)
    freq = jnp.asarray(np.concatenate([inv_freq, inv_freq]).reshape(1, HD))
    vmem = pl.BlockSpec(memory_space=pltpu.VMEM)
    hbm = pl.BlockSpec(memory_space=pl.ANY)
    dma = pltpu.SemaphoreType.DMA
    shapes = [
        ((framed, HD), F32),
        ((framed, HD), F32),
        ((positions, heads), BF16),
        ((framed, kv), BF16),
        ((framed, kv), BF16),
        ((positions, heads), BF16),
        ((heads, width), BF16),
        ((rows, width), BF16),
        ((rows, width), BF16),
        ((rows, width), BF16),
        ((rows, width), BF16),
        ((rows, width), BF16),
        ((width, units), BF16),
        ((strips, units, down_proj.shape[1]), BF16),
        ((up_proj.shape[0], units), BF16),
        ((units, down_proj.shape[1]), BF16),
        ((8 * rows, width), BF16),
        ((8 * rows, units), F32),
        ((8 * rows, units), BF16),
        ((strips // 2, 8 * rows, chunk), BF16),
        ((strips // 2, 4 * rows, chunk), BF16),
        ((strips // 2, 2 * rows, chunk), BF16),
        ((strips // 2, 2 * rows, chunk), BF16),
        ((strips // 2, rows, chunk), BF16),
        ((strips // 2, rows, chunk), BF16),
        ((rows, width), F32),
    ]
    sems = [(2,), (5,), (4,), (4,), None, None, (2, 2), (2,)] + [(2, 8)] * 4 + [(6,), (6,), (8,), (8,), (3, 8), (3, 8)]
    return pl.pallas_call(
        layer_kernel,
        out_shape=jax.ShapeDtypeStruct((rows, width), BF16),
        in_specs=[pl.BlockSpec(memory_space=pltpu.SMEM)] + [vmem] * 5 + [hbm] * 7,
        out_specs=vmem,
        scratch_shapes=[pltpu.VMEM(s, t) for s, t in shapes]
        + [dma if s is None else dma(s) for s in sems],
        compiler_params=pltpu.CompilerParams(
            collective_id=0, has_side_effects=True, vmem_limit_bytes=58 << 20
        ),
        name="layer",
    )(
        sink_logit,
        freq,
        doc_ids.reshape(-1, WINDOW),
        gain_mix.reshape(1, -1),
        gain_ffn_in.reshape(1, -1),
        gain_ffn_out.reshape(1, -1),
        queries,
        key_heads,
        value_heads,
        residual,
        out_proj,
        up_proj,
        down_proj,
    )


def solution(mesh):
    sp, tp = mesh.shape["sp"], mesh.shape["tp"]
    direct = sp == 16 and tp == 2
    if direct:
        body, fine, rows = slice_body, mesh, ("sp",)
    else:
        body, rows = general_body, SP
        fine = Mesh(mesh.devices.reshape(sp // 8, 2, 2, 2, tp), SP + ("tp",))
    return jax.shard_map(
        body,
        mesh=fine,
        in_specs=(
            P(rows, "tp"),
            P(rows, "tp"),
            P(rows, "tp"),
            P("tp"),
            P(),
            P(rows, None),
            P("tp", None),
            P(),
            P(rows, "tp"),
            P("tp", rows),
            P(),
            P(),
        ),
        out_specs=P(rows + ("tp",), None),
        check_vma=False,
    )
```

```python
import math

import jax
import jax.numpy as jnp
import numpy as np
from jax import lax
from jax.experimental import pallas as pl
from jax.experimental.pallas import tpu as pltpu
from jax.sharding import Mesh, PartitionSpec as P

MESH = pl.DeviceIdType.MESH
BF16, F32 = jnp.bfloat16, jnp.float32

HD = 128
WINDOW = 128
SP = ("a", "b", "c", "d")
GRP = ("c", "d")
CROSS = ("a", "b")


def padded(shard, sides, width):
    for axis, dim in sides:
        devices, length = (lax.axis_size(axis), shard.shape[dim])
        up = [(i, (i + 1) % devices) for i in range(devices - 1)]
        down = [(j, i) for i, j in up]
        last = lax.slice_in_dim(shard, length - width, length, axis=dim)
        first = lax.slice_in_dim(shard, 0, width, axis=dim)
        before = lax.ppermute(last, axis, up)
        after = lax.ppermute(first, axis, down)
        shard = jnp.concatenate([before, shard, after], axis=dim)
    return shard


def rotate(field, places):
    half_dim = HD // 2
    inv_freq = 10000.0 ** (-jnp.arange(0, HD, 2, dtype=jnp.float32) / HD)
    angles = places[:, None, None] * inv_freq[None, None, :]
    cosine = jnp.cos(angles)
    sine = jnp.sin(angles)
    lower = field[..., :half_dim].astype(jnp.float32)
    upper = field[..., half_dim:].astype(jnp.float32)
    return jnp.concatenate(
        [lower * cosine - upper * sine, upper * cosine + lower * sine], axis=-1
    ).astype(jnp.bfloat16)


def banded(field, blocks):
    framed = field.reshape((blocks + 2, WINDOW) + field.shape[1:])
    return jnp.concatenate([framed[:-2], framed[1:-1], framed[2:]], axis=1)


def rms_scale(field, gain_vec):
    return field * lax.rsqrt(jnp.mean(field * field, axis=-1, keepdims=True) + 1e-06) * gain_vec


def swap_tp(rows):
    return lax.ppermute(rows, "tp", [(0, 1), (1, 0)])


def gather_tp(rows):
    if lax.axis_size("tp") == 2:
        return jnp.concatenate([rows, swap_tp(rows)], axis=0)
    return lax.all_gather(rows, "tp", axis=0, tiled=True)


def scatter_tp(partial_value, own_first=True):
    devices = lax.axis_size("tp")
    if devices != 2:
        return lax.psum_scatter(partial_value, "tp", scatter_dimension=0, tiled=True).astype(
            jnp.float32
        )
    share = partial_value.shape[0] // 2
    if own_first:
        own, other = partial_value[:share], partial_value[share:]
    else:
        me = lax.axis_index("tp")
        own = lax.dynamic_slice_in_dim(partial_value, me * share, share, 0)
        other = lax.dynamic_slice_in_dim(partial_value, (1 - me) * share, share, 0)
    return own.astype(jnp.float32) + swap_tp(other).astype(jnp.float32)


def to_peer(rows, k):
    if k == 0:
        return rows
    return lax.ppermute(rows, GRP, [(i, i ^ k) for i in range(4)])


def attention_part(sp, queries, key_heads, value_heads, sink_logit, doc_ids, out_proj):
    tok_count = queries.shape[0]
    blocks = tok_count // WINDOW
    q_local = queries.shape[1] // HD
    kv_local = key_heads.shape[1] // HD
    group_size = q_local // kv_local
    offset = lax.axis_index(sp) * tok_count
    places = (offset + jnp.arange(tok_count)).astype(jnp.float32)
    rotated_q = rotate(queries.reshape(tok_count, q_local, HD), places).reshape(
        blocks, WINDOW, kv_local, group_size, HD
    )
    rotated_k = rotate(key_heads.reshape(tok_count, kv_local, HD), places).reshape(
        tok_count, kv_local * HD
    )
    rimmed = padded(jnp.stack([rotated_k, value_heads]), ((sp, 1),), WINDOW)
    key_win = banded(rimmed[0].reshape(-1, kv_local, HD), blocks)
    val_win = banded(rimmed[1].reshape(-1, kv_local, HD), blocks)
    padded_docs = jnp.pad(doc_ids, (WINDOW, WINDOW), constant_values=-1)
    key_docs = banded(lax.dynamic_slice_in_dim(padded_docs, offset, tok_count + 2 * WINDOW), blocks)
    query_docs = lax.dynamic_slice_in_dim(doc_ids, offset, tok_count).reshape(blocks, WINDOW)
    q_index = jnp.arange(WINDOW)[:, None]
    k_index = jnp.arange(3 * WINDOW)[None, :]
    in_window = jnp.abs(k_index - WINDOW - q_index) <= WINDOW
    allowed = (in_window[None] & (query_docs[:, :, None] == key_docs[:, None, :]))[:, None, None]
    scores = jnp.einsum(
        "nqkgd,nskd->nkgqs", rotated_q, key_win, preferred_element_type=jnp.float32
    ) * HD ** (-0.5)
    masked = jnp.where(allowed, scores, -1e30)
    sink_col = sink_logit.reshape(kv_local, group_size)[None, :, :, None]
    top_score = jnp.maximum(jnp.max(masked, axis=-1), sink_col)
    exp_scores = jnp.where(allowed, jnp.exp(masked - top_score[..., None]), 0.0)
    denom_sum = jnp.sum(exp_scores, axis=-1) + jnp.exp(sink_col - top_score)
    probs = (exp_scores / denom_sum[..., None]).astype(jnp.bfloat16)
    attn = (
        jnp.einsum("nkgqs,nskd->nqkgd", probs, val_win, preferred_element_type=jnp.float32)
        .astype(jnp.bfloat16)
        .reshape(tok_count, q_local * HD)
    )
    part = jnp.dot(attn, out_proj, preferred_element_type=jnp.float32).astype(jnp.bfloat16)
    return part


def general_body(
    queries,
    key_heads,
    value_heads,
    sink_logit,
    doc_ids,
    residual,
    out_proj,
    gain_mix,
    up_proj,
    down_proj,
    gain_ffn_in,
    gain_ffn_out,
):
    up_quarter = lax.all_to_all(up_proj, GRP, split_axis=1, concat_axis=0, tiled=True)
    down_quarter = lax.all_to_all(down_proj, GRP, split_axis=0, concat_axis=1, tiled=True)
    queries, key_heads, up_quarter, down_quarter = lax.optimization_barrier(
        (queries, key_heads, up_quarter, down_quarter)
    )
    half_units = up_quarter.shape[1] // 2
    up_early = lax.all_gather(up_quarter[:, :half_units], CROSS, axis=0, tiled=True)
    up_late = lax.all_gather(up_quarter[:, half_units:], CROSS, axis=0, tiled=True)
    down_all = lax.all_gather(down_quarter, CROSS, axis=0, tiled=False)
    share_rows = queries.shape[0] // lax.axis_size("tp")
    part = attention_part(SP, queries, key_heads, value_heads, sink_logit, doc_ids, out_proj)
    part, up_early = lax.optimization_barrier((part, up_early))
    mixed = scatter_tp(part, own_first=False)
    own_residual = lax.dynamic_slice_in_dim(
        residual, lax.axis_index("tp") * share_rows, share_rows, 0
    )
    after_mix = (own_residual.astype(jnp.float32) + rms_scale(mixed, gain_mix)).astype(jnp.bfloat16)
    normed = rms_scale(after_mix.astype(jnp.float32), gain_ffn_in).astype(jnp.bfloat16)
    sizes = [lax.axis_size(a) for a in SP]
    order = [SP.index(a) for a in CROSS + GRP]
    width = normed.shape[1]
    strip = width // math.prod(sizes)
    normed = (
        normed.reshape(share_rows, *sizes, strip)
        .transpose(0, *[1 + o for o in order], 5)
        .reshape(share_rows, width)
    )
    blocks = [to_peer(normed, k) for k in range(4)]
    partials = []
    for k in (3, 2, 1, 0):
        rows = gather_tp(blocks[k])
        hidden = jnp.concatenate(
            [
                jnp.square(
                    jax.nn.relu(jnp.dot(rows, w, preferred_element_type=jnp.float32))
                ).astype(jnp.bfloat16)
                for w in (up_early, up_late)
            ],
            axis=1,
        )
        partial_value = jnp.concatenate(
            [
                jnp.dot(hidden, down_all[i], preferred_element_type=jnp.float32).astype(jnp.bfloat16)
                for i in range(down_all.shape[0])
            ],
            axis=1,
        )
        partials.append(to_peer(scatter_tp(partial_value).astype(jnp.bfloat16), k))
    ffn_out = sum(p.astype(jnp.float32) for p in partials)
    back = [order.index(i) for i in range(4)]
    ffn_out = (
        ffn_out.reshape(share_rows, *[sizes[o] for o in order], strip)
        .transpose(0, *[1 + b for b in back], 5)
        .reshape(share_rows, width)
    )
    return (after_mix.astype(jnp.float32) + rms_scale(ffn_out, gain_ffn_out)).astype(jnp.bfloat16)


def layer_kernel(
    sink_ref,
    freq_ref,
    docs_ref,
    gain_mix_ref,
    gain_in_ref,
    gain_out_ref,
    q_ref,
    k_ref,
    v_ref,
    residual_ref,
    proj_ref,
    up_ref,
    down_ref,
    out_ref,
    cos_ref,
    sin_ref,
    q_buf,
    k_buf,
    v_buf,
    attn,
    proj,
    resid,
    mix_own,
    mix_out,
    mix_in,
    after,
    w_up,
    w_down,
    spare_up,
    spare_down,
    tokens,
    acts,
    hidden,
    part,
    peer,
    a_out,
    a_in,
    b_out,
    b_in,
    ffn,
    local_sem,
    load_sem,
    h_send,
    h_recv,
    m_send,
    m_recv,
    a_send,
    s_recv,
    w_send,
    w_recv,
    y_send,
    y_recv,
    t_send,
    t_recv,
    p_send,
    p_recv,
    c_send,
    c_recv,
):
    me, core = lax.axis_index("sp"), lax.axis_index("tp")
    last = lax.axis_size("sp") - 1
    z, y, x = me // 4, lax.rem(me // 2, 2), lax.rem(me, 2)
    zl = lax.rem(z, 2)
    z1, z2, z3 = z + 1 - 2 * zl, lax.rem(z + 2, 4), 3 - z
    xo, yo = 1 - x, 1 - y
    positions = q_ref.shape[0]
    rows = positions // 2
    strip, span = up_ref.shape[0], up_ref.shape[1] // 2
    small, big = span // 2 - strip, span // 2 + strip
    chunk = 2 * strip
    half = 4 * rows
    blocks = positions // WINDOW
    kv_heads = k_ref.shape[1] // HD
    group_size = q_ref.shape[1] // k_ref.shape[1]

    def place(zz, yy, xx):
        return zz * 4 + yy * 2 + xx

    def col(start, size):
        return pl.ds(pl.multiple_of(start, size), size)

    x_dev, z_dev, y_dev = place(z, y, xo), place(z1, y, x), place(z, yo, x)

    inner = (z == 1) | (z == 2)
    outer = jnp.logical_not(inner)

    def either(act):
        pl.when(inner)(lambda: act(True))
        pl.when(outer)(lambda: act(False))

    def size(role):
        return big if role else small

    def slot(w, s, role):
        if w == 0:
            return w_up.at[col(s * strip, strip), : size(role)]
        return w_down.at[s, : size(role), :]

    def spare(w, role):
        return spare_down.at[: size(role), :] if w else spare_up.at[:, : size(role)]

    def shard(w, role, xx):
        start = pl.multiple_of(xx * span + (small if role else 0), strip)
        if w == 0:
            return up_ref.at[:, pl.ds(start, size(role))]
        return down_ref.at[pl.ds(start, size(role)), :]

    def remote(src, dst, send, recv, dev, c):
        return pltpu.make_async_remote_copy(
            src_ref=src,
            dst_ref=dst,
            send_sem=send,
            recv_sem=recv,
            device_id=(dev, c),
            device_id_type=MESH,
        )

    def to_x(dx):
        return xo if dx else x

    def x_send(w, k, role):
        target = (not role) if k else role
        return remote(
            shard(w, target, xo),
            spare(w, target) if k else slot(w, me, target),
            a_send.at[w, k],
            s_recv.at[w] if k else w_recv.at[w, z * 2 + 1],
            x_dev,
            core,
        )

    columns_z = (z1, z3, z2)

    def z_own(w, k, role):
        target = role if k == 1 else not role
        return remote(
            shard(w, target, x),
            slot(w, me, target),
            w_send.at[w, k],
            w_recv.at[w, z * 2],
            place(columns_z[k], y, x),
            core,
        )

    def z_pass(w, k, role):
        target = role if k == 1 else not role
        return remote(
            slot(w, x_dev, target) if k == 1 else spare(w, target),
            slot(w, x_dev, target),
            w_send.at[w, 3 + k],
            w_recv.at[w, z * 2 + 1],
            place(columns_z[k], y, x),
            core,
        )

    def spare_arrival(w):
        def act(role):
            ref = spare(w, not role)
            remote(ref, ref, a_send.at[w, 1], s_recv.at[w], me, core).wait_recv()

        with jax.named_scope(f"spare#w={w}"):
            either(act)

    def send_own_y(w, role):
        return remote(
            shard(w, role, x),
            slot(w, me, role),
            w_send.at[w, 6],
            y_recv.at[w, z * 2],
            y_dev,
            core,
        )

    def keep_own(w, role):
        return pltpu.make_async_copy(shard(w, role, x), slot(w, me, role), local_sem.at[w])

    def arrival(w, zz, dx, role):
        s = slot(w, place(zz, y, to_x(dx)), role)
        return remote(s, s, y_send.at[w, zz * 2 + dx], w_recv.at[w, zz * 2 + dx], me, core)

    def forward(w, zz, dx, role):
        s = slot(w, place(zz, y, to_x(dx)), role)
        return remote(s, s, y_send.at[w, zz * 2 + dx], y_recv.at[w, zz * 2 + dx], y_dev, core)

    def y_arrival(w, zz, dx, role):
        s = slot(w, place(zz, yo, to_x(dx)), role)
        return remote(s, s, y_send.at[w, zz * 2 + dx], y_recv.at[w, zz * 2 + dx], me, core)

    def relay(w, zz, dx):
        def act(role):
            arrival(w, zz, dx, role).wait_recv()
            forward(w, zz, dx, role).start()

        with jax.named_scope(f"relay#w={w}"):
            either(act)

    def go(copy, *at):
        either(lambda role: copy(*at, role).start())

    def go_inner(copy, *at):
        pl.when(inner)(lambda: copy(*at, True).start())

    def go_outer(copy, *at):
        pl.when(outer)(lambda: copy(*at, False).start())

    m_own, m_z = zl * 2 + x, (1 - zl) * 2 + x
    m_x, m_d = zl * 2 + xo, (1 - zl) * 2 + xo
    bit = rows // 2

    def token_bit(c, m, h):
        return tokens.at[col((m * 2 + c) * rows + h * bit, bit), :]

    sent = ((m_own, 0, z_dev), (m_own, 1, z_dev), (m_own, 0, x_dev), (m_own, 1, x_dev), (m_z, 0, x_dev), (m_z, 1, x_dev))
    got = ((m_z, 0), (m_z, 1), (m_x, 0), (m_x, 1), (m_d, 0), (m_d, 1))

    def token_copy(k):
        m, h, dev = sent[k]
        s = token_bit(core, m, h)
        return remote(s, s, t_send.at[k], t_recv.at[k], dev, core)

    def token_arrival(k):
        m, h = got[k]
        s = token_bit(core, m, h)
        return remote(s, s, t_send.at[k], t_recv.at[k], me, core)

    def peer_token(k):
        m, h = got[k] if k < 6 else (m_own, k - 6)
        s = token_bit(core, m, h)
        return remote(s, s, p_send.at[k], p_recv.at[k], me, 1 - core)

    def peer_arrival(k):
        m, h = got[k] if k < 6 else (m_own, k - 6)
        s = token_bit(1 - core, m, h)
        return remote(s, s, p_send.at[k], p_recv.at[k], me, 1 - core)

    def take_token(k):
        with jax.named_scope(f"token#k={k}"):
            token_arrival(k).wait_recv()
        peer_token(k).start()

    def halo(k, side):
        ref, buf = ((k_ref, k_buf), (v_ref, v_buf))[k]
        src = ref.at[positions - WINDOW :, :] if side else ref.at[:WINDOW, :]
        dst = buf.at[:WINDOW, :] if side else buf.at[positions + WINDOW :, :]
        sem = k * 2 + side
        return remote(src, dst, h_send.at[sem], h_recv.at[sem], me + (1 if side else -1), core)

    loads = (
        (k_ref, k_buf.at[WINDOW : positions + WINDOW, :]),
        (v_ref, v_buf.at[WINDOW : positions + WINDOW, :]),
        (q_ref, q_buf),
        (proj_ref, proj),
        (residual_ref.at[col(core * rows, rows), :], resid),
    )

    def load(i):
        return pltpu.make_async_copy(loads[i][0], loads[i][1], load_sem.at[i])

    barrier = pltpu.get_barrier_semaphore()
    friends = [(place(zz, y, x), core) for zz in columns_z] + [(x_dev, core), (y_dev, core), (me, 1 - core)]
    for dev in friends:
        pl.semaphore_signal(barrier, inc=1, device_id=dev, device_id_type=MESH)
    beyond = me - 1 + 2 * x
    has_beyond = (beyond >= 0) & (beyond <= last)

    @pl.when(has_beyond)
    def _():
        pl.semaphore_signal(barrier, inc=1, device_id=(beyond, core), device_id_type=MESH)

    for i in range(len(loads)):
        load(i).start()
    for w in (0, 1):
        go(keep_own, w)

    @pl.when(me == 0)
    def _():
        k_buf[:WINDOW, :] = jnp.zeros((WINDOW, k_buf.shape[1]), BF16)
        v_buf[:WINDOW, :] = jnp.zeros((WINDOW, k_buf.shape[1]), BF16)

    @pl.when(me == last)
    def _():
        k_buf[positions + WINDOW :, :] = jnp.zeros((WINDOW, k_buf.shape[1]), BF16)
        v_buf[positions + WINDOW :, :] = jnp.zeros((WINDOW, k_buf.shape[1]), BF16)

    def turn(b, carry):
        shape = (WINDOW, HD)
        at = (me * blocks + b - 1) * WINDOW + lax.broadcasted_iota(jnp.int32, shape, 0)
        angles = at.astype(F32) * freq_ref[...]
        lower = lax.broadcasted_iota(jnp.int32, shape, 1) < HD // 2
        lines = col(b * WINDOW, WINDOW)
        cos_ref[lines, :] = jnp.cos(angles)
        sine = jnp.sin(angles)
        sin_ref[lines, :] = jnp.where(lower, -sine, sine)
        return carry

    with jax.named_scope("angles"):
        lax.fori_loop(0, blocks + 2, turn, 0)
    with jax.named_scope("entry"):
        pl.semaphore_wait(barrier, len(friends) + has_beyond.astype(jnp.int32))

    def near_halo(act):
        for k in (0, 1):
            pl.when(x == 0)(lambda: act(halo(k, 1)))
            pl.when(x == 1)(lambda: act(halo(k, 0)))

    def far_halo(act):
        for k in (0, 1):
            pl.when((x == 1) & has_beyond)(lambda: act(halo(k, 1)))
            pl.when((x == 0) & has_beyond)(lambda: act(halo(k, 0)))

    def near_halo_arrival(act):
        for k in (0, 1):
            pl.when(x == 1)(lambda: act(halo(k, 1)))
            pl.when(x == 0)(lambda: act(halo(k, 0)))

    def far_halo_arrival(act):
        for k in (0, 1):
            pl.when((x == 0) & has_beyond)(lambda: act(halo(k, 1)))
            pl.when((x == 1) & has_beyond)(lambda: act(halo(k, 0)))

    near_halo(lambda c: c.start())
    go(x_send, 0, 0)
    far_halo(lambda c: c.start())
    go(x_send, 0, 1)
    go(send_own_y, 0)
    for k in range(3):
        go(z_own, 0, k)
    soon, late = jnp.where(outer, z2, z3), jnp.where(outer, z3, z2)
    go(send_own_y, 1)
    go_inner(z_own, 1, 0)

    def rotate_rows(buf, base, heads, shift):
        def step(b, carry):
            lines = col(base + b * WINDOW, WINDOW)
            turn = col(base + shift + b * WINDOW, WINDOW)
            cosine, sine = cos_ref[turn, :], sin_ref[turn, :]
            for h in range(heads):
                lanes = slice(h * HD, (h + 1) * HD)
                u = buf[lines, lanes].astype(F32)
                buf[lines, lanes] = (u * cosine + pltpu.roll(u, HD // 2, 1) * sine).astype(BF16)
            return carry

        return step

    with jax.named_scope("rotate"):
        load(0).wait()
        lax.fori_loop(0, blocks, rotate_rows(k_buf, WINDOW, kv_heads, 0), 0)
        load(2).wait()
        lax.fori_loop(0, blocks, rotate_rows(q_buf, 0, kv_heads * group_size, WINDOW), 0)
        load(1).wait()

    def attend(b):
        lines = col(b * WINDOW, WINDOW)
        window = pl.ds(pl.multiple_of(b * WINDOW, WINDOW), 3 * WINDOW)
        shape = (WINDOW, WINDOW)
        away = lax.broadcasted_iota(jnp.int32, shape, 1) - lax.broadcasted_iota(jnp.int32, shape, 0)

        def docs(j):
            at = me * blocks + b + j - 1
            inside = (at >= 0) & (at <= (last + 1) * blocks - 1)
            row = docs_ref[pl.ds(jnp.clip(at, 0, (last + 1) * blocks - 1), 1), :]
            return jnp.broadcast_to(jnp.where(inside, row, -1).astype(F32), shape)

        own_docs = jnp.transpose(docs(1))
        limits = (away >= 0, None, away <= 0)
        bias = []
        for j in range(3):
            same = own_docs == docs(j)
            allowed = same if limits[j] is None else limits[j] & same
            bias.append(jnp.where(allowed, 0.0, -1e30))
        bias = jnp.concatenate(bias, axis=1)

        def step(h, carry):
            keys = k_buf[window, col(h * HD, HD)]
            values = v_buf[window, col(h * HD, HD)]
            for g in range(group_size):
                head = h * group_size + g
                sink = sink_ref[head]
                scores = lax.dot_general(
                    q_buf[lines, col(head * HD, HD)],
                    keys,
                    (((1,), (1,)), ((), ())),
                    preferred_element_type=F32,
                )
                scores = scores * HD ** (-0.5) + bias
                top = jnp.maximum(jnp.max(scores, axis=1, keepdims=True), sink)
                exps = jnp.exp(scores - top)
                total = jnp.sum(exps, axis=1, keepdims=True) + jnp.exp(sink - top)
                probs = (exps * (1.0 / total)).astype(BF16)
                attn[lines, col(head * HD, HD)] = jnp.dot(
                    probs, values, preferred_element_type=F32
                ).astype(BF16)
            return carry

        with jax.named_scope("attend"):
            lax.fori_loop(0, kv_heads, step, 0)

    attend(1)
    with jax.named_scope("halo_near"):
        near_halo_arrival(lambda c: c.wait_recv())
    rotate_rows(k_buf, (1 - x) * (positions + WINDOW), kv_heads, 0)(0, 0)
    attend((1 - x) * (blocks - 1))
    relay(0, z1, 0)
    with jax.named_scope("halo_far"):
        far_halo_arrival(lambda c: c.wait_recv())
    rotate_rows(k_buf, x * (positions + WINDOW), kv_heads, 0)(0, 0)
    attend(x * (blocks - 1))
    relay(0, z, 1)
    go(z_pass, 0, 1)
    load(3).wait()

    def project(start, target):
        def step(n, carry):
            cols = col(n * chunk, chunk)
            target[:, cols] = jnp.dot(
                attn[col(start, rows), :], proj[:, cols], preferred_element_type=F32
            ).astype(BF16)
            return carry

        with jax.named_scope("project"):
            lax.fori_loop(0, proj.shape[1] // chunk, step, 0)

    project((1 - core) * rows, mix_out)
    mix_copy = remote(mix_out, mix_in, m_send, m_recv, me, 1 - core)
    mix_copy.start()
    spare_arrival(0)
    for k in (0, 2):
        go(z_pass, 0, k)
    for k in (1, 0):
        go(x_send, 1, k)
    project(core * rows, mix_own)
    load(4).wait()
    mix_copy.wait_recv()

    def norm_rows(r, carry):
        lines = col(r * 16, 16)
        field = mix_own[lines, :].astype(F32) + mix_in[lines, :].astype(F32)
        scale = lax.rsqrt(jnp.mean(field * field, axis=-1, keepdims=True) + 1e-06)
        mixed = resid[lines, :].astype(F32) + field * scale * gain_mix_ref[...]
        after[lines, :] = mixed.astype(BF16)
        field = after[lines, :].astype(F32)
        scale = lax.rsqrt(jnp.mean(field * field, axis=-1, keepdims=True) + 1e-06)
        own = pl.ds(pl.multiple_of((m_own * 2 + core) * rows + r * 16, 16), 16)
        tokens[own, :] = (field * scale * gain_in_ref[...]).astype(BF16)
        return carry

    for h in (0, 1):
        with jax.named_scope("norm"):
            lax.fori_loop(h * bit // 16, (h + 1) * bit // 16, norm_rows, 0)
        token_copy(h).start()
        token_copy(2 + h).start()
        peer_token(6 + h).start()

    go_outer(z_own, 1, 0)
    go_inner(z_own, 1, 1)
    relay(0, z2, 0)
    relay(0, z3, 0)
    relay(0, z1, 1)
    spare_arrival(1)
    go(z_pass, 1, 0)
    go_outer(z_own, 1, 2)
    go_outer(z_pass, 1, 2)
    relay(0, z3, 1)
    relay(0, z2, 1)
    relay(1, z, 1)
    go_inner(z_pass, 1, 1)
    take_token(2)
    take_token(3)
    take_token(0)
    token_copy(4).start()
    take_token(1)
    token_copy(5).start()
    go_inner(z_own, 1, 2)
    go_inner(z_pass, 1, 2)

    either(lambda role: keep_own(0, role).wait())

    def half_dot(yy, m, cols):
        total = None
        for zz in range(4):
            depth = col((zz * 2 + yy) * chunk, chunk)
            term = jnp.dot(
                tokens[col(m * 2 * rows, 2 * rows), depth], w_up[depth, cols], preferred_element_type=F32
            )
            total = term if total is None else total + term
        return total

    full = jnp.where(inner, big // chunk, small // chunk)

    def each_columns(act):
        def step(n, carry):
            act(col(n * chunk, chunk))
            return carry

        lax.fori_loop(0, full, step, 0)
        act(pl.ds(pl.multiple_of(full * chunk, strip), strip))

    def up_early(m):
        def act(cols):
            acts[col(m * 2 * rows, 2 * rows), cols] = half_dot(y, m, cols)

        with jax.named_scope("up_early"):
            each_columns(act)

    def up_late(m):
        def act(cols):
            lines = col(m * 2 * rows, 2 * rows)
            total = jnp.maximum(acts[lines, cols] + half_dot(yo, m, cols), 0.0)
            hidden[lines, cols] = (total * total).astype(BF16)

        with jax.named_scope("up_late"):
            each_columns(act)

    def peer_pair(k):
        with jax.named_scope(f"peer#k={k}"):
            peer_arrival(k).wait_recv()
            peer_arrival(k + 1).wait_recv()

    peer_pair(6)
    up_early(m_own)

    peer_pair(2)
    up_early(m_x)


    peer_pair(0)
    up_early(m_z)
    relay(1, z1, 0)
    with jax.named_scope("up_y"):
        for zz in (z, z1, z3, z2):
            for dx in (0, 1):
                either(lambda role: y_arrival(0, zz, dx, role).wait_recv())
    up_late(m_own)
    relay(1, z1, 1)

    up_late(m_x)
    go_outer(z_own, 1, 1)
    go_outer(z_pass, 1, 1)
    up_late(m_z)
    take_token(4)
    take_token(5)
    peer_pair(4)
    up_early(m_d)
    up_late(m_d)
    either(lambda role: keep_own(1, role).wait())

    zh = z // 2
    near, far = (zh * 2, zh * 2 + 1), (soon, late)
    order = [(near[0], y), (near[1], y), (near[0], yo), (near[1], yo)]
    x_first = (True, True, True, False, True, False, True, False)
    order += [(far[0], y), (far[1], y), (far[0], yo), (far[1], yo)]

    def columns(i):
        zz, yy = order[i]
        return col((zz * 2 + yy) * chunk, chunk)

    def stage_a(i):
        zz, yy = order[i]
        if i % 4 >= 2:
            with jax.named_scope("down_y"):
                for dx in (0, 1):
                    either(lambda role: y_arrival(1, zz, dx, role).wait_recv())
        zz, yy = order[i]
        first = zz * 4 + yy * 2

        def multiply(role):
            depth = size(role)

            def step(p, carry):
                weights = jnp.concatenate(
                    [w_down[first, :depth, :], w_down[first + 1, :depth, :]], axis=1
                )
                both = jnp.dot(
                    hidden[col(p * half, half), :depth], weights, preferred_element_type=F32
                ).astype(BF16)
                for k in range(2):
                    for c in range(2):
                        lines = slice((2 * k + c) * rows, (2 * k + c + 1) * rows)
                        part[i, col((4 * c + 2 * p + k) * rows, rows), :] = both[lines]
                return carry

            lax.fori_loop(0, 2, step, 0)

        with jax.named_scope("down_mm"):
            either(multiply)
        peer_copy(i).start()

    def peer_copy(i):
        return remote(
            part.at[i, col((1 - core) * half, half), :],
            peer.at[i],
            c_send.at[0, i],
            c_recv.at[0, i],
            me,
            1 - core,
        )

    def chip_sum(i, m):
        own = part[i, col((core * 4 + m) * rows, rows), :].astype(F32)
        return own + peer[i, col(m * rows, rows), :].astype(F32)

    def legs(i):
        x_leg, z_leg = (x_dev, m_x), (z_dev, m_z)
        return (x_leg, z_leg) if x_first[i] else (z_leg, x_leg)

    def first_copy(i):
        dev = legs(i)[0][0]
        return remote(a_out.at[i], a_in.at[i], c_send.at[1, i], c_recv.at[1, i], dev, core)

    def second_copy(i):
        dev = legs(i)[1][0]
        return remote(b_out.at[i], b_in.at[i], c_send.at[2, i], c_recv.at[2, i], dev, core)

    def stage_b(i):
        with jax.named_scope("part_peer"):
            peer_copy(i).wait_recv()
        a_out[i, :rows, :] = chip_sum(i, legs(i)[0][1]).astype(BF16)
        a_out[i, rows:, :] = chip_sum(i, m_d).astype(BF16)
        first_copy(i).start()

    def stage_c(i):
        with jax.named_scope("part_first"):
            first_copy(i).wait_recv()
        b_out[i] = (chip_sum(i, legs(i)[1][1]) + a_in[i, rows:, :].astype(F32)).astype(BF16)
        second_copy(i).start()

    def stage_d(i):
        with jax.named_scope("part_second"):
            second_copy(i).wait_recv()
        ffn[:, columns(i)] = (
            chip_sum(i, m_own) + a_in[i, :rows, :].astype(F32) + b_in[i].astype(F32)
        )

    def far_relay(who, zz, sides):
        @pl.when(who)
        def _():
            for dx in sides:
                relay(1, zz, dx)


    far_relay(inner, soon, (0, 1))
    for i in range(8 + 5):
        if i < 8:
            stage_a(i)
        if 6 <= i < 8:
            stage_b(i)
        if i > 8 and i - 5 < 8:
            stage_d(i - 5)
        if 0 <= i - 2 < 8:
            stage_c(i - 2)
        if 0 <= i - 5 and i <= 8:
            stage_d(i - 5)
        if i < 6:
            stage_b(i)
        if i == 0:
            far_relay(inner, late, (0, 1))
        if i == 3:
            far_relay(outer, soon, (0, 1))
        if i == 3:
            far_relay(outer, late, (0,))
        if i == 4:
            far_relay(outer, late, (1,))

    def finish(r, carry):
        lines = col(r * 16, 16)
        field = ffn[lines, :]
        scale = lax.rsqrt(jnp.mean(field * field, axis=-1, keepdims=True) + 1e-06)
        out_ref[lines, :] = (
            after[lines, :].astype(F32) + field * scale * gain_out_ref[...]
        ).astype(BF16)
        return carry

    with jax.named_scope("finish"):
        lax.fori_loop(0, rows // 16, finish, 0)

    near_halo(lambda c: c.wait_send())
    far_halo(lambda c: c.wait_send())
    mix_copy.wait_send()
    for w in (0, 1):

        def done(role):
            send_own_y(w, role).wait_send()
            for k in (0, 1):
                x_send(w, k, role).wait_send()
            for k in range(3):
                z_own(w, k, role).wait_send()
                z_pass(w, k, role).wait_send()
            forward(w, z, 1, role).wait_send()
            for zz in columns_z:
                for dx in (0, 1):
                    forward(w, zz, dx, role).wait_send()

        either(done)
    for k in range(6):
        token_copy(k).wait_send()
    for k in range(8):
        peer_token(k).wait_send()
    for i in range(8):
        peer_copy(i).wait_send()
        first_copy(i).wait_send()
        second_copy(i).wait_send()


def slice_body(
    queries,
    key_heads,
    value_heads,
    sink_logit,
    doc_ids,
    residual,
    out_proj,
    gain_mix,
    up_proj,
    down_proj,
    gain_ffn_in,
    gain_ffn_out,
):
    positions, width = residual.shape
    rows = positions // lax.axis_size("tp")
    units = up_proj.shape[1] // 4 + up_proj.shape[0]
    strips = width // up_proj.shape[0]
    chunk = 2 * down_proj.shape[1]
    heads, kv = queries.shape[1], key_heads.shape[1]
    framed = positions + 2 * WINDOW
    inv_freq = np.float32(10000.0) ** (-np.arange(0, HD, 2, dtype=np.float32) / HD)
    freq = jnp.asarray(np.concatenate([inv_freq, inv_freq]).reshape(1, HD))
    vmem = pl.BlockSpec(memory_space=pltpu.VMEM)
    hbm = pl.BlockSpec(memory_space=pl.ANY)
    dma = pltpu.SemaphoreType.DMA
    shapes = [
        ((framed, HD), F32),
        ((framed, HD), F32),
        ((positions, heads), BF16),
        ((framed, kv), BF16),
        ((framed, kv), BF16),
        ((positions, heads), BF16),
        ((heads, width), BF16),
        ((rows, width), BF16),
        ((rows, width), BF16),
        ((rows, width), BF16),
        ((rows, width), BF16),
        ((rows, width), BF16),
        ((width, units), BF16),
        ((strips, units, down_proj.shape[1]), BF16),
        ((up_proj.shape[0], units), BF16),
        ((units, down_proj.shape[1]), BF16),
        ((8 * rows, width), BF16),
        ((8 * rows, units), F32),
        ((8 * rows, units), BF16),
        ((strips // 2, 8 * rows, chunk), BF16),
        ((strips // 2, 4 * rows, chunk), BF16),
        ((strips // 2, 2 * rows, chunk), BF16),
        ((strips // 2, 2 * rows, chunk), BF16),
        ((strips // 2, rows, chunk), BF16),
        ((strips // 2, rows, chunk), BF16),
        ((rows, width), F32),
    ]
    sems = [(2,), (5,), (4,), (4,), None, None, (2, 2), (2,)] + [(2, 8)] * 4 + [(6,), (6,), (8,), (8,), (3, 8), (3, 8)]
    return pl.pallas_call(
        layer_kernel,
        out_shape=jax.ShapeDtypeStruct((rows, width), BF16),
        in_specs=[pl.BlockSpec(memory_space=pltpu.SMEM)] + [vmem] * 5 + [hbm] * 7,
        out_specs=vmem,
        scratch_shapes=[pltpu.VMEM(s, t) for s, t in shapes]
        + [dma if s is None else dma(s) for s in sems],
        compiler_params=pltpu.CompilerParams(
            collective_id=0, has_side_effects=True, vmem_limit_bytes=58 << 20
        ),
        name="layer",
    )(
        sink_logit,
        freq,
        doc_ids.reshape(-1, WINDOW),
        gain_mix.reshape(1, -1),
        gain_ffn_in.reshape(1, -1),
        gain_ffn_out.reshape(1, -1),
        queries,
        key_heads,
        value_heads,
        residual,
        out_proj,
        up_proj,
        down_proj,
    )


def solution(mesh):
    sp, tp = mesh.shape["sp"], mesh.shape["tp"]
    direct = sp == 16 and tp == 2
    if direct:
        body, fine, rows = slice_body, mesh, ("sp",)
    else:
        body, rows = general_body, SP
        fine = Mesh(mesh.devices.reshape(sp // 8, 2, 2, 2, tp), SP + ("tp",))
    return jax.shard_map(
        body,
        mesh=fine,
        in_specs=(
            P(rows, "tp"),
            P(rows, "tp"),
            P(rows, "tp"),
            P("tp"),
            P(),
            P(rows, None),
            P("tp", None),
            P(),
            P(rows, "tp"),
            P("tp", rows),
            P(),
            P(),
        ),
        out_specs=P(rows + ("tp",), None),
        check_vma=False,
    )
```

```python
import math

import jax
import jax.numpy as jnp
import numpy as np
from jax import lax
from jax.experimental import pallas as pl
from jax.experimental.pallas import tpu as pltpu
from jax.sharding import Mesh, PartitionSpec as P

MESH = pl.DeviceIdType.MESH
BF16, F32 = jnp.bfloat16, jnp.float32

HD = 128
WINDOW = 128
SP = ("a", "b", "c", "d")
GRP = ("c", "d")
CROSS = ("a", "b")


def padded(shard, sides, width):
    for axis, dim in sides:
        devices, length = (lax.axis_size(axis), shard.shape[dim])
        up = [(i, (i + 1) % devices) for i in range(devices - 1)]
        down = [(j, i) for i, j in up]
        last = lax.slice_in_dim(shard, length - width, length, axis=dim)
        first = lax.slice_in_dim(shard, 0, width, axis=dim)
        before = lax.ppermute(last, axis, up)
        after = lax.ppermute(first, axis, down)
        shard = jnp.concatenate([before, shard, after], axis=dim)
    return shard


def rotate(field, places):
    half_dim = HD // 2
    inv_freq = 10000.0 ** (-jnp.arange(0, HD, 2, dtype=jnp.float32) / HD)
    angles = places[:, None, None] * inv_freq[None, None, :]
    cosine = jnp.cos(angles)
    sine = jnp.sin(angles)
    lower = field[..., :half_dim].astype(jnp.float32)
    upper = field[..., half_dim:].astype(jnp.float32)
    return jnp.concatenate(
        [lower * cosine - upper * sine, upper * cosine + lower * sine], axis=-1
    ).astype(jnp.bfloat16)


def banded(field, blocks):
    framed = field.reshape((blocks + 2, WINDOW) + field.shape[1:])
    return jnp.concatenate([framed[:-2], framed[1:-1], framed[2:]], axis=1)


def rms_scale(field, gain_vec):
    return field * lax.rsqrt(jnp.mean(field * field, axis=-1, keepdims=True) + 1e-06) * gain_vec


def swap_tp(rows):
    return lax.ppermute(rows, "tp", [(0, 1), (1, 0)])


def gather_tp(rows):
    if lax.axis_size("tp") == 2:
        return jnp.concatenate([rows, swap_tp(rows)], axis=0)
    return lax.all_gather(rows, "tp", axis=0, tiled=True)


def scatter_tp(partial_value, own_first=True):
    devices = lax.axis_size("tp")
    if devices != 2:
        return lax.psum_scatter(partial_value, "tp", scatter_dimension=0, tiled=True).astype(
            jnp.float32
        )
    share = partial_value.shape[0] // 2
    if own_first:
        own, other = partial_value[:share], partial_value[share:]
    else:
        me = lax.axis_index("tp")
        own = lax.dynamic_slice_in_dim(partial_value, me * share, share, 0)
        other = lax.dynamic_slice_in_dim(partial_value, (1 - me) * share, share, 0)
    return own.astype(jnp.float32) + swap_tp(other).astype(jnp.float32)


def to_peer(rows, k):
    if k == 0:
        return rows
    return lax.ppermute(rows, GRP, [(i, i ^ k) for i in range(4)])


def attention_part(sp, queries, key_heads, value_heads, sink_logit, doc_ids, out_proj):
    tok_count = queries.shape[0]
    blocks = tok_count // WINDOW
    q_local = queries.shape[1] // HD
    kv_local = key_heads.shape[1] // HD
    group_size = q_local // kv_local
    offset = lax.axis_index(sp) * tok_count
    places = (offset + jnp.arange(tok_count)).astype(jnp.float32)
    rotated_q = rotate(queries.reshape(tok_count, q_local, HD), places).reshape(
        blocks, WINDOW, kv_local, group_size, HD
    )
    rotated_k = rotate(key_heads.reshape(tok_count, kv_local, HD), places).reshape(
        tok_count, kv_local * HD
    )
    rimmed = padded(jnp.stack([rotated_k, value_heads]), ((sp, 1),), WINDOW)
    key_win = banded(rimmed[0].reshape(-1, kv_local, HD), blocks)
    val_win = banded(rimmed[1].reshape(-1, kv_local, HD), blocks)
    padded_docs = jnp.pad(doc_ids, (WINDOW, WINDOW), constant_values=-1)
    key_docs = banded(lax.dynamic_slice_in_dim(padded_docs, offset, tok_count + 2 * WINDOW), blocks)
    query_docs = lax.dynamic_slice_in_dim(doc_ids, offset, tok_count).reshape(blocks, WINDOW)
    q_index = jnp.arange(WINDOW)[:, None]
    k_index = jnp.arange(3 * WINDOW)[None, :]
    in_window = jnp.abs(k_index - WINDOW - q_index) <= WINDOW
    allowed = (in_window[None] & (query_docs[:, :, None] == key_docs[:, None, :]))[:, None, None]
    scores = jnp.einsum(
        "nqkgd,nskd->nkgqs", rotated_q, key_win, preferred_element_type=jnp.float32
    ) * HD ** (-0.5)
    masked = jnp.where(allowed, scores, -1e30)
    sink_col = sink_logit.reshape(kv_local, group_size)[None, :, :, None]
    top_score = jnp.maximum(jnp.max(masked, axis=-1), sink_col)
    exp_scores = jnp.where(allowed, jnp.exp(masked - top_score[..., None]), 0.0)
    denom_sum = jnp.sum(exp_scores, axis=-1) + jnp.exp(sink_col - top_score)
    probs = (exp_scores / denom_sum[..., None]).astype(jnp.bfloat16)
    attn = (
        jnp.einsum("nkgqs,nskd->nqkgd", probs, val_win, preferred_element_type=jnp.float32)
        .astype(jnp.bfloat16)
        .reshape(tok_count, q_local * HD)
    )
    part = jnp.dot(attn, out_proj, preferred_element_type=jnp.float32).astype(jnp.bfloat16)
    return part


def general_body(
    queries,
    key_heads,
    value_heads,
    sink_logit,
    doc_ids,
    residual,
    out_proj,
    gain_mix,
    up_proj,
    down_proj,
    gain_ffn_in,
    gain_ffn_out,
):
    up_quarter = lax.all_to_all(up_proj, GRP, split_axis=1, concat_axis=0, tiled=True)
    down_quarter = lax.all_to_all(down_proj, GRP, split_axis=0, concat_axis=1, tiled=True)
    queries, key_heads, up_quarter, down_quarter = lax.optimization_barrier(
        (queries, key_heads, up_quarter, down_quarter)
    )
    half_units = up_quarter.shape[1] // 2
    up_early = lax.all_gather(up_quarter[:, :half_units], CROSS, axis=0, tiled=True)
    up_late = lax.all_gather(up_quarter[:, half_units:], CROSS, axis=0, tiled=True)
    down_all = lax.all_gather(down_quarter, CROSS, axis=0, tiled=False)
    share_rows = queries.shape[0] // lax.axis_size("tp")
    part = attention_part(SP, queries, key_heads, value_heads, sink_logit, doc_ids, out_proj)
    part, up_early = lax.optimization_barrier((part, up_early))
    mixed = scatter_tp(part, own_first=False)
    own_residual = lax.dynamic_slice_in_dim(
        residual, lax.axis_index("tp") * share_rows, share_rows, 0
    )
    after_mix = (own_residual.astype(jnp.float32) + rms_scale(mixed, gain_mix)).astype(jnp.bfloat16)
    normed = rms_scale(after_mix.astype(jnp.float32), gain_ffn_in).astype(jnp.bfloat16)
    sizes = [lax.axis_size(a) for a in SP]
    order = [SP.index(a) for a in CROSS + GRP]
    width = normed.shape[1]
    strip = width // math.prod(sizes)
    normed = (
        normed.reshape(share_rows, *sizes, strip)
        .transpose(0, *[1 + o for o in order], 5)
        .reshape(share_rows, width)
    )
    blocks = [to_peer(normed, k) for k in range(4)]
    partials = []
    for k in (3, 2, 1, 0):
        rows = gather_tp(blocks[k])
        hidden = jnp.concatenate(
            [
                jnp.square(
                    jax.nn.relu(jnp.dot(rows, w, preferred_element_type=jnp.float32))
                ).astype(jnp.bfloat16)
                for w in (up_early, up_late)
            ],
            axis=1,
        )
        partial_value = jnp.concatenate(
            [
                jnp.dot(hidden, down_all[i], preferred_element_type=jnp.float32).astype(jnp.bfloat16)
                for i in range(down_all.shape[0])
            ],
            axis=1,
        )
        partials.append(to_peer(scatter_tp(partial_value).astype(jnp.bfloat16), k))
    ffn_out = sum(p.astype(jnp.float32) for p in partials)
    back = [order.index(i) for i in range(4)]
    ffn_out = (
        ffn_out.reshape(share_rows, *[sizes[o] for o in order], strip)
        .transpose(0, *[1 + b for b in back], 5)
        .reshape(share_rows, width)
    )
    return (after_mix.astype(jnp.float32) + rms_scale(ffn_out, gain_ffn_out)).astype(jnp.bfloat16)


def layer_kernel(
    sink_ref,
    freq_ref,
    docs_ref,
    gain_mix_ref,
    gain_in_ref,
    gain_out_ref,
    q_ref,
    k_ref,
    v_ref,
    residual_ref,
    proj_ref,
    up_ref,
    down_ref,
    out_ref,
    cos_ref,
    sin_ref,
    q_buf,
    k_buf,
    v_buf,
    attn,
    proj,
    resid,
    mix_own,
    mix_out,
    mix_in,
    after,
    w_up,
    w_down,
    spare_up,
    spare_down,
    tokens,
    acts,
    hidden,
    part,
    peer,
    a_out,
    a_in,
    b_out,
    b_in,
    ffn,
    local_sem,
    load_sem,
    h_send,
    h_recv,
    m_send,
    m_recv,
    a_send,
    s_recv,
    w_send,
    w_recv,
    y_send,
    y_recv,
    t_send,
    t_recv,
    p_send,
    p_recv,
    c_send,
    c_recv,
):
    me, core = lax.axis_index("sp"), lax.axis_index("tp")
    last = lax.axis_size("sp") - 1
    z, y, x = me // 4, lax.rem(me // 2, 2), lax.rem(me, 2)
    zl = lax.rem(z, 2)
    z1, z2, z3 = z + 1 - 2 * zl, lax.rem(z + 2, 4), 3 - z
    xo, yo = 1 - x, 1 - y
    positions = q_ref.shape[0]
    rows = positions // 2
    strip, span = up_ref.shape[0], up_ref.shape[1] // 2
    small, big = span // 2 - strip, span // 2 + strip
    chunk = 2 * strip
    half = 4 * rows
    blocks = positions // WINDOW
    kv_heads = k_ref.shape[1] // HD
    group_size = q_ref.shape[1] // k_ref.shape[1]

    def place(zz, yy, xx):
        return zz * 4 + yy * 2 + xx

    def col(start, size):
        return pl.ds(pl.multiple_of(start, size), size)

    x_dev, z_dev, y_dev = place(z, y, xo), place(z1, y, x), place(z, yo, x)

    inner = (z == 1) | (z == 2)
    outer = jnp.logical_not(inner)

    def either(act):
        pl.when(inner)(lambda: act(True))
        pl.when(outer)(lambda: act(False))

    def size(role):
        return big if role else small

    def slot(w, s, role):
        if w == 0:
            return w_up.at[col(s * strip, strip), : size(role)]
        return w_down.at[s, : size(role), :]

    def spare(w, role):
        return spare_down.at[: size(role), :] if w else spare_up.at[:, : size(role)]

    def shard(w, role, xx):
        start = pl.multiple_of(xx * span + (small if role else 0), strip)
        if w == 0:
            return up_ref.at[:, pl.ds(start, size(role))]
        return down_ref.at[pl.ds(start, size(role)), :]

    def remote(src, dst, send, recv, dev, c):
        return pltpu.make_async_remote_copy(
            src_ref=src,
            dst_ref=dst,
            send_sem=send,
            recv_sem=recv,
            device_id=(dev, c),
            device_id_type=MESH,
        )

    def to_x(dx):
        return xo if dx else x

    def x_send(w, k, role):
        target = (not role) if k else role
        return remote(
            shard(w, target, xo),
            spare(w, target) if k else slot(w, me, target),
            a_send.at[w, k],
            s_recv.at[w] if k else w_recv.at[w, z * 2 + 1],
            x_dev,
            core,
        )

    columns_z = (z1, z3, z2)

    def z_own(w, k, role):
        target = role if k == 1 else not role
        return remote(
            shard(w, target, x),
            slot(w, me, target),
            w_send.at[w, k],
            w_recv.at[w, z * 2],
            place(columns_z[k], y, x),
            core,
        )

    def z_pass(w, k, role):
        target = role if k == 1 else not role
        return remote(
            slot(w, x_dev, target) if k == 1 else spare(w, target),
            slot(w, x_dev, target),
            w_send.at[w, 3 + k],
            w_recv.at[w, z * 2 + 1],
            place(columns_z[k], y, x),
            core,
        )

    def spare_arrival(w):
        def act(role):
            ref = spare(w, not role)
            remote(ref, ref, a_send.at[w, 1], s_recv.at[w], me, core).wait_recv()

        with jax.named_scope(f"spare#w={w}"):
            either(act)

    def send_own_y(w, role):
        return remote(
            shard(w, role, x),
            slot(w, me, role),
            w_send.at[w, 6],
            y_recv.at[w, z * 2],
            y_dev,
            core,
        )

    def keep_own(w, role):
        return pltpu.make_async_copy(shard(w, role, x), slot(w, me, role), local_sem.at[w])

    def arrival(w, zz, dx, role):
        s = slot(w, place(zz, y, to_x(dx)), role)
        return remote(s, s, y_send.at[w, zz * 2 + dx], w_recv.at[w, zz * 2 + dx], me, core)

    def forward(w, zz, dx, role):
        s = slot(w, place(zz, y, to_x(dx)), role)
        return remote(s, s, y_send.at[w, zz * 2 + dx], y_recv.at[w, zz * 2 + dx], y_dev, core)

    def y_arrival(w, zz, dx, role):
        s = slot(w, place(zz, yo, to_x(dx)), role)
        return remote(s, s, y_send.at[w, zz * 2 + dx], y_recv.at[w, zz * 2 + dx], me, core)

    def relay(w, zz, dx):
        def act(role):
            arrival(w, zz, dx, role).wait_recv()
            forward(w, zz, dx, role).start()

        with jax.named_scope(f"relay#w={w}"):
            either(act)

    def go(copy, *at):
        either(lambda role: copy(*at, role).start())

    def go_inner(copy, *at):
        pl.when(inner)(lambda: copy(*at, True).start())

    def go_outer(copy, *at):
        pl.when(outer)(lambda: copy(*at, False).start())

    m_own, m_z = zl * 2 + x, (1 - zl) * 2 + x
    m_x, m_d = zl * 2 + xo, (1 - zl) * 2 + xo
    bit = rows // 2

    def token_bit(c, m, h):
        return tokens.at[col((m * 2 + c) * rows + h * bit, bit), :]

    sent = ((m_own, 0, z_dev), (m_own, 1, z_dev), (m_own, 0, x_dev), (m_own, 1, x_dev), (m_z, 0, x_dev), (m_z, 1, x_dev))
    got = ((m_z, 0), (m_z, 1), (m_x, 0), (m_x, 1), (m_d, 0), (m_d, 1))

    def token_copy(k):
        m, h, dev = sent[k]
        s = token_bit(core, m, h)
        return remote(s, s, t_send.at[k], t_recv.at[k], dev, core)

    def token_arrival(k):
        m, h = got[k]
        s = token_bit(core, m, h)
        return remote(s, s, t_send.at[k], t_recv.at[k], me, core)

    def peer_token(k):
        m, h = got[k] if k < 6 else (m_own, k - 6)
        s = token_bit(core, m, h)
        return remote(s, s, p_send.at[k], p_recv.at[k], me, 1 - core)

    def peer_arrival(k):
        m, h = got[k] if k < 6 else (m_own, k - 6)
        s = token_bit(1 - core, m, h)
        return remote(s, s, p_send.at[k], p_recv.at[k], me, 1 - core)

    def take_token(k):
        with jax.named_scope(f"token#k={k}"):
            token_arrival(k).wait_recv()
        peer_token(k).start()

    def halo(k, side):
        ref, buf = ((k_ref, k_buf), (v_ref, v_buf))[k]
        src = ref.at[positions - WINDOW :, :] if side else ref.at[:WINDOW, :]
        dst = buf.at[:WINDOW, :] if side else buf.at[positions + WINDOW :, :]
        sem = k * 2 + side
        return remote(src, dst, h_send.at[sem], h_recv.at[sem], me + (1 if side else -1), core)

    loads = (
        (k_ref, k_buf.at[WINDOW : positions + WINDOW, :]),
        (v_ref, v_buf.at[WINDOW : positions + WINDOW, :]),
        (q_ref, q_buf),
        (proj_ref, proj),
        (residual_ref.at[col(core * rows, rows), :], resid),
    )

    def load(i):
        return pltpu.make_async_copy(loads[i][0], loads[i][1], load_sem.at[i])

    barrier = pltpu.get_barrier_semaphore()
    friends = [(place(zz, y, x), core) for zz in columns_z] + [(x_dev, core), (y_dev, core), (me, 1 - core)]
    for dev in friends:
        pl.semaphore_signal(barrier, inc=1, device_id=dev, device_id_type=MESH)
    beyond = me - 1 + 2 * x
    has_beyond = (beyond >= 0) & (beyond <= last)

    @pl.when(has_beyond)
    def _():
        pl.semaphore_signal(barrier, inc=1, device_id=(beyond, core), device_id_type=MESH)

    for i in range(len(loads)):
        load(i).start()
    for w in (0, 1):
        go(keep_own, w)

    @pl.when(me == 0)
    def _():
        k_buf[:WINDOW, :] = jnp.zeros((WINDOW, k_buf.shape[1]), BF16)
        v_buf[:WINDOW, :] = jnp.zeros((WINDOW, k_buf.shape[1]), BF16)

    @pl.when(me == last)
    def _():
        k_buf[positions + WINDOW :, :] = jnp.zeros((WINDOW, k_buf.shape[1]), BF16)
        v_buf[positions + WINDOW :, :] = jnp.zeros((WINDOW, k_buf.shape[1]), BF16)

    def turn(b, carry):
        shape = (WINDOW, HD)
        at = (me * blocks + b - 1) * WINDOW + lax.broadcasted_iota(jnp.int32, shape, 0)
        angles = at.astype(F32) * freq_ref[...]
        lower = lax.broadcasted_iota(jnp.int32, shape, 1) < HD // 2
        lines = col(b * WINDOW, WINDOW)
        cos_ref[lines, :] = jnp.cos(angles)
        sine = jnp.sin(angles)
        sin_ref[lines, :] = jnp.where(lower, -sine, sine)
        return carry

    with jax.named_scope("angles"):
        lax.fori_loop(0, blocks + 2, turn, 0)
    with jax.named_scope("entry"):
        pl.semaphore_wait(barrier, len(friends) + has_beyond.astype(jnp.int32))

    def near_halo(act):
        for k in (0, 1):
            pl.when(x == 0)(lambda: act(halo(k, 1)))
            pl.when(x == 1)(lambda: act(halo(k, 0)))

    def far_halo(act):
        for k in (0, 1):
            pl.when((x == 1) & has_beyond)(lambda: act(halo(k, 1)))
            pl.when((x == 0) & has_beyond)(lambda: act(halo(k, 0)))

    def near_halo_arrival(act):
        for k in (0, 1):
            pl.when(x == 1)(lambda: act(halo(k, 1)))
            pl.when(x == 0)(lambda: act(halo(k, 0)))

    def far_halo_arrival(act):
        for k in (0, 1):
            pl.when((x == 0) & has_beyond)(lambda: act(halo(k, 1)))
            pl.when((x == 1) & has_beyond)(lambda: act(halo(k, 0)))

    near_halo(lambda c: c.start())
    go(x_send, 0, 0)
    far_halo(lambda c: c.start())
    go(x_send, 0, 1)
    go(send_own_y, 0)
    for k in range(3):
        go(z_own, 0, k)
    soon, late = jnp.where(outer, z2, z3), jnp.where(outer, z3, z2)
    go(send_own_y, 1)
    go_inner(z_own, 1, 0)

    def rotate_rows(buf, base, heads, shift):
        def step(b, carry):
            lines = col(base + b * WINDOW, WINDOW)
            turn = col(base + shift + b * WINDOW, WINDOW)
            cosine, sine = cos_ref[turn, :], sin_ref[turn, :]
            for h in range(heads):
                lanes = slice(h * HD, (h + 1) * HD)
                u = buf[lines, lanes].astype(F32)
                buf[lines, lanes] = (u * cosine + pltpu.roll(u, HD // 2, 1) * sine).astype(BF16)
            return carry

        return step

    with jax.named_scope("rotate"):
        load(0).wait()
        lax.fori_loop(0, blocks, rotate_rows(k_buf, WINDOW, kv_heads, 0), 0)
        load(2).wait()
        lax.fori_loop(0, blocks, rotate_rows(q_buf, 0, kv_heads * group_size, WINDOW), 0)
        load(1).wait()

    def attend(b):
        lines = col(b * WINDOW, WINDOW)
        window = pl.ds(pl.multiple_of(b * WINDOW, WINDOW), 3 * WINDOW)
        shape = (WINDOW, WINDOW)
        away = lax.broadcasted_iota(jnp.int32, shape, 1) - lax.broadcasted_iota(jnp.int32, shape, 0)

        def docs(j):
            at = me * blocks + b + j - 1
            inside = (at >= 0) & (at <= (last + 1) * blocks - 1)
            row = docs_ref[pl.ds(jnp.clip(at, 0, (last + 1) * blocks - 1), 1), :]
            return jnp.broadcast_to(jnp.where(inside, row, -1).astype(F32), shape)

        own_docs = jnp.transpose(docs(1))
        limits = (away >= 0, None, away <= 0)
        bias = []
        for j in range(3):
            same = own_docs == docs(j)
            allowed = same if limits[j] is None else limits[j] & same
            bias.append(jnp.where(allowed, 0.0, -1e30))
        bias = jnp.concatenate(bias, axis=1)

        def step(h, carry):
            keys = k_buf[window, col(h * HD, HD)]
            values = v_buf[window, col(h * HD, HD)]
            for g in range(group_size):
                head = h * group_size + g
                sink = sink_ref[head]
                scores = lax.dot_general(
                    q_buf[lines, col(head * HD, HD)],
                    keys,
                    (((1,), (1,)), ((), ())),
                    preferred_element_type=F32,
                )
                scores = scores * HD ** (-0.5) + bias
                top = jnp.maximum(jnp.max(scores, axis=1, keepdims=True), sink)
                exps = jnp.exp(scores - top)
                total = jnp.sum(exps, axis=1, keepdims=True) + jnp.exp(sink - top)
                probs = (exps * (1.0 / total)).astype(BF16)
                attn[lines, col(head * HD, HD)] = jnp.dot(
                    probs, values, preferred_element_type=F32
                ).astype(BF16)
            return carry

        with jax.named_scope("attend"):
            lax.fori_loop(0, kv_heads, step, 0)

    attend(1)
    with jax.named_scope("halo_near"):
        near_halo_arrival(lambda c: c.wait_recv())
    rotate_rows(k_buf, (1 - x) * (positions + WINDOW), kv_heads, 0)(0, 0)
    attend((1 - x) * (blocks - 1))
    relay(0, z1, 0)
    with jax.named_scope("halo_far"):
        far_halo_arrival(lambda c: c.wait_recv())
    rotate_rows(k_buf, x * (positions + WINDOW), kv_heads, 0)(0, 0)
    attend(x * (blocks - 1))
    relay(0, z, 1)
    go(z_pass, 0, 1)
    load(3).wait()

    def project(start, target):
        def step(n, carry):
            cols = col(n * chunk, chunk)
            target[:, cols] = jnp.dot(
                attn[col(start, rows), :], proj[:, cols], preferred_element_type=F32
            ).astype(BF16)
            return carry

        with jax.named_scope("project"):
            lax.fori_loop(0, proj.shape[1] // chunk, step, 0)

    project((1 - core) * rows, mix_out)
    mix_copy = remote(mix_out, mix_in, m_send, m_recv, me, 1 - core)
    mix_copy.start()
    spare_arrival(0)
    for k in (0, 2):
        go(z_pass, 0, k)
    for k in (1, 0):
        go(x_send, 1, k)
    project(core * rows, mix_own)
    load(4).wait()
    mix_copy.wait_recv()

    def norm_rows(r, carry):
        lines = col(r * 16, 16)
        field = mix_own[lines, :].astype(F32) + mix_in[lines, :].astype(F32)
        scale = lax.rsqrt(jnp.mean(field * field, axis=-1, keepdims=True) + 1e-06)
        mixed = resid[lines, :].astype(F32) + field * scale * gain_mix_ref[...]
        after[lines, :] = mixed.astype(BF16)
        field = after[lines, :].astype(F32)
        scale = lax.rsqrt(jnp.mean(field * field, axis=-1, keepdims=True) + 1e-06)
        own = pl.ds(pl.multiple_of((m_own * 2 + core) * rows + r * 16, 16), 16)
        tokens[own, :] = (field * scale * gain_in_ref[...]).astype(BF16)
        return carry

    for h in (0, 1):
        with jax.named_scope("norm"):
            lax.fori_loop(h * bit // 16, (h + 1) * bit // 16, norm_rows, 0)
        token_copy(h).start()
        token_copy(2 + h).start()
        peer_token(6 + h).start()

    go_outer(z_own, 1, 0)
    go_inner(z_own, 1, 1)
    relay(0, z2, 0)
    relay(0, z3, 0)
    relay(0, z1, 1)
    spare_arrival(1)
    go(z_pass, 1, 0)
    go_outer(z_own, 1, 2)
    go_outer(z_pass, 1, 2)
    relay(0, z3, 1)
    relay(0, z2, 1)
    relay(1, z, 1)
    go_inner(z_pass, 1, 1)
    take_token(2)
    take_token(3)
    take_token(0)
    token_copy(4).start()
    take_token(1)
    token_copy(5).start()
    go_inner(z_own, 1, 2)
    go_inner(z_pass, 1, 2)

    either(lambda role: keep_own(0, role).wait())

    def half_dot(yy, m, cols):
        total = None
        for zz in range(4):
            depth = col((zz * 2 + yy) * chunk, chunk)
            term = jnp.dot(
                tokens[col(m * 2 * rows, 2 * rows), depth], w_up[depth, cols], preferred_element_type=F32
            )
            total = term if total is None else total + term
        return total

    full = jnp.where(inner, big // chunk, small // chunk)

    def each_columns(act):
        def step(n, carry):
            act(col(n * chunk, chunk))
            return carry

        lax.fori_loop(0, full, step, 0)
        act(pl.ds(pl.multiple_of(full * chunk, strip), strip))

    def up_early(m):
        def act(cols):
            acts[col(m * 2 * rows, 2 * rows), cols] = half_dot(y, m, cols)

        with jax.named_scope("up_early"):
            each_columns(act)

    def up_late(m):
        def act(cols):
            lines = col(m * 2 * rows, 2 * rows)
            total = jnp.maximum(acts[lines, cols] + half_dot(yo, m, cols), 0.0)
            hidden[lines, cols] = (total * total).astype(BF16)

        with jax.named_scope("up_late"):
            each_columns(act)

    def peer_pair(k):
        with jax.named_scope(f"peer#k={k}"):
            peer_arrival(k).wait_recv()
            peer_arrival(k + 1).wait_recv()

    peer_pair(6)
    up_early(m_own)

    peer_pair(2)
    up_early(m_x)


    peer_pair(0)
    up_early(m_z)
    relay(1, z1, 0)
    with jax.named_scope("up_y"):
        for zz in (z, z1, z3, z2):
            for dx in (0, 1):
                either(lambda role: y_arrival(0, zz, dx, role).wait_recv())
    up_late(m_own)
    relay(1, z1, 1)

    up_late(m_x)
    go_outer(z_own, 1, 1)
    go_outer(z_pass, 1, 1)
    up_late(m_z)
    take_token(4)
    take_token(5)
    peer_pair(4)
    up_early(m_d)
    up_late(m_d)
    either(lambda role: keep_own(1, role).wait())

    zh = z // 2
    near, far = (zh * 2, zh * 2 + 1), (soon, late)
    order = [(near[0], y), (near[1], y), (near[0], yo), (near[1], yo)]
    x_first = (True, True, True, False, True, False, True, False)
    order += [(far[0], y), (far[1], y), (far[0], yo), (far[1], yo)]

    def columns(i):
        zz, yy = order[i]
        return col((zz * 2 + yy) * chunk, chunk)

    def stage_a(i):
        zz, yy = order[i]
        if i % 4 >= 2:
            with jax.named_scope("down_y"):
                for dx in (0, 1):
                    either(lambda role: y_arrival(1, zz, dx, role).wait_recv())
        zz, yy = order[i]
        first = zz * 4 + yy * 2

        def multiply(role):
            depth = size(role)

            def step(p, carry):
                weights = jnp.concatenate(
                    [w_down[first, :depth, :], w_down[first + 1, :depth, :]], axis=1
                )
                both = jnp.dot(
                    hidden[col(p * half, half), :depth], weights, preferred_element_type=F32
                ).astype(BF16)
                for k in range(2):
                    for c in range(2):
                        lines = slice((2 * k + c) * rows, (2 * k + c + 1) * rows)
                        part[i, col((4 * c + 2 * p + k) * rows, rows), :] = both[lines]
                return carry

            lax.fori_loop(0, 2, step, 0)

        with jax.named_scope("down_mm"):
            either(multiply)
        peer_copy(i).start()

    def peer_copy(i):
        return remote(
            part.at[i, col((1 - core) * half, half), :],
            peer.at[i],
            c_send.at[0, i],
            c_recv.at[0, i],
            me,
            1 - core,
        )

    def chip_sum(i, m):
        own = part[i, col((core * 4 + m) * rows, rows), :].astype(F32)
        return own + peer[i, col(m * rows, rows), :].astype(F32)

    def legs(i):
        x_leg, z_leg = (x_dev, m_x), (z_dev, m_z)
        return (x_leg, z_leg) if x_first[i] else (z_leg, x_leg)

    def first_copy(i):
        dev = legs(i)[0][0]
        return remote(a_out.at[i], a_in.at[i], c_send.at[1, i], c_recv.at[1, i], dev, core)

    def second_copy(i):
        dev = legs(i)[1][0]
        return remote(b_out.at[i], b_in.at[i], c_send.at[2, i], c_recv.at[2, i], dev, core)

    def stage_b(i):
        with jax.named_scope("part_peer"):
            peer_copy(i).wait_recv()
        a_out[i, :rows, :] = chip_sum(i, legs(i)[0][1]).astype(BF16)
        a_out[i, rows:, :] = chip_sum(i, m_d).astype(BF16)
        first_copy(i).start()

    def stage_c(i):
        with jax.named_scope("part_first"):
            first_copy(i).wait_recv()
        b_out[i] = (chip_sum(i, legs(i)[1][1]) + a_in[i, rows:, :].astype(F32)).astype(BF16)
        second_copy(i).start()

    def stage_d(i):
        with jax.named_scope("part_second"):
            second_copy(i).wait_recv()
        ffn[:, columns(i)] = (
            chip_sum(i, m_own) + a_in[i, :rows, :].astype(F32) + b_in[i].astype(F32)
        )

    def far_relay(who, zz, sides):
        @pl.when(who)
        def _():
            for dx in sides:
                relay(1, zz, dx)


    far_relay(inner, soon, (0, 1))
    for i in range(8 + 5):
        if i < 8:
            stage_a(i)
        if 5 <= i < 8:
            stage_b(i)
        if i > 8 and i - 5 < 8:
            stage_d(i - 5)
        if 0 <= i - 2 < 8:
            stage_c(i - 2)
        if 0 <= i - 5 and i <= 8:
            stage_d(i - 5)
        if i < 5:
            stage_b(i)
        if i == 0:
            far_relay(inner, late, (0, 1))
        if i == 3:
            far_relay(outer, soon, (0, 1))
        if i == 3:
            far_relay(outer, late, (0,))
        if i == 4:
            far_relay(outer, late, (1,))

    def finish(r, carry):
        lines = col(r * 16, 16)
        field = ffn[lines, :]
        scale = lax.rsqrt(jnp.mean(field * field, axis=-1, keepdims=True) + 1e-06)
        out_ref[lines, :] = (
            after[lines, :].astype(F32) + field * scale * gain_out_ref[...]
        ).astype(BF16)
        return carry

    with jax.named_scope("finish"):
        lax.fori_loop(0, rows // 16, finish, 0)

    near_halo(lambda c: c.wait_send())
    far_halo(lambda c: c.wait_send())
    mix_copy.wait_send()
    for w in (0, 1):

        def done(role):
            send_own_y(w, role).wait_send()
            for k in (0, 1):
                x_send(w, k, role).wait_send()
            for k in range(3):
                z_own(w, k, role).wait_send()
                z_pass(w, k, role).wait_send()
            forward(w, z, 1, role).wait_send()
            for zz in columns_z:
                for dx in (0, 1):
                    forward(w, zz, dx, role).wait_send()

        either(done)
    for k in range(6):
        token_copy(k).wait_send()
    for k in range(8):
        peer_token(k).wait_send()
    for i in range(8):
        peer_copy(i).wait_send()
        first_copy(i).wait_send()
        second_copy(i).wait_send()


def slice_body(
    queries,
    key_heads,
    value_heads,
    sink_logit,
    doc_ids,
    residual,
    out_proj,
    gain_mix,
    up_proj,
    down_proj,
    gain_ffn_in,
    gain_ffn_out,
):
    positions, width = residual.shape
    rows = positions // lax.axis_size("tp")
    units = up_proj.shape[1] // 4 + up_proj.shape[0]
    strips = width // up_proj.shape[0]
    chunk = 2 * down_proj.shape[1]
    heads, kv = queries.shape[1], key_heads.shape[1]
    framed = positions + 2 * WINDOW
    inv_freq = np.float32(10000.0) ** (-np.arange(0, HD, 2, dtype=np.float32) / HD)
    freq = jnp.asarray(np.concatenate([inv_freq, inv_freq]).reshape(1, HD))
    vmem = pl.BlockSpec(memory_space=pltpu.VMEM)
    hbm = pl.BlockSpec(memory_space=pl.ANY)
    dma = pltpu.SemaphoreType.DMA
    shapes = [
        ((framed, HD), F32),
        ((framed, HD), F32),
        ((positions, heads), BF16),
        ((framed, kv), BF16),
        ((framed, kv), BF16),
        ((positions, heads), BF16),
        ((heads, width), BF16),
        ((rows, width), BF16),
        ((rows, width), BF16),
        ((rows, width), BF16),
        ((rows, width), BF16),
        ((rows, width), BF16),
        ((width, units), BF16),
        ((strips, units, down_proj.shape[1]), BF16),
        ((up_proj.shape[0], units), BF16),
        ((units, down_proj.shape[1]), BF16),
        ((8 * rows, width), BF16),
        ((8 * rows, units), F32),
        ((8 * rows, units), BF16),
        ((strips // 2, 8 * rows, chunk), BF16),
        ((strips // 2, 4 * rows, chunk), BF16),
        ((strips // 2, 2 * rows, chunk), BF16),
        ((strips // 2, 2 * rows, chunk), BF16),
        ((strips // 2, rows, chunk), BF16),
        ((strips // 2, rows, chunk), BF16),
        ((rows, width), F32),
    ]
    sems = [(2,), (5,), (4,), (4,), None, None, (2, 2), (2,)] + [(2, 8)] * 4 + [(6,), (6,), (8,), (8,), (3, 8), (3, 8)]
    return pl.pallas_call(
        layer_kernel,
        out_shape=jax.ShapeDtypeStruct((rows, width), BF16),
        in_specs=[pl.BlockSpec(memory_space=pltpu.SMEM)] + [vmem] * 5 + [hbm] * 7,
        out_specs=vmem,
        scratch_shapes=[pltpu.VMEM(s, t) for s, t in shapes]
        + [dma if s is None else dma(s) for s in sems],
        compiler_params=pltpu.CompilerParams(
            collective_id=0, has_side_effects=True, vmem_limit_bytes=58 << 20
        ),
        name="layer",
    )(
        sink_logit,
        freq,
        doc_ids.reshape(-1, WINDOW),
        gain_mix.reshape(1, -1),
        gain_ffn_in.reshape(1, -1),
        gain_ffn_out.reshape(1, -1),
        queries,
        key_heads,
        value_heads,
        residual,
        out_proj,
        up_proj,
        down_proj,
    )


def solution(mesh):
    sp, tp = mesh.shape["sp"], mesh.shape["tp"]
    direct = sp == 16 and tp == 2
    if direct:
        body, fine, rows = slice_body, mesh, ("sp",)
    else:
        body, rows = general_body, SP
        fine = Mesh(mesh.devices.reshape(sp // 8, 2, 2, 2, tp), SP + ("tp",))
    return jax.shard_map(
        body,
        mesh=fine,
        in_specs=(
            P(rows, "tp"),
            P(rows, "tp"),
            P(rows, "tp"),
            P("tp"),
            P(),
            P(rows, None),
            P("tp", None),
            P(),
            P(rows, "tp"),
            P("tp", rows),
            P(),
            P(),
        ),
        out_specs=P(rows + ("tp",), None),
        check_vma=False,
    )
```
